128 devices in a mesh: ep: 128 (over z, y, x, core).
Axes of the slice: x: 4, y: 4, z: 4, core: 2. Of those that a mesh axis runs over, the one named last changes fastest.
Arguments:
- tokens: bfloat16 [2048, 2048], P('ep'), may hold values from -6 to 6
- state: float32 [2, 2048, 2048], P(None, 'ep'), may hold values from -4 to 4
- norm_mix: float32 [2048], replicated, may hold values from 0.1 to 1.9
- w_drive: bfloat16 [2048, 512], replicated, may hold values from -0.125 to 0.125
- lam_real: float32 [32, 64], replicated, may hold values from -1 to -0.05
- lam_imag: float32 [32, 64], replicated, may hold values from -3 to 3
- log_step: float32 [32], replicated, may hold values from -2.5 to 0.5
- b_real: float32 [32, 64, 16], replicated, may hold values from -1 to 1
- b_imag: float32 [32, 64, 16], replicated, may hold values from -1 to 1
- readout_real: float32 [32, 16, 64], replicated, may hold values from -0.5 to 0.5
- readout_imaginary: float32 [32, 16, 64], replicated, may hold values from -0.5 to 0.5
- d_skip: float32 [512], replicated, may hold values from -4 to 4
- w_value: bfloat16 [512, 512], replicated, may hold values from -0.25 to 0.25
- w_glugate: bfloat16 [512, 512], replicated, may hold values from -0.25 to 0.25
- w_output: bfloat16 [512, 2048], replicated, may hold values from -0.25 to 0.25
- norm_ffn: float32 [2048], replicated, may hold values from 0.1 to 1.9
- w_group: bfloat16 [2048, 4], replicated, may hold values from -0.125 to 0.125
- w_expert: bfloat16 [2048, 128], replicated, may hold values from -0.125 to 0.125
- route_ids: int32 [2048, 6], P('ep'), may hold values from 0 to 127, all different within a row; in each aligned block of 16 rows (0 to 15, 16 to 31, ...) at most 2 rows name the same one
- expert_gate: bfloat16 [128, 2048, 512], P('ep'), may hold values from -0.125 to 0.125
- expert_up: bfloat16 [128, 2048, 512], P('ep'), may hold values from -0.125 to 0.125
- expert_down: bfloat16 [128, 512, 2048], P('ep'), may hold values from -1 to 1
- dense_vector: float32 [2048], replicated, may hold values from -0.125 to 0.125
- dense_gate: bfloat16 [2048, 8192], P(None, 'ep'), may hold values from -0.125 to 0.125
- dense_up: bfloat16 [2048, 8192], P(None, 'ep'), may hold values from -0.125 to 0.125
- dense_down: bfloat16 [8192, 2048], P('ep'), may hold values from -0.25 to 0.25
Outputs:
- layer_out: bfloat16 [2048, 2048], P('ep')
- new_state: float32 [2, 2048, 2048], P(None, 'ep')
The draws below stay inside these ranges and needn't reach their ends.
Inputs may be any that keep to these rules, and one draw needn't show every extreme that they name: `route_ids`: each row names 6 different experts. Among the rows of one device no expert is named more than 2 times, a bound that some block reaches.
All inputs are finite; a program needn't handle non-finite values.
Results may differ from the reference program's by a relative error of at most 0.018.
Values may be sent and summed in bfloat16 or wider, within the bound.
A program may use at most 128 MiB of HBM per device.

```python
import math
import jax
import jax.numpy as jnp
import numpy as np
from jax import lax

D = 2048
S5W = 512
CH = 16
P_SIZE = 64
G = 32
GP = 2048
DENSE_FF = 8192
EXP_FF = 512
GROUPS = 4
TOPK = 6
SEQ_DEV = 16
SEQS = 2048
EXPERTS = 128
CAP = 2
N_EP = 128


def steps_of(stream_key, extent, cuts, smallest, largest):
    level, own = 1.0, jax.random.fold_in(stream_key, 6)
    for position, shards_of in cuts:
        steps = jnp.exp(jax.random.uniform(jax.random.fold_in(own, position), (shards_of,), jnp.float32, smallest / len(cuts), largest / len(cuts)))
        level = level * jnp.repeat(steps, extent[position] // shards_of).reshape([-1 if axis == position else 1 for axis in range(len(extent))])
    return level


def assign_block(stream_key, own, number, rows, amount, top, limit, slope):
    ranking = jax.random.permutation(stream_key, amount)
    crowded, usual = load_shares(amount, rows * top, limit, slope, True), load_shares(amount, rows * top, limit, slope, False)
    places = jnp.arange(amount)

    def named(tallies, rotation):
        used = int((tallies > 0).sum())
        fixed = max(1, used // 4)
        moved = fixed + (places - fixed + rotation * (used - fixed)) % max(1, amount - fixed)
        return jnp.zeros((amount,), jnp.int32).at[ranking[jnp.where(places < fixed, places, moved)]].set(jnp.asarray(tallies, jnp.int32))

    tallies = jnp.where(number % 4 == 0, named(crowded, number // 4), named(usual, number - number // 4 - 1))
    mixed = jax.random.permutation(jax.random.fold_in(own, 3), amount)
    source_of, sink = mixed[0:amount // 2 * 2:2], mixed[1:amount // 2 * 2:2]
    margin = jnp.minimum(tallies[source_of] - 1, limit - tallies[sink]) // 2
    margin = jnp.where((source_of == ranking[0]) | (sink == ranking[0]) | (tallies[sink] == 0), 0, jnp.maximum(margin, 0))
    moved = jax.random.randint(jax.random.fold_in(own, 4), (amount // 2,), 0, 1 << 20) % (margin + 1)
    tallies = tallies.at[source_of].add(-moved).at[sink].add(moved)
    items = jnp.searchsorted(jnp.cumsum(tallies), jnp.arange(rows * top), side="right").astype(jnp.int32)
    listing = items.reshape(top, rows).T
    listing = listing[jax.random.permutation(jax.random.fold_in(own, 1), rows)]
    rotation = jax.random.randint(jax.random.fold_in(own, 2), (rows, 1), 0, top)
    return jnp.take_along_axis(listing, (jnp.arange(top)[None, :] + rotation) % top, axis=1)


def load_shares(number_of, total, most, skew, full):
    loads = [(1 << 20) // math.isqrt(grade ** skew) + 1 for grade in range(1, number_of + 1)]
    largest = most if full else min(most, max(-(-total // number_of), total * loads[0] // sum(loads)))
    least = 1 if total - largest >= number_of - 1 else 0
    holding, rest = [largest] + [least] * (number_of - 1), total - largest - least * (number_of - 1)
    while rest > 0:
        free = [i for i in range(1, number_of) if holding[i] < largest] or [i for i in range(1, number_of) if holding[i] < most]
        pool, remaining = sum([loads[i] for i in free]), rest
        for i in free:
            addition = min(most - holding[i], max(1, remaining * loads[i] // pool), rest)
            holding[i] = holding[i] + addition
            rest = rest - addition
    return np.array(holding)


def bell_draw(stream_key, extent, spread, limit, cuts=(), kind=jnp.bfloat16):
    array = spread * jax.random.normal(stream_key, extent, jnp.float32)
    if cuts:
        array = array * steps_of(stream_key, extent, cuts, -0.22, 0.18)
    return jnp.clip(array, -limit, limit).astype(kind)


def setup_inputs(seed: int = 0) -> dict:
    key_list = jax.random.split(jax.random.key(seed), 27)
    tokens = bell_draw(key_list[0], (SEQS, D), 1.0, 6.0, ((0, 128),))
    state = bell_draw(key_list[1], (2, SEQS, GP), 0.5, 4.0, ((1, 128),), jnp.float32)
    norm_mix = jnp.clip(1.0 + 0.18 * jax.random.normal(key_list[2], (D,), jnp.float32), 0.1, 1.9)
    w_drive = bell_draw(key_list[3], (D, S5W), D ** -0.5, 0.125)
    lam_real = jnp.clip(jax.random.uniform(key_list[4], (G, P_SIZE), jnp.float32, -1.0, -0.05), -1.0, -0.05)
    lam_imag = jnp.clip(jax.random.uniform(key_list[5], (G, P_SIZE), jnp.float32, -3.0, 3.0), -3.0, 3.0)
    log_step = jnp.clip(jax.random.uniform(key_list[6], (G,), jnp.float32, -2.5, 0.5), -2.5, 0.5)
    b_real = bell_draw(key_list[7], (G, P_SIZE, CH), (2 * CH) ** -0.5, 1.0, (), jnp.float32)
    b_imag = bell_draw(key_list[8], (G, P_SIZE, CH), (2 * CH) ** -0.5, 1.0, (), jnp.float32)
    readout_real = bell_draw(key_list[9], (G, CH, P_SIZE), (2 * P_SIZE) ** -0.5, 0.5, (), jnp.float32)
    readout_imaginary = bell_draw(key_list[10], (G, CH, P_SIZE), (2 * P_SIZE) ** -0.5, 0.5, (), jnp.float32)
    d_skip = bell_draw(key_list[11], (S5W,), 1.0, 4.0, (), jnp.float32)
    w_value = bell_draw(key_list[12], (S5W, S5W), S5W ** -0.5, 0.25)
    w_glugate = bell_draw(key_list[13], (S5W, S5W), S5W ** -0.5, 0.25)
    w_output = bell_draw(key_list[14], (S5W, D), S5W ** -0.5, 0.25)
    norm_ffn = jnp.clip(1.0 + 0.18 * jax.random.normal(key_list[15], (D,), jnp.float32), 0.1, 1.9)
    w_group = bell_draw(key_list[16], (D, GROUPS), D ** -0.5, 0.125)
    w_expert = bell_draw(key_list[17], (D, EXPERTS), D ** -0.5, 0.125)
    route_ids_keys = jax.random.split(jax.random.fold_in(key_list[18], 1), SEQS // SEQ_DEV)
    route_ids_turns = jax.random.permutation(jax.random.fold_in(key_list[18], 3), SEQS // SEQ_DEV)
    route_ids = jax.vmap(lambda own, number: assign_block(jax.random.fold_in(key_list[18], 2), own, number, SEQ_DEV, EXPERTS, TOPK, CAP, 2))(route_ids_keys, route_ids_turns).reshape((SEQS, TOPK))
    expert_gate = bell_draw(key_list[19], (EXPERTS, D, EXP_FF), D ** -0.5, 0.125, ((0, 128),))
    expert_up = bell_draw(key_list[20], (EXPERTS, D, EXP_FF), D ** -0.5, 0.125, ((0, 128),))
    expert_down = bell_draw(key_list[21], (EXPERTS, EXP_FF, D), (EXP_FF // 16) ** -0.5, 1.0, ((0, 128),))
    dense_vector = bell_draw(key_list[22], (D,), D ** -0.5, 0.125, (), jnp.float32)
    dense_gate = bell_draw(key_list[23], (D, DENSE_FF), D ** -0.5, 0.125, ((1, 128),))
    dense_up = bell_draw(key_list[24], (D, DENSE_FF), D ** -0.5, 0.125, ((1, 128),))
    dense_down = bell_draw(key_list[25], (DENSE_FF, D), (DENSE_FF // 16) ** -0.5, 0.25, ((0, 128),))
    return dict(tokens=tokens, state=state, norm_mix=norm_mix, w_drive=w_drive, lam_real=lam_real, lam_imag=lam_imag, log_step=log_step, b_real=b_real, b_imag=b_imag, readout_real=readout_real, readout_imaginary=readout_imaginary, d_skip=d_skip, w_value=w_value, w_glugate=w_glugate, w_output=w_output, norm_ffn=norm_ffn, w_group=w_group, w_expert=w_expert, route_ids=route_ids, expert_gate=expert_gate, expert_up=expert_up, expert_down=expert_down, dense_vector=dense_vector, dense_gate=dense_gate, dense_up=dense_up, dense_down=dense_down)


EPS = 1e-05
HIGH_PRECISION = lax.Precision.HIGHEST

def rms_scale(values, gain):
    widened = values.astype(jnp.float32)
    scaled = widened * lax.rsqrt(lax.optimization_barrier(jnp.mean(widened * widened, axis=-1, keepdims=True)) + EPS)
    return (scaled * gain).astype(jnp.bfloat16)

def state_mixer(tokens, state, norm_mix, w_drive, lam_real, lam_imag, log_step, b_real, b_imag, readout_real, readout_imaginary, d_skip, w_value, w_glugate, w_output):
    row_count = tokens.shape[0]
    group_count, state_dimension = lam_real.shape
    channels = b_real.shape[2]
    normed_in = rms_scale(tokens, norm_mix)
    drive = jnp.dot(normed_in, w_drive, preferred_element_type=jnp.float32).astype(jnp.bfloat16)
    time_step = jnp.exp(log_step)[:, None]
    magnitude = jnp.exp(lam_real * time_step)
    decay_re = magnitude * jnp.cos(lam_imag * time_step)
    decay_im = magnitude * jnp.sin(lam_imag * time_step)
    modulus = lam_real * lam_real + lam_imag * lam_imag
    factor_re = ((decay_re - 1.0) * lam_real + decay_im * lam_imag) / modulus
    factor_im = (decay_im * lam_real - (decay_re - 1.0) * lam_imag) / modulus
    map_re = factor_re[:, :, None] * b_real - factor_im[:, :, None] * b_imag
    map_im = factor_re[:, :, None] * b_imag + factor_im[:, :, None] * b_real
    drive_wide = drive.astype(jnp.float32)
    grouped = drive_wide.reshape(row_count, group_count, channels)
    input_re = jnp.einsum('gpc,sgc->sgp', map_re, grouped, precision=HIGH_PRECISION)
    input_im = jnp.einsum('gpc,sgc->sgp', map_im, grouped, precision=HIGH_PRECISION)
    old_re = state[0].reshape(row_count, group_count, state_dimension)
    old_im = state[1].reshape(row_count, group_count, state_dimension)
    incoming_real = decay_re * old_re - decay_im * old_im + input_re
    incoming_imaginary = decay_re * old_im + decay_im * old_re + input_im
    projected_output = jnp.einsum('xej,fxj->fxe', readout_real, incoming_real, precision=HIGH_PRECISION) - jnp.einsum('xej,fxj->fxe', readout_imaginary, incoming_imaginary, precision=HIGH_PRECISION)
    readout = jax.nn.gelu(projected_output.reshape(row_count, group_count * channels) + d_skip * drive_wide).astype(jnp.bfloat16)
    value_part = jnp.dot(readout, w_value, preferred_element_type=jnp.float32)
    gate_part = jnp.dot(readout, w_glugate, preferred_element_type=jnp.float32)
    mixed = (value_part * jax.nn.sigmoid(gate_part)).astype(jnp.bfloat16)
    resid = (tokens.astype(jnp.float32) + jnp.dot(mixed, w_output, preferred_element_type=jnp.float32)).astype(jnp.bfloat16)
    new_state = jnp.stack([incoming_real.reshape(row_count, -1), incoming_imaginary.reshape(row_count, -1)])
    return (resid, new_state)

def route_gates(normed, w_group, w_expert, route_ids):
    row_count = normed.shape[0]
    group_count = w_group.shape[1]
    expert_count = w_expert.shape[1]
    per_group = expert_count // group_count
    group_exp = jnp.exp(jnp.dot(normed, w_group, preferred_element_type=jnp.float32))
    group_prob = group_exp / lax.optimization_barrier(jnp.sum(group_exp, axis=1, keepdims=True))
    inner_exp = jnp.exp(jnp.dot(normed, w_expert, preferred_element_type=jnp.float32)).reshape(row_count, group_count, per_group)
    inner_prob = inner_exp / lax.optimization_barrier(jnp.sum(inner_exp, axis=2, keepdims=True))
    joint = (group_prob[:, :, None] * inner_prob).reshape(row_count, expert_count)
    inner_flat = inner_prob.reshape(row_count, expert_count)
    matched = route_ids[:, :, None] == jnp.arange(expert_count, dtype=jnp.int32)[None, None, :]
    picked_joint = lax.optimization_barrier(jnp.sum(jnp.where(matched, joint[:, None, :], 0.0), axis=2))
    picked_inner = lax.optimization_barrier(jnp.sum(jnp.where(matched, inner_flat[:, None, :], 0.0), axis=2))
    return picked_joint / lax.optimization_barrier(jnp.sum(picked_inner, axis=1, keepdims=True))

def expert_rows(rows_in, w_gate, w_up, w_down):
    gate_part = jnp.dot(rows_in, w_gate, preferred_element_type=jnp.float32)
    up_part = jnp.dot(rows_in, w_up, preferred_element_type=jnp.float32)
    hidden = (jax.nn.silu(gate_part) * up_part).astype(jnp.bfloat16)
    return jnp.dot(hidden, w_down, preferred_element_type=jnp.float32).astype(jnp.bfloat16)

def reference(tokens, state, norm_mix, w_drive, lam_real, lam_imag, log_step, b_real, b_imag, readout_real, readout_imaginary, d_skip, w_value, w_glugate, w_output, norm_ffn, w_group, w_expert, route_ids, expert_gate, expert_up, expert_down, dense_vector, dense_gate, dense_up, dense_down):
    resid, new_state = state_mixer(tokens, state, norm_mix, w_drive, lam_real, lam_imag, log_step, b_real, b_imag, readout_real, readout_imaginary, d_skip, w_value, w_glugate, w_output)
    normed = rms_scale(resid, norm_ffn)
    gates = route_gates(normed, w_group, w_expert, route_ids)
    total_rows, width = normed.shape
    expert_count = w_expert.shape[1]
    slot_total = N_EP * CAP
    positions = jnp.arange(total_rows, dtype=jnp.int32)

    def visit(carry, matmul_argument):
        expert_id, w_gate, w_up, w_down = matmul_argument
        matched = route_ids == expert_id
        weight = lax.optimization_barrier(jnp.sum(jnp.where(matched, gates, 0.0), axis=1))
        chosen = jnp.any(matched, axis=1)
        ordinal = jnp.cumsum(chosen.astype(jnp.int32)) - 1
        target = jnp.where(chosen, ordinal, slot_total).astype(jnp.int32)
        slot_token = jnp.zeros((slot_total,), jnp.int32).at[target].set(positions, mode='drop')
        slot_live = jnp.zeros((slot_total,), jnp.float32).at[target].set(1.0, mode='drop')
        result = expert_rows(normed[slot_token], w_gate, w_up, w_down)
        contrib = result.astype(jnp.float32) * (weight[slot_token] * slot_live)[:, None]
        return (carry.at[slot_token].add(contrib), None)
    start_sum = jnp.zeros((total_rows, width), jnp.float32)
    expert_ids = jnp.arange(expert_count, dtype=jnp.int32)
    expert_sum, _ = lax.scan(visit, start_sum, (expert_ids, expert_gate, expert_up, expert_down))
    normed_wide = normed.astype(jnp.float32)
    branch_gate = jax.nn.sigmoid(jnp.dot(normed_wide, dense_vector, precision=HIGH_PRECISION))
    dense_g = jnp.dot(normed, dense_gate, preferred_element_type=jnp.float32)
    dense_u = jnp.dot(normed, dense_up, preferred_element_type=jnp.float32)
    dense_hidden = (branch_gate[:, None] * jax.nn.silu(dense_g) * dense_u).astype(jnp.bfloat16)
    dense_sum = jnp.dot(dense_hidden, dense_down, preferred_element_type=jnp.float32)
    layer_out = (resid.astype(jnp.float32) + dense_sum + expert_sum).astype(jnp.bfloat16)
    return (layer_out, new_state)
```

```python
import jax
import jax.numpy as jnp
from jax import lax
from jax.experimental import pallas as pl
from jax.experimental.pallas import tpu as pltpu
from jax.sharding import PartitionSpec as P

EPS = 1e-05
F32 = jnp.float32
BF16 = jnp.bfloat16
MESH = pl.DeviceIdType.MESH
ORDERS = (("x", "y", "z"), ("y", "z", "x"), ("z", "x", "y"))
GATHER_COLS = ((0, 768), (768, 768), (1536, 768))
SCATTER_COLS = ((0, 768), (768, 512), (1280, 768))
KINDS = (
    [("m1", 0, s) for s in (1, -1)]
    + [("f1", 0, s) for s in (1, -1)]
    + [("m2", o, s) for o in (0, 1, 3, 2) for s in (1, -1)]
    + [("f2", 0, 1), ("f2", 1, 1), ("f2", 3, -1), ("f2", 2, -1)]
    + [("m3a", o, s) for o in (0, 1, 3, 2) for s in (1, -1)]
    + [("m3", o, s) for o in (1, 3, 2) for s in (1, -1)]
    + [("f3", 0, 1), ("f3", 1, 1), ("f3", 3, -1), ("f3", 2, -1)]
)
SLOT = {kind: i for i, kind in enumerate(KINDS)}
FORWARD_PLUS = (0, 1)


def dot(a, b):
    return jnp.dot(a, b, preferred_element_type=F32)


def dot_nt(a, b):
    return lax.dot_general(a, b, (((1,), (1,)), ((), ())), preferred_element_type=F32)


def layer_kernel(
    normed_ref,
    resid_ref,
    ids_ref,
    vector_ref,
    group_ref,
    router_ref,
    gate_hbm,
    up_hbm,
    down_hbm,
    eg_hbm,
    eu_hbm,
    ed_hbm,
    out_ref,
    own,
    x,
    w_in,
    w_out,
    eg,
    eu,
    ed,
    hc,
    ct,
    picked,
    group_rows,
    p,
    r1,
    r2,
    r3,
    local_sem,
    swap_send,
    swap_recv,
    ag_send,
    ag_recv,
    rs_send,
    rs_recv,
):
    me = lax.axis_index("ep")
    core = lax.rem(me, 2)
    pos = {"x": lax.rem(me // 2, 4), "y": lax.rem(me // 8, 4), "z": me // 32}
    near = {d: [lax.rem(pos[d] + k, 4) for k in range(4)] for d in "xyz"}

    def device(at):
        return ((at["z"] * 4 + at["y"]) * 4 + at["x"]) * 2 + core

    def neighbour(d, s):
        at = dict(pos)
        at[d] = near[d][s % 4]
        return device(at)

    peers = {(d, s): neighbour(d, s) for d in "xyz" for s in (1, -1)}
    partner = me + 1 - 2 * core

    barrier = pltpu.get_barrier_semaphore()
    for peer in [*peers.values(), partner]:
        pl.semaphore_signal(barrier, inc=1, device_id=(peer,), device_id_type=MESH)

    def rows(i):
        return pl.ds(pl.multiple_of(i * 64, 64), 64)

    weights = [
        (gate_hbm, w_in.at[rows(core)]),
        (up_hbm, w_in.at[rows(2 + core)]),
        (down_hbm, w_out.at[rows(core)]),
        (eg_hbm, eg.at[core]),
        (eu_hbm, eu.at[core]),
        (ed_hbm, ed.at[core]),
    ]
    local = [pltpu.make_async_copy(s, t, local_sem.at[i]) for i, (s, t) in enumerate(weights)]
    for copy in local:
        copy.start()
    swaps = [
        pltpu.make_async_remote_copy(
            src_ref=s,
            dst_ref=t,
            send_sem=swap_send.at[i],
            recv_sem=swap_recv.at[i],
            device_id=(partner,),
            device_id_type=MESH,
        )
        for i, (s, t) in enumerate(weights)
    ]

    normed = normed_ref[...]
    own[:, pl.ds(0, 2048)] = normed
    ids = ids_ref[...]
    lanes = lax.broadcasted_iota(jnp.int32, (16, 128), 1)
    chosen = jnp.zeros((16, 128), F32)
    for t in range(6):
        chosen = chosen + jnp.where(ids[:, t : t + 1] == lanes, 1.0, 0.0)
    earlier = jnp.where(
        lax.broadcasted_iota(jnp.int32, (16, 16), 1) < lax.broadcasted_iota(jnp.int32, (16, 16), 0),
        1.0,
        0.0,
    )
    ordinal = dot(earlier.astype(BF16), chosen.astype(BF16))
    own[:, pl.ds(2048, 128)] = (chosen * (1.0 + ordinal)).astype(BF16)
    branch = jax.nn.sigmoid(
        jnp.sum(normed.astype(F32) * vector_ref[...], axis=1, keepdims=True)
    )
    high = branch.astype(BF16).astype(F32)
    middle = (branch - high).astype(BF16).astype(F32)
    low = branch - high - middle
    extra = jnp.where(lanes == 0, high, jnp.where(lanes == 1, middle, jnp.where(lanes == 2, low, 0.0)))
    own[:, pl.ds(2176, 128)] = extra.astype(BF16)
    own_copy = pltpu.make_async_copy(
        own, x.at[pos["z"], pos["y"], pos["x"]], local_sem.at[6]
    )
    own_copy.start()

    pl.semaphore_wait(barrier, 7)
    for copy in swaps:
        copy.start()

    def view(ref, colour, offsets, cols):
        at = {}
        for d, o in zip(ORDERS[colour], offsets):
            at[d] = slice(None) if o is None else near[d][o % 4]
        return ref.at[at["z"], at["y"], at["x"], :, cols]

    def gather_copy(colour, kind, receiving=False):
        name, o, s = kind
        start, width = GATHER_COLS[colour]
        cols = pl.ds(start, width)
        order = ORDERS[colour]
        back = -s if receiving else 0
        if name == "m1":
            d, where = order[0], (back, 0, 0)
        elif name == "f1":
            d, where = order[0], (back - s, 0, 0)
            half = width // 2
            cols = pl.ds(start, half) if s == 1 else pl.ds(start + half, half)
        elif name == "m2":
            d, where = order[1], (o, back, 0)
        elif name == "f2":
            d, where = order[1], (o, back - s, 0)
        elif name == "m3a":
            d, where = order[2], (o, 0, back)
        elif name == "m3":
            d, where = order[2], (None, o, back)
        else:
            d, where = order[2], (None, o, back - s)
        target = view(x, colour, where, cols)
        source = target
        if name == "m1" or (name in ("m2", "m3a") and o == 0):
            source = own.at[:, cols]
            if receiving:
                source = target
        i = SLOT[kind]
        return pltpu.make_async_remote_copy(
            src_ref=source,
            dst_ref=target,
            send_sem=ag_send.at[colour, i],
            recv_sem=ag_recv.at[colour, i],
            device_id=(peers[d, s],),
            device_id_type=MESH,
        )

    started = []

    def send(colour, name, o, s):
        copy = gather_copy(colour, (name, o, s))
        copy.start()
        started.append(copy)

    def both(colour, name, o):
        send(colour, name, o, 1)
        send(colour, name, o, -1)

    def receive(colour, name, o, s):
        gather_copy(colour, (name, o, s), True).wait_recv()

    colours = range(3)
    for c in colours:
        both(c, "m1", 0)
    for c in colours:
        both(c, "m2", 0)
    for c in colours:
        both(c, "m3a", 0)
    own_copy.wait()
    for s in (1, -1):
        for c in colours:
            receive(c, "m1", 0, s)
            o = 3 if s == 1 else 1
            send(c, "f1", 0, s)
            both(c, "m2", o)
            both(c, "m3a", o)
    for c in colours:
        receive(c, "m2", 0, 1)
        send(c, "f2", 0, 1)
        receive(c, "m2", 0, -1)
    for c in colours:
        receive(c, "f1", 0, 1)
        receive(c, "f1", 0, -1)
        both(c, "m2", 2)
        both(c, "m3a", 2)
    for o in (3, 1):
        for c in colours:
            receive(c, "m2", o, 1)
            if o == 1:
                send(c, "f2", 1, 1)
            receive(c, "m2", o, -1)
            if o == 3:
                send(c, "f2", 3, -1)
    for c in colours:
        receive(c, "m2", 2, 1)
        receive(c, "m2", 2, -1)
        send(c, "f2", 2, -1)
        both(c, "m3", 3)
        both(c, "m3", 1)
    for c in colours:
        for o in (0, 1, 3, 2):
            receive(c, "m3a", o, 1)
        send(c, "f3", 0, 1)
        for o in (0, 1, 3, 2):
            receive(c, "m3a", o, -1)
    for c in colours:
        for o, s in ((0, 1), (1, 1), (3, -1), (2, -1)):
            receive(c, "f2", o, s)
        both(c, "m3", 2)
    for c in colours:
        receive(c, "m3", 3, 1)
        receive(c, "m3", 3, -1)
        send(c, "f3", 3, -1)
        receive(c, "m3", 1, 1)
        send(c, "f3", 1, 1)
        receive(c, "m3", 1, -1)
    for c in colours:
        receive(c, "m3", 2, 1)
        receive(c, "m3", 2, -1)
        send(c, "f3", 2, -1)
    for c in colours:
        for o, s in ((0, 1), (1, 1), (3, -1), (2, -1)):
            receive(c, "f3", o, s)

    for copy in local:
        copy.wait()
    for copy in swaps:
        copy.wait_recv()

    first = me - core

    @pl.loop(0, 4)
    def _(zi):
        block = x.at[zi]
        values = block[:, :, :, pl.ds(0, 2048)].reshape(256, 2048)
        products = dot_nt(values, w_in[...])
        gate_part = products[:, :128]
        up_part = products[:, 128:]
        extras = block[:, :, :, pl.ds(2176, 128)].reshape(256, 128)
        scale = dot(extras, jnp.ones((128, 128), BF16))
        hidden = (scale * jax.nn.silu(gate_part) * up_part).astype(BF16)
        hc[zi, :, :, :, pl.ds(0, 128)] = hidden.reshape(4, 4, 16, 128)
        table = block[:, :, :, pl.ds(2048, 128)].reshape(256, 128)
        slot = lax.broadcasted_iota(jnp.int32, (128, 256), 1)
        expert_of = jnp.where(
            lax.broadcasted_iota(jnp.int32, (128, 256), 0) == first + slot // 128, 1.0, 0.0
        ).astype(BF16)
        entry = dot(table, expert_of)
        row = lax.broadcasted_iota(jnp.int32, (256, 256), 0)
        lane = lax.broadcasted_iota(jnp.int32, (256, 256), 1)
        wanted = (lax.rem(lane // 64, 2) + 1).astype(F32)
        sender = lax.rem(lane, 64)
        hit = (entry == wanted) & (sender == zi * 16 + row // 16)
        hc[zi, :, :, :, pl.ds(128, 256)] = (
            jnp.where(hit, 1.0, 0.0).astype(BF16).reshape(4, 4, 16, 256)
        )
        slot_t = lax.broadcasted_iota(jnp.int32, (256, 128), 0)
        expert_t = jnp.where(
            lax.broadcasted_iota(jnp.int32, (256, 128), 1) == first + slot_t // 128, 1.0, 0.0
        ).astype(BF16)
        entry_t = dot_nt(expert_t, table)
        wanted_t = (lax.rem(row // 64, 2) + 1).astype(F32)
        hit_t = (entry_t == wanted_t) & (lax.rem(row, 64) == zi * 16 + lane // 16)
        ct[:, pl.ds(pl.multiple_of(zi * 256, 256), 256)] = jnp.where(hit_t, 1.0, 0.0).astype(BF16)

    pick = ct[...]

    @pl.loop(0, 4)
    def _(j):
        cols = pl.ds(pl.multiple_of(j * 512, 512), 512)
        picked[:, cols] = dot(pick, x[:, :, :, :, cols].reshape(1024, 512)).astype(BF16)

    choices = dot(pick, x[:, :, :, :, pl.ds(2048, 128)].reshape(1024, 128))

    for g in range(4):
        group_rows[pl.ds(32 * g, 32), :] = jnp.broadcast_to(
            group_ref[pl.ds(g, 1), :].astype(F32), (32, 2048)
        ).astype(BF16)
    selected = picked[...]
    group_exp = jnp.exp(dot_nt(selected, group_rows[...]))
    inner_exp = jnp.exp(dot(selected, router_ref[...]))
    lane = lax.broadcasted_iota(jnp.int32, (256, 128), 1)
    row = lax.broadcasted_iota(jnp.int32, (256, 128), 0)
    group_sum = jnp.sum(jnp.where(lax.rem(lane, 32) == 0, group_exp, 0.0), axis=1, keepdims=True)
    inner_sum = jnp.zeros((256, 128), F32)
    for g in range(4):
        inside = lane // 32 == g
        total = jnp.sum(jnp.where(inside, inner_exp, 0.0), axis=1, keepdims=True)
        inner_sum = jnp.where(inside, total, inner_sum)
    inner = inner_exp / inner_sum
    joint = (group_exp / group_sum) * inner
    mine = lane == first + row // 128
    numerator = jnp.sum(jnp.where(mine, joint, 0.0), axis=1, keepdims=True)
    taken = choices > 0.0
    denominator = jnp.sum(jnp.where(taken, inner, 0.0), axis=1, keepdims=True)
    live = jnp.sum(jnp.where(taken, 1.0, 0.0), axis=1, keepdims=True) > 0.0
    gates = jnp.where(live, numerator / jnp.where(live, denominator, 1.0), 0.0)

    for e in range(2):
        rows_in = selected[e * 128 : (e + 1) * 128]
        gate_part = dot(rows_in, eg[e])
        up_part = dot(rows_in, eu[e])
        hidden = (jax.nn.silu(gate_part) * up_part).astype(BF16)
        result = dot(hidden, ed[e])
        weighted = result * gates[e * 128 : (e + 1) * 128]
        w_out[pl.ds(128 + e * 128, 128), :] = weighted.astype(BF16)

    def scatter_copy(colour, kind, receiving=False):
        name, o, s = kind
        start, width = SCATTER_COLS[colour]
        cols = pl.ds(start, width)
        order = ORDERS[colour]
        half = width // 2
        k = 0 if s == 1 else 1
        if name == "m1":
            d, where = order[0], (-s, 0, 0)
            target = r1.at[colour, k, :, pl.ds(0, width)]
        elif name == "f1":
            d, where = order[0], (2, 0, 0)
            cols = pl.ds(start, half) if s == 1 else pl.ds(start + half, half)
            target = r1.at[colour, 2 + k, :, pl.ds(0, half)]
        elif name == "m2":
            d, where = order[1], (o, -s, 0)
            target = r2.at[colour, k, o, :, pl.ds(0, width)]
        elif name == "f2":
            d, where = order[1], (o, 2, 0)
            target = r2.at[colour, 2, o, :, pl.ds(0, width)]
        elif name == "m3":
            d, where = order[2], (None, o, -s)
            target = r3.at[colour, k, o, :, :, pl.ds(0, width)]
        else:
            d, where = order[2], (None, o, 2)
            target = r3.at[colour, 2, o, :, :, pl.ds(0, width)]
        i = SLOT[kind] if kind in SLOT else SLOT["m3a", o, s]
        return pltpu.make_async_remote_copy(
            src_ref=target if receiving else view(p, colour, where, cols),
            dst_ref=target,
            send_sem=rs_send.at[colour, i],
            recv_sem=rs_recv.at[colour, i],
            device_id=(peers[d, -s],),
            device_id_type=MESH,
        )

    def pass_on(colour, name, o, s):
        copy = scatter_copy(colour, (name, o, s))
        copy.start()
        started.append(copy)

    def arrive(colour, name, o, s):
        scatter_copy(colour, (name, o, s), True).wait_recv()

    def partial(colour, o):
        start, width = SCATTER_COLS[colour]
        d = ORDERS[colour][2]
        i = near[d][o]
        cols = pl.ds(start, width)
        if d == "z":
            left = hc[i]
        elif d == "y":
            left = hc[:, i]
        else:
            left = hc[:, :, i]
        values = dot(left.reshape(256, 384), w_out[:, cols]).astype(BF16).reshape(4, 4, 16, width)
        if d == "z":
            p[i, :, :, :, cols] = values
        elif d == "y":
            p[:, i, :, :, cols] = values
        else:
            p[:, :, i, :, cols] = values

    def block(colour, where, cols=None):
        start, width = SCATTER_COLS[colour]
        return view(p, colour, where, pl.ds(start, width) if cols is None else cols)

    def add(colour, where, *arrived, cols=None):
        ref = block(colour, where, cols)
        total = ref[...].astype(F32)
        for a in arrived:
            total = total + a[...].astype(F32)
        ref[...] = total.astype(BF16)

    def in3(c, k, o):
        return r3.at[c, k, o, :, :, pl.ds(0, SCATTER_COLS[c][1])]

    def in2(c, k, o):
        return r2.at[c, k, o, :, pl.ds(0, SCATTER_COLS[c][1])]

    backwards = (2, 3, 1, 0)

    def sign_of(o):
        return 1 if o in FORWARD_PLUS else -1

    for c in colours:
        partial(c, 2)
        for o in backwards:
            pass_on(c, "f3", o, sign_of(o))
    for s in (1, -1):
        for c in colours:
            partial(c, (-s) % 4)
            for o in backwards:
                if sign_of(o) != s:
                    pass_on(c, "m3", o, s)
    for c in colours:
        partial(c, 0)
    for o in backwards:
        for c in colours:
            s = sign_of(o)
            arrive(c, "f3", o, s)
            add(c, (None, o, -s), in3(c, 2, o))
            pass_on(c, "m3", o, s)
    for o in backwards:
        for c in colours:
            arrive(c, "m3", o, 1)
            arrive(c, "m3", o, -1)
            add(c, (None, o, 0), in3(c, 0, o), in3(c, 1, o))
            if o == 2:
                for q in backwards:
                    pass_on(c, "f2", q, sign_of(q))
            elif o in (1, 3):
                s = -1 if o == 1 else 1
                for q in backwards:
                    if sign_of(q) != s:
                        pass_on(c, "m2", q, s)
    for q in backwards:
        for c in colours:
            s = sign_of(q)
            arrive(c, "f2", q, s)
            add(c, (q, -s, 0), in2(c, 2, q))
            pass_on(c, "m2", q, s)
    for q in backwards:
        for c in colours:
            arrive(c, "m2", q, 1)
            arrive(c, "m2", q, -1)
            add(c, (q, 0, 0), in2(c, 0, q), in2(c, 1, q))
            if q == 2:
                pass_on(c, "f1", 0, 1)
                pass_on(c, "f1", 0, -1)
    for s in (1, -1):
        for c in colours:
            start, width = SCATTER_COLS[c]
            half = width // 2
            arrive(c, "f1", 0, s)
            cols = pl.ds(start, half) if s == 1 else pl.ds(start + half, half)
            add(c, (-s, 0, 0), r1.at[c, 2 if s == 1 else 3, :, pl.ds(0, half)], cols=cols)
            pass_on(c, "m1", 0, s)
    for c in colours:
        start, width = SCATTER_COLS[c]
        cols = pl.ds(start, width)
        arrive(c, "m1", 0, 1)
        arrive(c, "m1", 0, -1)
        total = resid_ref[:, cols].astype(F32) + block(c, (0, 0, 0))[...].astype(F32)
        for k in range(2):
            total = total + r1[c, k, :, pl.ds(0, width)].astype(F32)
        out_ref[:, cols] = total.astype(BF16)

    for copy in started:
        copy.wait_send()
    for copy in swaps:
        copy.wait_send()


def layer(normed, resid, route_ids, dense_vector, w_group, w_expert, dense_gate, dense_up,
          dense_down, expert_gate, expert_up, expert_down):
    kinds = len(KINDS)
    vmem = pl.BlockSpec(memory_space=pltpu.VMEM)
    hbm = pl.BlockSpec(memory_space=pl.ANY)
    return pl.pallas_call(
        layer_kernel,
        out_shape=jax.ShapeDtypeStruct((16, 2048), BF16),
        in_specs=[vmem] * 6 + [hbm] * 6,
        out_specs=vmem,
        scratch_shapes=[
            pltpu.VMEM((16, 2304), BF16),
            pltpu.VMEM((4, 4, 4, 16, 2304), BF16),
            pltpu.VMEM((256, 2048), BF16),
            pltpu.VMEM((384, 2048), BF16),
            pltpu.VMEM((2, 2048, 512), BF16),
            pltpu.VMEM((2, 2048, 512), BF16),
            pltpu.VMEM((2, 512, 2048), BF16),
            pltpu.VMEM((4, 4, 4, 16, 384), BF16),
            pltpu.VMEM((256, 1024), BF16),
            pltpu.VMEM((256, 2048), BF16),
            pltpu.VMEM((128, 2048), BF16),
            pltpu.VMEM((4, 4, 4, 16, 2048), BF16),
            pltpu.VMEM((3, 4, 16, 768), BF16),
            pltpu.VMEM((3, 3, 4, 16, 768), BF16),
            pltpu.VMEM((3, 3, 4, 4, 16, 768), BF16),
            pltpu.SemaphoreType.DMA((7,)),
            pltpu.SemaphoreType.DMA((6,)),
            pltpu.SemaphoreType.DMA((6,)),
            pltpu.SemaphoreType.DMA((3, kinds)),
            pltpu.SemaphoreType.DMA((3, kinds)),
            pltpu.SemaphoreType.DMA((3, kinds)),
            pltpu.SemaphoreType.DMA((3, kinds)),
        ],
        compiler_params=pltpu.CompilerParams(
            collective_id=0, has_side_effects=True, vmem_limit_bytes=58 * 1024 * 1024
        ),
        cost_estimate=pl.CostEstimate(flops=8_000_000_000, bytes_accessed=20_000_000, transcendentals=0),
    )(
        normed,
        resid,
        route_ids,
        dense_vector.reshape(1, -1),
        jnp.transpose(w_group),
        w_expert,
        jnp.transpose(dense_gate),
        jnp.transpose(dense_up),
        dense_down,
        expert_gate[0],
        expert_up[0],
        expert_down[0],
    )


def rms_scale(values, gain):
    widened = values.astype(jnp.float32)
    scaled = widened * lax.rsqrt(jnp.mean(widened * widened, axis=-1, keepdims=True) + EPS)
    return (scaled * gain).astype(jnp.bfloat16)


def state_mixer(
    tokens,
    state,
    norm_mix,
    w_drive,
    lam_real,
    lam_imag,
    log_step,
    b_real,
    b_imag,
    readout_real,
    readout_imaginary,
    d_skip,
    w_value,
    w_glugate,
    w_output,
):
    row_count = tokens.shape[0]
    group_count, state_dimension = lam_real.shape
    channels = b_real.shape[2]
    normed_in = rms_scale(tokens, norm_mix)
    drive = jnp.dot(normed_in, w_drive, preferred_element_type=jnp.float32).astype(jnp.bfloat16)
    time_step = jnp.exp(log_step)[:, None]
    magnitude = jnp.exp(lam_real * time_step)
    decay_re = magnitude * jnp.cos(lam_imag * time_step)
    decay_im = magnitude * jnp.sin(lam_imag * time_step)
    modulus = lam_real * lam_real + lam_imag * lam_imag
    factor_re = ((decay_re - 1.0) * lam_real + decay_im * lam_imag) / modulus
    factor_im = (decay_im * lam_real - (decay_re - 1.0) * lam_imag) / modulus
    map_re = factor_re[:, :, None] * b_real - factor_im[:, :, None] * b_imag
    map_im = factor_re[:, :, None] * b_imag + factor_im[:, :, None] * b_real
    drive_wide = drive.astype(jnp.float32)
    grouped = drive_wide.reshape(row_count, group_count, channels)
    input_re = jnp.einsum("gpc,sgc->sgp", map_re, grouped)
    input_im = jnp.einsum("gpc,sgc->sgp", map_im, grouped)
    old_re = state[0].reshape(row_count, group_count, state_dimension)
    old_im = state[1].reshape(row_count, group_count, state_dimension)
    incoming_real = decay_re * old_re - decay_im * old_im + input_re
    incoming_imaginary = decay_re * old_im + decay_im * old_re + input_im
    projected_output = jnp.einsum("xej,fxj->fxe", readout_real, incoming_real) - jnp.einsum(
        "xej,fxj->fxe", readout_imaginary, incoming_imaginary
    )
    readout = jax.nn.gelu(
        projected_output.reshape(row_count, group_count * channels) + d_skip * drive_wide
    ).astype(jnp.bfloat16)
    value_part = jnp.dot(readout, w_value, preferred_element_type=jnp.float32)
    gate_part = jnp.dot(readout, w_glugate, preferred_element_type=jnp.float32)
    mixed = (value_part * jax.nn.sigmoid(gate_part)).astype(jnp.bfloat16)
    resid = (
        tokens.astype(jnp.float32) + jnp.dot(mixed, w_output, preferred_element_type=jnp.float32)
    ).astype(jnp.bfloat16)
    new_state = jnp.stack(
        [incoming_real.reshape(row_count, -1), incoming_imaginary.reshape(row_count, -1)]
    )
    return (resid, new_state)


def on_device(
    tokens,
    state,
    norm_mix,
    w_drive,
    lam_real,
    lam_imag,
    log_step,
    b_real,
    b_imag,
    readout_real,
    readout_imaginary,
    d_skip,
    w_value,
    w_glugate,
    w_output,
    norm_ffn,
    w_group,
    w_expert,
    route_ids,
    expert_gate,
    expert_up,
    expert_down,
    dense_vector,
    dense_gate,
    dense_up,
    dense_down,
):
    resid, new_state = state_mixer(
        tokens,
        state,
        norm_mix,
        w_drive,
        lam_real,
        lam_imag,
        log_step,
        b_real,
        b_imag,
        readout_real,
        readout_imaginary,
        d_skip,
        w_value,
        w_glugate,
        w_output,
    )
    normed = rms_scale(resid, norm_ffn)
    layer_out = layer(
        normed, resid, route_ids, dense_vector, w_group, w_expert, dense_gate, dense_up,
        dense_down, expert_gate, expert_up, expert_down,
    )
    return (layer_out, new_state)


def solution(mesh):
    placed = (
        P("ep", None),
        P(None, "ep", None),
        P(),
        P(),
        P(),
        P(),
        P(),
        P(),
        P(),
        P(),
        P(),
        P(),
        P(),
        P(),
        P(),
        P(),
        P(),
        P(),
        P("ep", None),
        P("ep", None, None),
        P("ep", None, None),
        P("ep", None, None),
        P(),
        P(None, "ep"),
        P(None, "ep"),
        P("ep", None),
    )
    return jax.shard_map(
        on_device,
        mesh=mesh,
        in_specs=placed,
        out_specs=(P("ep", None), P(None, "ep", None)),
        check_vma=False,
    )
```

```python
import jax
import jax.numpy as jnp
from jax import lax
from jax.experimental import pallas as pl
from jax.experimental.pallas import tpu as pltpu
from jax.sharding import PartitionSpec as P

EPS = 1e-05
F32 = jnp.float32
BF16 = jnp.bfloat16
MESH = pl.DeviceIdType.MESH
ORDERS = (("x", "y", "z"), ("y", "z", "x"), ("z", "x", "y"))
GATHER_COLS = ((0, 768), (768, 768), (1536, 768))
SCATTER_COLS = ((0, 768), (768, 512), (1280, 768))
KINDS = (
    [("m1", 0, s) for s in (1, -1)]
    + [("f1", 0, s) for s in (1, -1)]
    + [("m2", o, s) for o in (0, 1, 3, 2) for s in (1, -1)]
    + [("f2", 0, 1), ("f2", 1, 1), ("f2", 3, -1), ("f2", 2, -1)]
    + [("m3a", o, s) for o in (0, 1, 3, 2) for s in (1, -1)]
    + [("m3", o, s) for o in (1, 3, 2) for s in (1, -1)]
    + [("f3", 0, 1), ("f3", 1, 1), ("f3", 3, -1), ("f3", 2, -1)]
)
SLOT = {kind: i for i, kind in enumerate(KINDS)}
FORWARD_PLUS = (0, 1)


def dot(a, b):
    return jnp.dot(a, b, preferred_element_type=F32)


def dot_nt(a, b):
    return lax.dot_general(a, b, (((1,), (1,)), ((), ())), preferred_element_type=F32)


def layer_kernel(
    tokens_hbm,
    state_hbm,
    norm_mix_hbm,
    w_drive_hbm,
    lam_real_hbm,
    lam_imag_hbm,
    log_step_hbm,
    b_real_hbm,
    b_imag_hbm,
    readout_real_hbm,
    readout_imag_hbm,
    d_skip_hbm,
    w_value_hbm,
    w_glugate_hbm,
    w_output_hbm,
    norm_ffn_hbm,
    group_hbm,
    router_hbm,
    ids_hbm,
    vector_hbm,
    gate_hbm,
    up_hbm,
    down_hbm,
    eg_hbm,
    eu_hbm,
    ed_hbm,
    out_ref,
    state_out,
    tokens_ref,
    state_ref,
    norm_mix_ref,
    w_drive_ref,
    lam_real_ref,
    lam_imag_ref,
    log_step_ref,
    b_real_ref,
    b_imag_ref,
    readout_real_ref,
    readout_imag_ref,
    d_skip_ref,
    w_value_ref,
    w_glugate_ref,
    w_output_ref,
    norm_ffn_ref,
    group_ref,
    router_ref,
    ids_ref,
    vector_ref,
    input_re,
    input_im,
    readout_re,
    readout_im,
    decay_rows,
    resid_ref,
    own,
    x,
    w_in,
    w_out,
    eg,
    eu,
    ed,
    hc,
    ct,
    picked,
    group_rows,
    p,
    r1,
    r2,
    r3,
    load_sem,
    local_sem,
    swap_send,
    swap_recv,
    ag_send,
    ag_recv,
    rs_send,
    rs_recv,
):
    me = lax.axis_index("ep")
    core = lax.rem(me, 2)
    pos = {"x": lax.rem(me // 2, 4), "y": lax.rem(me // 8, 4), "z": me // 32}
    near = {d: [lax.rem(pos[d] + k, 4) for k in range(4)] for d in "xyz"}

    def device(at):
        return ((at["z"] * 4 + at["y"]) * 4 + at["x"]) * 2 + core

    def neighbour(d, s):
        at = dict(pos)
        at[d] = near[d][s % 4]
        return device(at)

    peers = {(d, s): neighbour(d, s) for d in "xyz" for s in (1, -1)}
    partner = me + 1 - 2 * core

    barrier = pltpu.get_barrier_semaphore()
    for peer in [*peers.values(), partner]:
        pl.semaphore_signal(barrier, inc=1, device_id=(peer,), device_id_type=MESH)

    sources = (
        lam_real_hbm, lam_imag_hbm, log_step_hbm, b_real_hbm, b_imag_hbm, readout_real_hbm,
        readout_imag_hbm, tokens_hbm, norm_mix_hbm, w_drive_hbm, state_hbm, d_skip_hbm,
        w_value_hbm, w_glugate_hbm, w_output_hbm, norm_ffn_hbm, ids_hbm, vector_hbm, group_hbm,
        router_hbm,
    )
    targets = (
        lam_real_ref, lam_imag_ref, log_step_ref, b_real_ref, b_imag_ref, readout_real_ref,
        readout_imag_ref, tokens_ref, norm_mix_ref, w_drive_ref, state_ref, d_skip_ref,
        w_value_ref, w_glugate_ref, w_output_ref, norm_ffn_ref, ids_ref, vector_ref, group_ref,
        router_ref,
    )
    loads = [
        pltpu.make_async_copy(a, b, load_sem.at[i]) for i, (a, b) in enumerate(zip(sources, targets))
    ]
    for copy in loads:
        copy.start()

    def loaded(first, last):
        for copy in loads[first:last]:
            copy.wait()

    def rows(i):
        return pl.ds(pl.multiple_of(i * 64, 64), 64)

    weights = [
        (gate_hbm, w_in.at[rows(core)]),
        (up_hbm, w_in.at[rows(2 + core)]),
        (down_hbm, w_out.at[rows(core)]),
        (eg_hbm, eg.at[core]),
        (eu_hbm, eu.at[core]),
        (ed_hbm, ed.at[core]),
    ]
    local = [pltpu.make_async_copy(s, t, local_sem.at[i]) for i, (s, t) in enumerate(weights)]
    for copy in local:
        copy.start()
    swaps = [
        pltpu.make_async_remote_copy(
            src_ref=s,
            dst_ref=t,
            send_sem=swap_send.at[i],
            recv_sem=swap_recv.at[i],
            device_id=(partner,),
            device_id_type=MESH,
        )
        for i, (s, t) in enumerate(weights)
    ]

    for ref in (input_re, input_im, readout_re, readout_im):
        ref[...] = jnp.zeros((4, 128, 512), BF16)
    loaded(0, 7)
    square = lax.broadcasted_iota(jnp.int32, (32, 32), 0) == lax.broadcasted_iota(
        jnp.int32, (32, 32), 1
    )
    time_step = jnp.sum(
        jnp.where(square, jnp.exp(log_step_ref[...]), 0.0), axis=1, keepdims=True
    )
    lam_re = lam_real_ref[...]
    lam_im = lam_imag_ref[...]
    magnitude = jnp.exp(lam_re * time_step)
    decay_re = magnitude * jnp.cos(lam_im * time_step)
    decay_im = magnitude * jnp.sin(lam_im * time_step)
    modulus = lam_re * lam_re + lam_im * lam_im
    factor_re = ((decay_re - 1.0) * lam_re + decay_im * lam_im) / modulus
    factor_im = (decay_im * lam_re - (decay_re - 1.0) * lam_im) / modulus
    for g in range(32):
        q, j = divmod(g, 8)
        at = (q, pl.ds(16 * j, 16), pl.ds(64 * j, 64))
        f_re = factor_re[g : g + 1]
        f_im = factor_im[g : g + 1]
        b_re = b_real_ref[g]
        b_im = b_imag_ref[g]
        input_re[at] = (f_re * b_re - f_im * b_im).astype(BF16)
        input_im[at] = (f_re * b_im + f_im * b_re).astype(BF16)
        readout_re[at] = readout_real_ref[g].astype(BF16)
        readout_im[at] = readout_imag_ref[g].astype(BF16)
        lane = pl.ds(64 * g, 64)
        decay_rows[pl.ds(0, 1), lane] = decay_re[g : g + 1]
        decay_rows[pl.ds(1, 1), lane] = decay_im[g : g + 1]

    def rms_scale(values, gain):
        mean = jnp.mean(values * values, axis=1, keepdims=True)
        return (values * lax.rsqrt(mean + EPS) * gain).astype(BF16)

    loaded(7, 10)
    tokens = tokens_ref[...].astype(F32)
    drive = dot(rms_scale(tokens, norm_mix_ref[...]), w_drive_ref[...]).astype(BF16)
    loaded(10, 12)
    projected = []
    for q in range(4):
        channels = drive[:, 128 * q : 128 * q + 128]
        cols = pl.ds(512 * q, 512)
        old_re = state_ref[0, :, cols]
        old_im = state_ref[1, :, cols]
        d_re = decay_rows[pl.ds(0, 1), cols]
        d_im = decay_rows[pl.ds(1, 1), cols]
        new_re = d_re * old_re - d_im * old_im + dot(channels, input_re[q])
        new_im = d_re * old_im + d_im * old_re + dot(channels, input_im[q])
        state_out[0, :, cols] = new_re
        state_out[1, :, cols] = new_im
        projected.append(
            dot_nt(new_re.astype(BF16), readout_re[q]) - dot_nt(new_im.astype(BF16), readout_im[q])
        )
    skipped = d_skip_ref[...] * drive.astype(F32)
    readout = jax.nn.gelu(jnp.concatenate(projected, axis=1) + skipped).astype(BF16)
    loaded(12, 15)
    value_part = dot(readout, w_value_ref[...])
    gate_part = dot(readout, w_glugate_ref[...])
    mixed = (value_part * jax.nn.sigmoid(gate_part)).astype(BF16)
    resid = (tokens + dot(mixed, w_output_ref[...])).astype(BF16)
    resid_ref[...] = resid
    loaded(15, 20)
    normed = rms_scale(resid.astype(F32), norm_ffn_ref[...])

    own[:, pl.ds(0, 2048)] = normed
    ids = ids_ref[...].astype(F32)
    lanes = lax.broadcasted_iota(jnp.int32, (16, 128), 1)
    this = lax.broadcasted_iota(jnp.int32, (16, 16), 0)
    that = lax.broadcasted_iota(jnp.int32, (16, 16), 1)
    chosen = jnp.zeros((16, 128), F32)
    for t in range(6):
        column = jnp.sum(jnp.where(this == that, ids[t : t + 1], 0.0), axis=1, keepdims=True)
        chosen = chosen + jnp.where(column == lanes.astype(F32), 1.0, 0.0)
    earlier = jnp.where(that < this, 1.0, 0.0)
    ordinal = dot(earlier.astype(BF16), chosen.astype(BF16))
    own[:, pl.ds(2048, 128)] = (chosen * (1.0 + ordinal)).astype(BF16)
    branch = jax.nn.sigmoid(
        jnp.sum(normed.astype(F32) * vector_ref[...], axis=1, keepdims=True)
    )
    high = branch.astype(BF16).astype(F32)
    middle = (branch - high).astype(BF16).astype(F32)
    low = branch - high - middle
    extra = jnp.where(lanes == 0, high, jnp.where(lanes == 1, middle, jnp.where(lanes == 2, low, 0.0)))
    own[:, pl.ds(2176, 128)] = extra.astype(BF16)
    own_copy = pltpu.make_async_copy(
        own, x.at[pos["z"], pos["y"], pos["x"]], local_sem.at[6]
    )
    own_copy.start()

    pl.semaphore_wait(barrier, 7)
    for copy in swaps:
        copy.start()

    def view(ref, colour, offsets, cols):
        at = {}
        for d, o in zip(ORDERS[colour], offsets):
            at[d] = slice(None) if o is None else near[d][o % 4]
        return ref.at[at["z"], at["y"], at["x"], :, cols]

    def gather_copy(colour, kind, receiving=False):
        name, o, s = kind
        start, width = GATHER_COLS[colour]
        cols = pl.ds(start, width)
        order = ORDERS[colour]
        back = -s if receiving else 0
        if name == "m1":
            d, where = order[0], (back, 0, 0)
        elif name == "f1":
            d, where = order[0], (back - s, 0, 0)
            half = width // 2
            cols = pl.ds(start, half) if s == 1 else pl.ds(start + half, half)
        elif name == "m2":
            d, where = order[1], (o, back, 0)
        elif name == "f2":
            d, where = order[1], (o, back - s, 0)
        elif name == "m3a":
            d, where = order[2], (o, 0, back)
        elif name == "m3":
            d, where = order[2], (None, o, back)
        else:
            d, where = order[2], (None, o, back - s)
        target = view(x, colour, where, cols)
        source = target
        if name == "m1" or (name in ("m2", "m3a") and o == 0):
            source = own.at[:, cols]
            if receiving:
                source = target
        i = SLOT[kind]
        return pltpu.make_async_remote_copy(
            src_ref=source,
            dst_ref=target,
            send_sem=ag_send.at[colour, i],
            recv_sem=ag_recv.at[colour, i],
            device_id=(peers[d, s],),
            device_id_type=MESH,
        )

    started = []

    def send(colour, name, o, s):
        copy = gather_copy(colour, (name, o, s))
        copy.start()
        started.append(copy)

    def both(colour, name, o):
        send(colour, name, o, 1)
        send(colour, name, o, -1)

    def receive(colour, name, o, s):
        gather_copy(colour, (name, o, s), True).wait_recv()

    colours = range(3)
    for c in colours:
        both(c, "m1", 0)
    for c in colours:
        both(c, "m2", 0)
    for c in colours:
        both(c, "m3a", 0)
    own_copy.wait()
    for s in (1, -1):
        for c in colours:
            receive(c, "m1", 0, s)
            o = 3 if s == 1 else 1
            send(c, "f1", 0, s)
            both(c, "m2", o)
            both(c, "m3a", o)
    for c in colours:
        receive(c, "m2", 0, 1)
        send(c, "f2", 0, 1)
        receive(c, "m2", 0, -1)
    for c in colours:
        receive(c, "f1", 0, 1)
        receive(c, "f1", 0, -1)
        both(c, "m2", 2)
        both(c, "m3a", 2)
    for o in (3, 1):
        for c in colours:
            receive(c, "m2", o, 1)
            if o == 1:
                send(c, "f2", 1, 1)
            receive(c, "m2", o, -1)
            if o == 3:
                send(c, "f2", 3, -1)
    for c in colours:
        receive(c, "m2", 2, 1)
        receive(c, "m2", 2, -1)
        send(c, "f2", 2, -1)
        both(c, "m3", 3)
        both(c, "m3", 1)
    for c in colours:
        for o in (0, 1, 3, 2):
            receive(c, "m3a", o, 1)
        send(c, "f3", 0, 1)
        for o in (0, 1, 3, 2):
            receive(c, "m3a", o, -1)
    for c in colours:
        for o, s in ((0, 1), (1, 1), (3, -1), (2, -1)):
            receive(c, "f2", o, s)
        both(c, "m3", 2)
    for c in colours:
        receive(c, "m3", 3, 1)
        receive(c, "m3", 3, -1)
        send(c, "f3", 3, -1)
        receive(c, "m3", 1, 1)
        send(c, "f3", 1, 1)
        receive(c, "m3", 1, -1)
    for c in colours:
        receive(c, "m3", 2, 1)
        receive(c, "m3", 2, -1)
        send(c, "f3", 2, -1)
    for c in colours:
        for o, s in ((0, 1), (1, 1), (3, -1), (2, -1)):
            receive(c, "f3", o, s)

    for copy in local:
        copy.wait()
    for copy in swaps:
        copy.wait_recv()

    first = me - core

    @pl.loop(0, 4)
    def _(zi):
        block = x.at[zi]
        values = block[:, :, :, pl.ds(0, 2048)].reshape(256, 2048)
        products = dot_nt(values, w_in[...])
        gate_part = products[:, :128]
        up_part = products[:, 128:]
        extras = block[:, :, :, pl.ds(2176, 128)].reshape(256, 128)
        scale = dot(extras, jnp.ones((128, 128), BF16))
        hidden = (scale * jax.nn.silu(gate_part) * up_part).astype(BF16)
        hc[zi, :, :, :, pl.ds(0, 128)] = hidden.reshape(4, 4, 16, 128)
        table = block[:, :, :, pl.ds(2048, 128)].reshape(256, 128)
        slot = lax.broadcasted_iota(jnp.int32, (128, 256), 1)
        expert_of = jnp.where(
            lax.broadcasted_iota(jnp.int32, (128, 256), 0) == first + slot // 128, 1.0, 0.0
        ).astype(BF16)
        entry = dot(table, expert_of)
        row = lax.broadcasted_iota(jnp.int32, (256, 256), 0)
        lane = lax.broadcasted_iota(jnp.int32, (256, 256), 1)
        wanted = (lax.rem(lane // 64, 2) + 1).astype(F32)
        sender = lax.rem(lane, 64)
        hit = (entry == wanted) & (sender == zi * 16 + row // 16)
        hc[zi, :, :, :, pl.ds(128, 256)] = (
            jnp.where(hit, 1.0, 0.0).astype(BF16).reshape(4, 4, 16, 256)
        )
        slot_t = lax.broadcasted_iota(jnp.int32, (256, 128), 0)
        expert_t = jnp.where(
            lax.broadcasted_iota(jnp.int32, (256, 128), 1) == first + slot_t // 128, 1.0, 0.0
        ).astype(BF16)
        entry_t = dot_nt(expert_t, table)
        wanted_t = (lax.rem(row // 64, 2) + 1).astype(F32)
        hit_t = (entry_t == wanted_t) & (lax.rem(row, 64) == zi * 16 + lane // 16)
        ct[:, pl.ds(pl.multiple_of(zi * 256, 256), 256)] = jnp.where(hit_t, 1.0, 0.0).astype(BF16)

    pick = ct[...]

    @pl.loop(0, 4)
    def _(j):
        cols = pl.ds(pl.multiple_of(j * 512, 512), 512)
        picked[:, cols] = dot(pick, x[:, :, :, :, cols].reshape(1024, 512)).astype(BF16)

    choices = dot(pick, x[:, :, :, :, pl.ds(2048, 128)].reshape(1024, 128))

    for g in range(4):
        group_rows[pl.ds(32 * g, 32), :] = jnp.broadcast_to(
            group_ref[pl.ds(g, 1), :].astype(F32), (32, 2048)
        ).astype(BF16)
    selected = picked[...]
    group_exp = jnp.exp(dot_nt(selected, group_rows[...]))
    inner_exp = jnp.exp(dot(selected, router_ref[...]))
    lane = lax.broadcasted_iota(jnp.int32, (256, 128), 1)
    row = lax.broadcasted_iota(jnp.int32, (256, 128), 0)
    group_sum = jnp.sum(jnp.where(lax.rem(lane, 32) == 0, group_exp, 0.0), axis=1, keepdims=True)
    inner_sum = jnp.zeros((256, 128), F32)
    for g in range(4):
        inside = lane // 32 == g
        total = jnp.sum(jnp.where(inside, inner_exp, 0.0), axis=1, keepdims=True)
        inner_sum = jnp.where(inside, total, inner_sum)
    inner = inner_exp / inner_sum
    joint = (group_exp / group_sum) * inner
    mine = lane == first + row // 128
    numerator = jnp.sum(jnp.where(mine, joint, 0.0), axis=1, keepdims=True)
    taken = choices > 0.0
    denominator = jnp.sum(jnp.where(taken, inner, 0.0), axis=1, keepdims=True)
    live = jnp.sum(jnp.where(taken, 1.0, 0.0), axis=1, keepdims=True) > 0.0
    gates = jnp.where(live, numerator / jnp.where(live, denominator, 1.0), 0.0)

    for e in range(2):
        rows_in = selected[e * 128 : (e + 1) * 128]
        gate_part = dot(rows_in, eg[e])
        up_part = dot(rows_in, eu[e])
        hidden = (jax.nn.silu(gate_part) * up_part).astype(BF16)
        result = dot(hidden, ed[e])
        weighted = result * gates[e * 128 : (e + 1) * 128]
        w_out[pl.ds(128 + e * 128, 128), :] = weighted.astype(BF16)

    def scatter_copy(colour, kind, receiving=False):
        name, o, s = kind
        start, width = SCATTER_COLS[colour]
        cols = pl.ds(start, width)
        order = ORDERS[colour]
        half = width // 2
        k = 0 if s == 1 else 1
        if name == "m1":
            d, where = order[0], (-s, 0, 0)
            target = r1.at[colour, k, :, pl.ds(0, width)]
        elif name == "f1":
            d, where = order[0], (2, 0, 0)
            cols = pl.ds(start, half) if s == 1 else pl.ds(start + half, half)
            target = r1.at[colour, 2 + k, :, pl.ds(0, half)]
        elif name == "m2":
            d, where = order[1], (o, -s, 0)
            target = r2.at[colour, k, o, :, pl.ds(0, width)]
        elif name == "f2":
            d, where = order[1], (o, 2, 0)
            target = r2.at[colour, 2, o, :, pl.ds(0, width)]
        elif name == "m3":
            d, where = order[2], (None, o, -s)
            target = r3.at[colour, k, o, :, :, pl.ds(0, width)]
        else:
            d, where = order[2], (None, o, 2)
            target = r3.at[colour, 2, o, :, :, pl.ds(0, width)]
        i = SLOT[kind] if kind in SLOT else SLOT["m3a", o, s]
        return pltpu.make_async_remote_copy(
            src_ref=target if receiving else view(p, colour, where, cols),
            dst_ref=target,
            send_sem=rs_send.at[colour, i],
            recv_sem=rs_recv.at[colour, i],
            device_id=(peers[d, -s],),
            device_id_type=MESH,
        )

    def pass_on(colour, name, o, s):
        copy = scatter_copy(colour, (name, o, s))
        copy.start()
        started.append(copy)

    def arrive(colour, name, o, s):
        scatter_copy(colour, (name, o, s), True).wait_recv()

    def partial(colour, o):
        start, width = SCATTER_COLS[colour]
        d = ORDERS[colour][2]
        i = near[d][o]
        cols = pl.ds(start, width)
        if d == "z":
            left = hc[i]
        elif d == "y":
            left = hc[:, i]
        else:
            left = hc[:, :, i]
        values = dot(left.reshape(256, 384), w_out[:, cols]).astype(BF16).reshape(4, 4, 16, width)
        if d == "z":
            p[i, :, :, :, cols] = values
        elif d == "y":
            p[:, i, :, :, cols] = values
        else:
            p[:, :, i, :, cols] = values

    def block(colour, where, cols=None):
        start, width = SCATTER_COLS[colour]
        return view(p, colour, where, pl.ds(start, width) if cols is None else cols)

    def add(colour, where, *arrived, cols=None):
        ref = block(colour, where, cols)
        total = ref[...].astype(F32)
        for a in arrived:
            total = total + a[...].astype(F32)
        ref[...] = total.astype(BF16)

    def in3(c, k, o):
        return r3.at[c, k, o, :, :, pl.ds(0, SCATTER_COLS[c][1])]

    def in2(c, k, o):
        return r2.at[c, k, o, :, pl.ds(0, SCATTER_COLS[c][1])]

    backwards = (2, 3, 1, 0)

    def sign_of(o):
        return 1 if o in FORWARD_PLUS else -1

    for c in colours:
        partial(c, 2)
        for o in backwards:
            pass_on(c, "f3", o, sign_of(o))
    for s in (1, -1):
        for c in colours:
            partial(c, (-s) % 4)
            for o in backwards:
                if sign_of(o) != s:
                    pass_on(c, "m3", o, s)
    for c in colours:
        partial(c, 0)
    for o in backwards:
        for c in colours:
            s = sign_of(o)
            arrive(c, "f3", o, s)
            add(c, (None, o, -s), in3(c, 2, o))
            pass_on(c, "m3", o, s)
    for o in backwards:
        for c in colours:
            arrive(c, "m3", o, 1)
            arrive(c, "m3", o, -1)
            add(c, (None, o, 0), in3(c, 0, o), in3(c, 1, o))
            if o == 2:
                for q in backwards:
                    pass_on(c, "f2", q, sign_of(q))
            elif o in (1, 3):
                s = -1 if o == 1 else 1
                for q in backwards:
                    if sign_of(q) != s:
                        pass_on(c, "m2", q, s)
    for q in backwards:
        for c in colours:
            s = sign_of(q)
            arrive(c, "f2", q, s)
            add(c, (q, -s, 0), in2(c, 2, q))
            pass_on(c, "m2", q, s)
    for q in backwards:
        for c in colours:
            arrive(c, "m2", q, 1)
            arrive(c, "m2", q, -1)
            add(c, (q, 0, 0), in2(c, 0, q), in2(c, 1, q))
            if q == 2:
                pass_on(c, "f1", 0, 1)
                pass_on(c, "f1", 0, -1)
    for s in (1, -1):
        for c in colours:
            start, width = SCATTER_COLS[c]
            half = width // 2
            arrive(c, "f1", 0, s)
            cols = pl.ds(start, half) if s == 1 else pl.ds(start + half, half)
            add(c, (-s, 0, 0), r1.at[c, 2 if s == 1 else 3, :, pl.ds(0, half)], cols=cols)
            pass_on(c, "m1", 0, s)
    for c in colours:
        start, width = SCATTER_COLS[c]
        cols = pl.ds(start, width)
        arrive(c, "m1", 0, 1)
        arrive(c, "m1", 0, -1)
        total = resid_ref[:, cols].astype(F32) + block(c, (0, 0, 0))[...].astype(F32)
        for k in range(2):
            total = total + r1[c, k, :, pl.ds(0, width)].astype(F32)
        out_ref[:, cols] = total.astype(BF16)

    for copy in started:
        copy.wait_send()
    for copy in swaps:
        copy.wait_send()


def on_device(
    tokens,
    state,
    norm_mix,
    w_drive,
    lam_real,
    lam_imag,
    log_step,
    b_real,
    b_imag,
    readout_real,
    readout_imaginary,
    d_skip,
    w_value,
    w_glugate,
    w_output,
    norm_ffn,
    w_group,
    w_expert,
    route_ids,
    expert_gate,
    expert_up,
    expert_down,
    dense_vector,
    dense_gate,
    dense_up,
    dense_down,
):
    kinds = len(KINDS)
    vmem = pl.BlockSpec(memory_space=pltpu.VMEM)
    hbm = pl.BlockSpec(memory_space=pl.ANY)
    return pl.pallas_call(
        layer_kernel,
        out_shape=(
            jax.ShapeDtypeStruct((16, 2048), BF16),
            jax.ShapeDtypeStruct((2, 16, 2048), F32),
        ),
        in_specs=[hbm] * 26,
        out_specs=(vmem, vmem),
        scratch_shapes=[
            pltpu.VMEM((16, 2048), BF16),
            pltpu.VMEM((2, 16, 2048), F32),
            pltpu.VMEM((1, 2048), F32),
            pltpu.VMEM((2048, 512), BF16),
            pltpu.VMEM((32, 64), F32),
            pltpu.VMEM((32, 64), F32),
            pltpu.VMEM((1, 32), F32),
            pltpu.VMEM((32, 16, 64), F32),
            pltpu.VMEM((32, 16, 64), F32),
            pltpu.VMEM((32, 16, 64), F32),
            pltpu.VMEM((32, 16, 64), F32),
            pltpu.VMEM((1, 512), F32),
            pltpu.VMEM((512, 512), BF16),
            pltpu.VMEM((512, 512), BF16),
            pltpu.VMEM((512, 2048), BF16),
            pltpu.VMEM((1, 2048), F32),
            pltpu.VMEM((4, 2048), BF16),
            pltpu.VMEM((2048, 128), BF16),
            pltpu.VMEM((6, 16), jnp.int32),
            pltpu.VMEM((1, 2048), F32),
            pltpu.VMEM((4, 128, 512), BF16),
            pltpu.VMEM((4, 128, 512), BF16),
            pltpu.VMEM((4, 128, 512), BF16),
            pltpu.VMEM((4, 128, 512), BF16),
            pltpu.VMEM((2, 2048), F32),
            pltpu.VMEM((16, 2048), BF16),
            pltpu.VMEM((16, 2304), BF16),
            pltpu.VMEM((4, 4, 4, 16, 2304), BF16),
            pltpu.VMEM((256, 2048), BF16),
            pltpu.VMEM((384, 2048), BF16),
            pltpu.VMEM((2, 2048, 512), BF16),
            pltpu.VMEM((2, 2048, 512), BF16),
            pltpu.VMEM((2, 512, 2048), BF16),
            pltpu.VMEM((4, 4, 4, 16, 384), BF16),
            pltpu.VMEM((256, 1024), BF16),
            pltpu.VMEM((256, 2048), BF16),
            pltpu.VMEM((128, 2048), BF16),
            pltpu.VMEM((4, 4, 4, 16, 2048), BF16),
            pltpu.VMEM((3, 4, 16, 768), BF16),
            pltpu.VMEM((3, 3, 4, 16, 768), BF16),
            pltpu.VMEM((3, 3, 4, 4, 16, 768), BF16),
            pltpu.SemaphoreType.DMA((20,)),
            pltpu.SemaphoreType.DMA((7,)),
            pltpu.SemaphoreType.DMA((6,)),
            pltpu.SemaphoreType.DMA((6,)),
            pltpu.SemaphoreType.DMA((3, kinds)),
            pltpu.SemaphoreType.DMA((3, kinds)),
            pltpu.SemaphoreType.DMA((3, kinds)),
            pltpu.SemaphoreType.DMA((3, kinds)),
        ],
        compiler_params=pltpu.CompilerParams(
            collective_id=0, has_side_effects=True, vmem_limit_bytes=58 * 1024 * 1024
        ),
        cost_estimate=pl.CostEstimate(
            flops=8_000_000_000, bytes_accessed=20_000_000, transcendentals=0
        ),
    )(
        tokens,
        state,
        norm_mix.reshape(1, -1),
        w_drive,
        lam_real,
        lam_imag,
        log_step.reshape(1, -1),
        jnp.transpose(b_real, (0, 2, 1)),
        jnp.transpose(b_imag, (0, 2, 1)),
        readout_real,
        readout_imaginary,
        d_skip.reshape(1, -1),
        w_value,
        w_glugate,
        w_output,
        norm_ffn.reshape(1, -1),
        jnp.transpose(w_group),
        w_expert,
        jnp.transpose(route_ids),
        dense_vector.reshape(1, -1),
        jnp.transpose(dense_gate),
        jnp.transpose(dense_up),
        dense_down,
        expert_gate[0],
        expert_up[0],
        expert_down[0],
    )


def solution(mesh):
    placed = (
        P("ep", None),
        P(None, "ep", None),
        P(),
        P(),
        P(),
        P(),
        P(),
        P(),
        P(),
        P(),
        P(),
        P(),
        P(),
        P(),
        P(),
        P(),
        P(),
        P(),
        P("ep", None),
        P("ep", None, None),
        P("ep", None, None),
        P("ep", None, None),
        P(),
        P(None, "ep"),
        P(None, "ep"),
        P("ep", None),
    )
    return jax.shard_map(
        on_device,
        mesh=mesh,
        in_specs=placed,
        out_specs=(P("ep", None), P(None, "ep", None)),
        check_vma=False,
    )
```

```python
import heapq

import jax
import jax.numpy as jnp
from jax import lax
from jax.experimental import pallas as pl
from jax.experimental.pallas import tpu as pltpu
from jax.sharding import PartitionSpec as P

EPS = 1e-05
F32 = jnp.float32
BF16 = jnp.bfloat16
MESH = pl.DeviceIdType.MESH
ORDERS = (("x", "y", "z"), ("y", "z", "x"), ("z", "x", "y"))
COLS = ((0, 640), (640, 640), (1280, 768))
HALVES = (384, 384, 384)
RATE, DELAY, AHEAD, STEP = 46700.0, 2.0, 1.0, 0.36


def sign_of(offset):
    return 1 if offset in (0, 1) else -1


def messages():
    one = [("m1", s) for s in (1, -1)] + [("f1", s) for s in (1, -1)]
    two = [("m2", o, s) for o in range(4) for s in (1, -1)] + [("f2", o) for o in range(4)]
    pairs = [(o, q) for o in range(4) for q in range(4)]
    three = [("m3", o, q, s) for o, q in pairs for s in (1, -1)] + [("f3", o, q) for o, q in pairs]
    return one + two + three


SLOT = {m: i for i, m in enumerate(messages())}


def link_of(c, m):
    phase = int(m[0][1]) - 1
    s = m[-1] if m[0] in ("m1", "m2", "m3", "f1") else sign_of(m[-1])
    return ORDERS[c][phase], s


def bytes_of(c, m):
    width = COLS[c][1]
    if m[0] == "f1":
        width = HALVES[c] if m[1] == 1 else width - HALVES[c]
    return 32.0 * width


def simulate(first, react, rank):
    queue, waiting, free, count = [], {}, {}, 0
    sent, came, ready = {}, {}, {}

    def push(t, kind, item):
        nonlocal count
        count += 1
        heapq.heappush(queue, (t, count, kind, item))

    for t, items in first:
        for item in items:
            push(t, "ready", item)
    while queue:
        t, _, kind, item = heapq.heappop(queue)
        if kind == "ready":
            ready[item] = t
            count += 1
            heapq.heappush(waiting.setdefault(link_of(*item), []), (rank(item), count, item))
            links = [link_of(*item)]
        elif kind == "free":
            links = [item]
        else:
            came[item] = t
            links = []
            for new in react(item):
                push(t, "ready", new)
        for k in links:
            if free.get(k, 0.0) <= t + 1e-9 and waiting.get(k):
                _, _, m = heapq.heappop(waiting[k])
                free[k] = t + bytes_of(*m) / RATE
                sent[m] = t
                push(free[k], "free", k)
                push(free[k] + DELAY, "came", m)
    steps = [(t, 0, "receive", m) for m, t in came.items()]
    steps += [(max(ready[m], t - AHEAD), 1, "send", m) for m, t in sent.items()]
    return steps, sent


def plan_gather():
    halves = {}

    def present(c, o, q):
        new = [(c, ("m2", o, 1)), (c, ("m2", o, -1))] if q == 0 else []
        return new + [(c, ("m3", o, q, 1)), (c, ("m3", o, q, -1))]

    def react(item):
        c, m = item
        if m[0] == "m1":
            return [(c, ("f1", m[1]))] + present(c, 3 if m[1] == 1 else 1, 0)
        if m[0] == "f1":
            halves[c] = halves.get(c, 0) + 1
            return present(c, 2, 0) if halves[c] == 2 else []
        if m[0] == "m2":
            o, s = m[1:]
            new = [(c, ("f2", o))] if sign_of(o) == s else []
            return new + present(c, o, 3 if s == 1 else 1)
        if m[0] == "f2":
            return present(c, m[1], 2)
        if m[0] == "m3" and sign_of(m[2]) == m[3]:
            return [(c, ("f3", m[1], m[2]))]
        return []

    start = [(c, ("m1", s)) for c in range(3) for s in (1, -1)]
    for c in range(3):
        start += present(c, 0, 0)
    rank = {"m1": 0, "f1": 0, "m2": 1, "f2": 1, "m3": 2, "f3": 3}
    steps, sent = simulate([(0.0, start)], react, lambda item: rank[item[1][0]])
    return [(kind, *m) for _, _, kind, m in sorted(steps, key=lambda s: s[:2])], sent, steps


def plan_scatter(sent):
    seen = {}

    def react(item):
        c, m = item

        def both(key):
            seen[c, key] = seen.get((c, key), 0) + 1
            return seen[c, key] == 2

        def level2(o, q):
            if q == 2:
                return [(c, ("f2", o))]
            if q == 0:
                return level1(o)
            s = -1 if q == 1 else 1
            return [(c, ("m2", o, s))] if sign_of(o) != s or both(("m2", o, s)) else []

        def level1(o):
            seen[c, "sum", o] = seen.get((c, "sum", o), 0) + 1
            if seen[c, "sum", o] < 3:
                return []
            if o == 2:
                return [(c, ("f1", 1)), (c, ("f1", -1))]
            if o == 0:
                return []
            s = -1 if o == 1 else 1
            return [(c, ("m1", s))] if both(("m1", s)) else []

        if m[0] == "f3":
            s = sign_of(m[2])
            return [(c, ("m3", m[1], m[2], s))] if both(("m3",) + m[1:] + (s,)) else []
        if m[0] == "m3":
            return level2(m[1], m[2]) if both(("sum3",) + m[1:3]) else []
        if m[0] == "f2":
            s = sign_of(m[1])
            return [(c, ("m2", m[1], s))] if both(("m2", m[1], s)) else []
        if m[0] == "m2":
            return level1(m[1])
        if m[0] == "f1":
            return [(c, ("m1", m[1]))] if both(("m1", m[1])) else []
        return []

    first, products, t = [], [], 0.0
    pairs = [(o, q) for o in range(4) for q in range(4)]
    for k in (2, 3, 1, 0):
        for c in range(3):
            products.append((t, 0, "product", (c, k)))
            t += STEP
            if k == 2:
                first.append((t, [(c, ("f3", o, q)) for o, q in pairs]))
            elif k in (1, 3):
                s = -1 if k == 1 else 1
                free = [(c, ("m3", o, q, s)) for o, q in pairs if sign_of(q) != s]
                first.append((t, free))
                for o, q in pairs:
                    if sign_of(q) == s:
                        seen[c, ("m3", o, q, s)] = 1
    last = max(sent.values())
    steps, out = simulate(first, react, lambda item: last - sent[item])
    steps = steps + products
    return [(kind, *m) for _, _, kind, m in sorted(steps, key=lambda s: s[:2])], out, steps


def dot(a, b):
    return jnp.dot(a, b, preferred_element_type=F32)


def dot_nt(a, b):
    return lax.dot_general(a, b, (((1,), (1,)), ((), ())), preferred_element_type=F32)


def layer_kernel(
    tokens_hbm,
    state_hbm,
    norm_mix_hbm,
    w_drive_hbm,
    lam_real_hbm,
    lam_imag_hbm,
    log_step_hbm,
    b_real_hbm,
    b_imag_hbm,
    readout_real_hbm,
    readout_imag_hbm,
    d_skip_hbm,
    w_value_hbm,
    w_glugate_hbm,
    w_output_hbm,
    norm_ffn_hbm,
    group_hbm,
    router_hbm,
    ids_hbm,
    vector_hbm,
    gate_hbm,
    up_hbm,
    down_hbm,
    eg_hbm,
    eu_hbm,
    ed_hbm,
    out_ref,
    state_out,
    tokens_ref,
    state_ref,
    norm_mix_ref,
    w_drive_ref,
    lam_real_ref,
    lam_imag_ref,
    log_step_ref,
    b_real_ref,
    b_imag_ref,
    readout_real_ref,
    readout_imag_ref,
    d_skip_ref,
    w_value_ref,
    w_glugate_ref,
    w_output_ref,
    norm_ffn_ref,
    group_ref,
    router_ref,
    ids_ref,
    vector_ref,
    input_re,
    input_im,
    readout_re,
    readout_im,
    decay_rows,
    resid_ref,
    own,
    x,
    w_in,
    w_out,
    eg,
    eu,
    ed,
    ids_all,
    ids_own,
    sums,
    hc,
    picking,
    group_rows,
    p,
    r1,
    r2,
    r3,
    load_sem,
    local_sem,
    swap_send,
    swap_recv,
    id_send,
    id_recv,
    ag_send,
    ag_recv,
    rs_send,
    rs_recv,
):
    me = lax.axis_index("ep")
    core = lax.rem(me, 2)
    pos = {"x": lax.rem(me // 2, 4), "y": lax.rem(me // 8, 4), "z": me // 32}
    near = {d: [lax.rem(pos[d] + k, 4) for k in range(4)] for d in "xyz"}

    def device(at):
        return ((at["z"] * 4 + at["y"]) * 4 + at["x"]) * 2 + core

    def neighbour(d, s):
        at = dict(pos)
        at[d] = near[d][s % 4]
        return device(at)

    peers = {(d, s): neighbour(d, s) for d in "xyz" for s in (1, -1, 2)}
    partner = me + 1 - 2 * core

    barrier = pltpu.get_barrier_semaphore()
    for peer in [*peers.values(), partner]:
        pl.semaphore_signal(barrier, inc=1, device_id=(peer,), device_id_type=MESH)

    sources = (
        lam_real_hbm, lam_imag_hbm, log_step_hbm, b_real_hbm, b_imag_hbm, readout_real_hbm,
        readout_imag_hbm, tokens_hbm, norm_mix_hbm, w_drive_hbm, state_hbm, d_skip_hbm,
        w_value_hbm, w_glugate_hbm, w_output_hbm, norm_ffn_hbm, ids_hbm, vector_hbm, group_hbm,
        router_hbm,
    )
    targets = (
        lam_real_ref, lam_imag_ref, log_step_ref, b_real_ref, b_imag_ref, readout_real_ref,
        readout_imag_ref, tokens_ref, norm_mix_ref, w_drive_ref, state_ref, d_skip_ref,
        w_value_ref, w_glugate_ref, w_output_ref, norm_ffn_ref, ids_ref, vector_ref, group_ref,
        router_ref,
    )
    loads = [
        pltpu.make_async_copy(a, b, load_sem.at[i]) for i, (a, b) in enumerate(zip(sources, targets))
    ]
    for copy in loads:
        copy.start()

    def loaded(first, last):
        for copy in loads[first:last]:
            copy.wait()

    def rows(i):
        return pl.ds(pl.multiple_of(i * 64, 64), 64)

    weights = [
        (gate_hbm, w_in.at[rows(core)]),
        (up_hbm, w_in.at[rows(2 + core)]),
        (down_hbm, w_out.at[rows(core)]),
        (eg_hbm, eg.at[core]),
        (eu_hbm, eu.at[core]),
        (ed_hbm, ed.at[core]),
    ]
    local = [pltpu.make_async_copy(s, t, local_sem.at[i]) for i, (s, t) in enumerate(weights)]
    for copy in local:
        copy.start()
    pieces = list(weights[:3])
    for s, t in weights[3:]:
        depth = s.shape[0] // 4
        pieces += [(s.at[pl.ds(i * depth, depth)], t.at[pl.ds(i * depth, depth)]) for i in range(4)]
    swaps = [
        pltpu.make_async_remote_copy(
            src_ref=s,
            dst_ref=t,
            send_sem=swap_send.at[i],
            recv_sem=swap_recv.at[i],
            device_id=(partner,),
            device_id_type=MESH,
        )
        for i, (s, t) in enumerate(pieces)
    ]

    for ref in (input_re, input_im, readout_re, readout_im):
        ref[...] = jnp.zeros((4, 128, 512), BF16)
    loaded(0, 7)
    square = lax.broadcasted_iota(jnp.int32, (32, 32), 0) == lax.broadcasted_iota(
        jnp.int32, (32, 32), 1
    )
    time_step = jnp.sum(
        jnp.where(square, jnp.exp(log_step_ref[...]), 0.0), axis=1, keepdims=True
    )
    lam_re = lam_real_ref[...]
    lam_im = lam_imag_ref[...]
    magnitude = jnp.exp(lam_re * time_step)
    decay_re = magnitude * jnp.cos(lam_im * time_step)
    decay_im = magnitude * jnp.sin(lam_im * time_step)
    modulus = lam_re * lam_re + lam_im * lam_im
    factor_re = ((decay_re - 1.0) * lam_re + decay_im * lam_im) / modulus
    factor_im = (decay_im * lam_re - (decay_re - 1.0) * lam_im) / modulus
    for g in range(32):
        q, j = divmod(g, 8)
        at = (q, pl.ds(16 * j, 16), pl.ds(64 * j, 64))
        f_re = factor_re[g : g + 1]
        f_im = factor_im[g : g + 1]
        b_re = b_real_ref[g]
        b_im = b_imag_ref[g]
        input_re[at] = (f_re * b_re - f_im * b_im).astype(BF16)
        input_im[at] = (f_re * b_im + f_im * b_re).astype(BF16)
        readout_re[at] = readout_real_ref[g].astype(BF16)
        readout_im[at] = readout_imag_ref[g].astype(BF16)
        lane = pl.ds(64 * g, 64)
        decay_rows[pl.ds(0, 1), lane] = decay_re[g : g + 1]
        decay_rows[pl.ds(1, 1), lane] = decay_im[g : g + 1]

    pl.semaphore_wait(barrier, 10)
    for copy in swaps[:7]:
        copy.start()

    def rms_scale(values, gain):
        mean = jnp.mean(values * values, axis=1, keepdims=True)
        return (values * lax.rsqrt(mean + EPS) * gain).astype(BF16)

    loaded(7, 10)
    tokens = tokens_ref[...].astype(F32)
    drive = dot(rms_scale(tokens, norm_mix_ref[...]), w_drive_ref[...]).astype(BF16)
    loaded(10, 12)
    projected = []
    for q in range(4):
        channels = drive[:, 128 * q : 128 * q + 128]
        cols = pl.ds(512 * q, 512)
        old_re = state_ref[0, :, cols]
        old_im = state_ref[1, :, cols]
        d_re = decay_rows[pl.ds(0, 1), cols]
        d_im = decay_rows[pl.ds(1, 1), cols]
        new_re = d_re * old_re - d_im * old_im + dot(channels, input_re[q])
        new_im = d_re * old_im + d_im * old_re + dot(channels, input_im[q])
        state_out[0, :, cols] = new_re
        state_out[1, :, cols] = new_im
        projected.append(
            dot_nt(new_re.astype(BF16), readout_re[q]) - dot_nt(new_im.astype(BF16), readout_im[q])
        )
    skipped = d_skip_ref[...] * drive.astype(F32)
    readout = jax.nn.gelu(jnp.concatenate(projected, axis=1) + skipped).astype(BF16)
    loaded(12, 15)
    value_part = dot(readout, w_value_ref[...])
    gate_part = dot(readout, w_glugate_ref[...])
    mixed = (value_part * jax.nn.sigmoid(gate_part)).astype(BF16)
    resid = (tokens + dot(mixed, w_output_ref[...])).astype(BF16)
    resid_ref[...] = resid
    loaded(15, 20)
    normed = rms_scale(resid.astype(F32), norm_ffn_ref[...])

    own[...] = normed

    ids = ids_ref[...].astype(F32)
    lanes = lax.broadcasted_iota(jnp.int32, (16, 128), 1)
    down = lax.broadcasted_iota(jnp.int32, (16, 128), 0)
    this = lax.broadcasted_iota(jnp.int32, (16, 16), 0)
    that = lax.broadcasted_iota(jnp.int32, (16, 16), 1)
    columns = [
        jnp.sum(jnp.where(this == that, ids[t : t + 1], 0.0), axis=1, keepdims=True)
        for t in range(6)
    ]
    chosen = jnp.zeros((16, 128), F32)
    for column in columns:
        chosen = chosen + jnp.where(column == lanes.astype(F32), 1.0, 0.0)
    earlier = jnp.where(that < this, 1.0, 0.0)
    ordinal = dot(earlier.astype(BF16), chosen.astype(BF16))
    branch = jax.nn.sigmoid(
        jnp.sum(normed.astype(F32) * vector_ref[...], axis=1, keepdims=True)
    )
    words = jnp.where(lanes == 96 + down, branch, 0.0)
    for t, column in enumerate(columns):
        rank = jnp.sum(
            jnp.where(column == lanes.astype(F32), ordinal, 0.0), axis=1, keepdims=True
        )
        words = words + jnp.where(lanes == 16 * t + down, column + 128.0 * rank, 0.0)
    words = jnp.sum(words, axis=0, keepdims=True)
    ids_own[...] = words
    ids_all[pos["z"], pos["y"], pos["x"]] = words
    x[pos["z"], pos["y"], pos["x"]] = normed

    def view(ref, colour, offsets, cols):
        at = {}
        for d, o in zip(ORDERS[colour], offsets):
            at[d] = slice(None) if o is None else near[d][o % 4]
        return ref.at[at["z"], at["y"], at["x"], :, cols]

    def columns_of(colour, m):
        start, width = COLS[colour]
        if m[0] != "f1":
            return pl.ds(start, width)
        half = HALVES[colour]
        return pl.ds(start, half) if m[1] == 1 else pl.ds(start + half, width - half)

    def gather_copy(colour, m, receiving=False):
        d, s = link_of(colour, m)
        back = -s if receiving else 0
        where = {
            "m1": lambda: (back, 0, 0),
            "f1": lambda: (back - s, 0, 0),
            "m2": lambda: (m[1], back, 0),
            "f2": lambda: (m[1], back - s, 0),
            "m3": lambda: (m[1], m[2], back),
            "f3": lambda: (m[1], m[2], back - s),
        }[m[0]]()
        cols = columns_of(colour, m)
        target = view(x, colour, where, cols)
        source = own.at[:, cols] if where == (0, 0, 0) else target
        return pltpu.make_async_remote_copy(
            src_ref=source,
            dst_ref=target,
            send_sem=ag_send.at[colour, SLOT[m]],
            recv_sem=ag_recv.at[colour, SLOT[m]],
            device_id=(peers[d, s],),
            device_id_type=MESH,
        )

    started = []

    def id_copy(level, s, receiving=False):
        d = "xyz"[level]
        at = {"x": near["x"][0], "y": near["y"][0], "z": near["z"][0]}
        at[d] = near[d][-s % 4] if receiving else near[d][0]
        for axis in "xyz"[:level]:
            at[axis] = slice(None)
        target = ids_all.at[at["z"], at["y"], at["x"]]
        i = level * 3 + s % 4 - 1
        return pltpu.make_async_remote_copy(
            src_ref=ids_own if level == 0 and not receiving else target,
            dst_ref=target,
            send_sem=id_send.at[i],
            recv_sem=id_recv.at[i],
            device_id=(peers[d, s],),
            device_id_type=MESH,
        )

    def ids_send(level):
        for s in (1, -1, 2):
            copy = id_copy(level, s)
            copy.start()
            started.append(copy)

    def ids_receive(level):
        for s in (1, -1, 2):
            id_copy(level, s, True).wait_recv()

    first = me - core

    def slab_of(ref, d, k, cols):
        i = near[d][k]
        if d == "z":
            return ref[i, :, :, :, cols]
        if d == "y":
            return ref[:, i, :, :, cols]
        return ref[:, :, i, :, cols]

    def slab_store(ref, d, k, cols, values):
        i = near[d][k]
        values = values.reshape(4, 4, 16, values.shape[-1])
        if d == "z":
            ref[i, :, :, :, cols] = values
        elif d == "y":
            ref[:, i, :, :, cols] = values
        else:
            ref[:, :, i, :, cols] = values

    tables = {}

    def read_ids():
        table = ids_all[...].reshape(64, 128)
        lane = lax.broadcasted_iota(jnp.int32, (64, 128), 1)
        sender = lax.broadcasted_iota(jnp.int32, (64, 128), 0)
        found = []
        for e in range(2):
            for k in range(2):
                wanted = (first + e + 128 * k).astype(F32)
                hit = (table == wanted) & (lane < 96)
                row = jnp.where(hit, lax.rem(lane, 16) + 16 * sender, -1)
                found.append(jnp.max(row.astype(F32), axis=1, keepdims=True))
        code = jnp.concatenate(found, axis=0)
        tables["code"] = code
        wide = jnp.broadcast_to(code, (256, 256))
        diagonal = lax.broadcasted_iota(jnp.int32, (256, 256), 0) == lax.broadcasted_iota(
            jnp.int32, (256, 256), 1
        )
        across = jnp.sum(jnp.where(diagonal, wide, 0.0), axis=0, keepdims=True)
        tables["across"] = across

    def slots_by_rows(z):
        number = z * 256 + lax.broadcasted_iota(jnp.int32, (256, 256), 0)
        hot = jnp.where(number.astype(F32) == tables["across"], 1.0, 0.0).astype(BF16)
        hc[z, :, :, :, pl.ds(128, 256)] = hot.reshape(4, 4, 16, 256)

    def read_choices():
        code = tables["code"]
        table = ids_all[...].reshape(64, 128)
        lane = lax.broadcasted_iota(jnp.int32, (64, 128), 1)
        slot = lax.broadcasted_iota(jnp.int32, (256, 64), 0)
        same = lax.rem(slot, 64) == lax.broadcasted_iota(jnp.int32, (256, 64), 1)
        choices = dot(
            jnp.where(same, 1.0, 0.0).astype(BF16), jnp.where(lane < 96, table, 0.0).astype(BF16)
        )
        lane = lax.broadcasted_iota(jnp.int32, (256, 128), 1)
        within = code - 16.0 * lax.rem(
            lax.broadcasted_iota(jnp.int32, (256, 1), 0), 64
        ).astype(F32)
        taken = jnp.zeros((256, 128), F32)
        for t in range(6):
            word = jnp.sum(
                jnp.where(lane.astype(F32) == within + 16.0 * t, choices, 0.0), axis=1, keepdims=True
            )
            expert = jnp.where(word >= 128.0, word - 128.0, word)
            hit = (expert == lane.astype(F32)) & (code >= 0.0)
            taken = jnp.where(hit, 1.0, taken)
        tables["taken"] = taken

    def use_slab(colour, k):
        start, width = COLS[colour]
        cols = pl.ds(start, width)
        d = ORDERS[colour][2]
        values = slab_of(x, d, k, cols).reshape(256, width)
        every = pl.ds(0, 256)
        total = slab_of(sums, d, k, every).reshape(256, 256) + dot_nt(values, w_in[:, cols])
        slab_store(sums, d, k, every, total)
        lane = lax.broadcasted_iota(jnp.int32, (1, 256), 1)
        a, b, r = lane // 64, lax.rem(lane // 16, 4), lax.rem(lane, 16)
        i = near[d][k]
        if d == "z":
            sender = i * 16 + a * 4 + b
        elif d == "y":
            sender = a * 16 + i * 4 + b
        else:
            sender = a * 16 + b * 4 + i
        number = (sender * 16 + r).astype(F32)
        hot = jnp.where(tables["code"] == number, 1.0, 0.0).astype(BF16)
        rows = dot(hot, values)
        if k == 0:
            picking[:, cols] = rows
        else:
            picking[:, cols] += rows

    for g in range(4):
        group_rows[pl.ds(32 * g, 32), :] = jnp.broadcast_to(
            group_ref[pl.ds(g, 1), :].astype(F32), (32, 2048)
        ).astype(BF16)
    sums[...] = jnp.zeros((4, 4, 4, 16, 256), F32)

    gather_steps, gather_sent, _ = plan_gather()
    scatter_steps, _, _ = plan_scatter(gather_sent)
    ids_send(0)
    done = 0
    ready = []
    arrived = {}
    level = 0
    for action, c, m in gather_steps:
        if action == "send":
            copy = gather_copy(c, m)
            copy.start()
            started.append(copy)
            continue
        if done == 6:
            ids_receive(0)
            ids_send(1)
        if done == 44:
            ids_receive(1)
            ids_send(2)
        if done == 88:
            ids_receive(2)
            read_ids()
            for copy in local[:3]:
                copy.wait()
            for copy in swaps[:3]:
                copy.wait_recv()
        if done in (92, 96, 100, 104):
            slots_by_rows((done - 92) // 4)
        if done == 108:
            read_choices()
        if done >= 16 and done % 12 == 4 and 7 + done // 12 - 1 < len(swaps):
            swaps[7 + done // 12 - 1].start()
        gather_copy(c, m, True).wait_recv()
        done += 1
        k = {"f3": 2, "m3": (3 if m[-1] == 1 else 1)}.get(m[0], 0)
        arrived[c, k] = arrived.get((c, k), 1 if k == 0 else 0) + (0.5 if m[0] == "f1" else 1)
        if arrived[c, k] == 16:
            ready.append((c, k))
        if done >= 88:
            while ready:
                use_slab(*ready.pop(0))
    for copy in local[3:]:
        copy.wait()
    for copy in swaps[3:]:
        copy.wait_recv()


    @pl.loop(0, 4)
    def _(zi):
        products = sums[zi].reshape(256, 256)
        words = jnp.broadcast_to(ids_all[zi], (4, 4, 16, 128)).reshape(256, 128)
        lane = lax.broadcasted_iota(jnp.int32, (256, 128), 1)
        row = lax.broadcasted_iota(jnp.int32, (256, 128), 0)
        own_word = lane == 96 + lax.rem(row, 16)
        scale = jnp.sum(jnp.where(own_word, words, 0.0), axis=1, keepdims=True)
        hidden = (scale * jax.nn.silu(products[:, :128]) * products[:, 128:]).astype(BF16)
        hc[zi, :, :, :, pl.ds(0, 128)] = hidden.reshape(4, 4, 16, 128)

    selected = picking[...].astype(BF16)
    group_exp = jnp.exp(dot_nt(selected, group_rows[...]))
    inner_exp = jnp.exp(dot(selected, router_ref[...]))
    lane = lax.broadcasted_iota(jnp.int32, (256, 128), 1)
    row = lax.broadcasted_iota(jnp.int32, (256, 128), 0)
    group_sum = jnp.sum(jnp.where(lax.rem(lane, 32) == 0, group_exp, 0.0), axis=1, keepdims=True)
    inner_sum = jnp.zeros((256, 128), F32)
    for g in range(4):
        inside = lane // 32 == g
        total = jnp.sum(jnp.where(inside, inner_exp, 0.0), axis=1, keepdims=True)
        inner_sum = jnp.where(inside, total, inner_sum)
    inner = inner_exp / inner_sum
    joint = (group_exp / group_sum) * inner
    mine = lane == first + row // 128
    numerator = jnp.sum(jnp.where(mine, joint, 0.0), axis=1, keepdims=True)
    denominator = jnp.sum(tables["taken"] * inner, axis=1, keepdims=True)
    live = tables["code"] >= 0.0
    gates = jnp.where(live, numerator / jnp.where(live, denominator, 1.0), 0.0)

    for e in range(2):
        rows_in = selected[e * 128 : (e + 1) * 128]
        gate_part = dot(rows_in, eg[e])
        up_part = dot(rows_in, eu[e])
        hidden = (jax.nn.silu(gate_part) * up_part).astype(BF16)
        result = dot(hidden, ed[e])
        weighted = result * gates[e * 128 : (e + 1) * 128]
        w_out[pl.ds(128 + e * 128, 128), :] = weighted.astype(BF16)

    def landing(colour, m):
        width = COLS[colour][1]
        if m[0] == "m1":
            return r1.at[colour, 0 if m[1] == 1 else 1, :, pl.ds(0, width)]
        if m[0] == "f1":
            width = HALVES[colour] if m[1] == 1 else width - HALVES[colour]
            return r1.at[colour, 2 if m[1] == 1 else 3, :, pl.ds(0, width)]
        if m[0] == "m2":
            return r2.at[colour, 0 if m[2] == 1 else 1, m[1], :, pl.ds(0, width)]
        if m[0] == "f2":
            return r2.at[colour, 2, m[1], :, pl.ds(0, width)]
        if m[0] == "m3":
            return r3.at[colour, 0 if m[3] == 1 else 1, m[1], m[2], :, pl.ds(0, width)]
        return r3.at[colour, 2, m[1], m[2], :, pl.ds(0, width)]

    def scatter_copy(colour, m, receiving=False):
        d, s = link_of(colour, m)
        where = {
            "m1": lambda: (-s, 0, 0),
            "f1": lambda: (2, 0, 0),
            "m2": lambda: (m[1], -s, 0),
            "f2": lambda: (m[1], 2, 0),
            "m3": lambda: (m[1], m[2], -s),
            "f3": lambda: (m[1], m[2], 2),
        }[m[0]]()
        target = landing(colour, m)
        return pltpu.make_async_remote_copy(
            src_ref=target if receiving else view(p, colour, where, columns_of(colour, m)),
            dst_ref=target,
            send_sem=rs_send.at[colour, SLOT[m]],
            recv_sem=rs_recv.at[colour, SLOT[m]],
            device_id=(peers[d, -s],),
            device_id_type=MESH,
        )

    def product(colour, k):
        start, width = COLS[colour]
        cols = pl.ds(start, width)
        d = ORDERS[colour][2]
        left = slab_of(hc, d, k, pl.ds(0, 384)).reshape(256, 384)
        slab_store(p, d, k, cols, dot(left, w_out[:, cols]).astype(BF16))

    def add(colour, where, *messages, cols=None):
        start, width = COLS[colour]
        ref = view(p, colour, where, pl.ds(start, width) if cols is None else cols)
        total = ref[...].astype(F32)
        for m in messages:
            total = total + landing(colour, m)[...].astype(F32)
        ref[...] = total.astype(BF16)

    landed = set()
    done = 0
    for action, *what in scatter_steps:
        if action == "product":
            product(*what)
            continue
        c, m = what
        if action == "send":
            copy = scatter_copy(c, m)
            copy.start()
            started.append(copy)
            continue
        done += 1
        scatter_copy(c, m, True).wait_recv()
        landed.add((c, m))
        if m[0] == "f3":
            add(c, (m[1], m[2], -sign_of(m[2])), m)
        elif m[0] == "m3":
            other = ("m3", m[1], m[2], -m[3])
            if (c, other) in landed:
                add(c, (m[1], m[2], 0), m, other)
        elif m[0] == "f2":
            add(c, (m[1], -sign_of(m[1]), 0), m)
        elif m[0] == "m2":
            other = ("m2", m[1], -m[2])
            if (c, other) in landed:
                add(c, (m[1], 0, 0), m, other)
        elif m[0] == "f1":
            add(c, (-m[1], 0, 0), m, cols=columns_of(c, m))
    for c in range(3):
        start, width = COLS[c]
        cols = pl.ds(start, width)
        total = resid_ref[:, cols].astype(F32) + view(p, c, (0, 0, 0), cols)[...].astype(F32)
        for k in range(2):
            total = total + r1[c, k, :, pl.ds(0, width)].astype(F32)
        out_ref[:, cols] = total.astype(BF16)

    for copy in started:
        copy.wait_send()
    for copy in swaps:
        copy.wait_send()


def on_device(
    tokens,
    state,
    norm_mix,
    w_drive,
    lam_real,
    lam_imag,
    log_step,
    b_real,
    b_imag,
    readout_real,
    readout_imaginary,
    d_skip,
    w_value,
    w_glugate,
    w_output,
    norm_ffn,
    w_group,
    w_expert,
    route_ids,
    expert_gate,
    expert_up,
    expert_down,
    dense_vector,
    dense_gate,
    dense_up,
    dense_down,
):
    kinds = len(SLOT)
    vmem = pl.BlockSpec(memory_space=pltpu.VMEM)
    hbm = pl.BlockSpec(memory_space=pltpu.HBM)
    return pl.pallas_call(
        layer_kernel,
        out_shape=(
            jax.ShapeDtypeStruct((16, 2048), BF16),
            jax.ShapeDtypeStruct((2, 16, 2048), F32),
        ),
        in_specs=[hbm] * 26,
        out_specs=(vmem, vmem),
        scratch_shapes=[
            pltpu.VMEM((16, 2048), BF16),
            pltpu.VMEM((2, 16, 2048), F32),
            pltpu.VMEM((1, 2048), F32),
            pltpu.VMEM((2048, 512), BF16),
            pltpu.VMEM((32, 64), F32),
            pltpu.VMEM((32, 64), F32),
            pltpu.VMEM((1, 32), F32),
            pltpu.VMEM((32, 16, 64), F32),
            pltpu.VMEM((32, 16, 64), F32),
            pltpu.VMEM((32, 16, 64), F32),
            pltpu.VMEM((32, 16, 64), F32),
            pltpu.VMEM((1, 512), F32),
            pltpu.VMEM((512, 512), BF16),
            pltpu.VMEM((512, 512), BF16),
            pltpu.VMEM((512, 2048), BF16),
            pltpu.VMEM((1, 2048), F32),
            pltpu.VMEM((4, 2048), BF16),
            pltpu.VMEM((2048, 128), BF16),
            pltpu.VMEM((6, 16), jnp.int32),
            pltpu.VMEM((1, 2048), F32),
            pltpu.VMEM((4, 128, 512), BF16),
            pltpu.VMEM((4, 128, 512), BF16),
            pltpu.VMEM((4, 128, 512), BF16),
            pltpu.VMEM((4, 128, 512), BF16),
            pltpu.VMEM((2, 2048), F32),
            pltpu.VMEM((16, 2048), BF16),
            pltpu.VMEM((16, 2048), BF16),
            pltpu.VMEM((4, 4, 4, 16, 2048), BF16),
            pltpu.VMEM((256, 2048), BF16),
            pltpu.VMEM((384, 2048), BF16),
            pltpu.VMEM((2, 2048, 512), BF16),
            pltpu.VMEM((2, 2048, 512), BF16),
            pltpu.VMEM((2, 512, 2048), BF16),
            pltpu.VMEM((4, 4, 4, 1, 128), F32),
            pltpu.VMEM((1, 128), F32),
            pltpu.VMEM((4, 4, 4, 16, 256), F32),
            pltpu.VMEM((4, 4, 4, 16, 384), BF16),
            pltpu.VMEM((256, 2048), F32),
            pltpu.VMEM((128, 2048), BF16),
            pltpu.VMEM((4, 4, 4, 16, 2048), BF16),
            pltpu.VMEM((3, 4, 16, 768), BF16),
            pltpu.VMEM((3, 3, 4, 16, 768), BF16),
            pltpu.VMEM((3, 3, 4, 4, 16, 768), BF16),
            pltpu.SemaphoreType.DMA((20,)),
            pltpu.SemaphoreType.DMA((6,)),
            pltpu.SemaphoreType.DMA((15,)),
            pltpu.SemaphoreType.DMA((15,)),
            pltpu.SemaphoreType.DMA((9,)),
            pltpu.SemaphoreType.DMA((9,)),
            pltpu.SemaphoreType.DMA((3, kinds)),
            pltpu.SemaphoreType.DMA((3, kinds)),
            pltpu.SemaphoreType.DMA((3, kinds)),
            pltpu.SemaphoreType.DMA((3, kinds)),
        ],
        compiler_params=pltpu.CompilerParams(
            collective_id=0, has_side_effects=True, vmem_limit_bytes=47 * 1024 * 1024
        ),
        cost_estimate=pl.CostEstimate(
            flops=8_000_000_000, bytes_accessed=20_000_000, transcendentals=0
        ),
    )(*[pltpu.with_memory_space_constraint(a, pltpu.HBM) for a in (
        tokens,
        state,
        norm_mix.reshape(1, -1),
        w_drive,
        lam_real,
        lam_imag,
        log_step.reshape(1, -1),
        jnp.transpose(b_real, (0, 2, 1)),
        jnp.transpose(b_imag, (0, 2, 1)),
        readout_real,
        readout_imaginary,
        d_skip.reshape(1, -1),
        w_value,
        w_glugate,
        w_output,
        norm_ffn.reshape(1, -1),
        jnp.transpose(w_group),
        w_expert,
        jnp.transpose(route_ids),
        dense_vector.reshape(1, -1),
        jnp.transpose(dense_gate),
        jnp.transpose(dense_up),
        dense_down,
        expert_gate[0],
        expert_up[0],
        expert_down[0],
    )])


def solution(mesh):
    placed = (
        P("ep", None),
        P(None, "ep", None),
        P(),
        P(),
        P(),
        P(),
        P(),
        P(),
        P(),
        P(),
        P(),
        P(),
        P(),
        P(),
        P(),
        P(),
        P(),
        P(),
        P("ep", None),
        P("ep", None, None),
        P("ep", None, None),
        P("ep", None, None),
        P(),
        P(None, "ep"),
        P(None, "ep"),
        P("ep", None),
    )
    return jax.shard_map(
        on_device,
        mesh=mesh,
        in_specs=placed,
        out_specs=(P("ep", None), P(None, "ep", None)),
        check_vma=False,
    )
```

```python
import heapq

import jax
import jax.numpy as jnp
from jax import lax
from jax.experimental import pallas as pl
from jax.experimental.pallas import tpu as pltpu
from jax.sharding import PartitionSpec as P

EPS = 1e-05
F32 = jnp.float32
BF16 = jnp.bfloat16
MESH = pl.DeviceIdType.MESH
ORDERS = (("x", "y", "z"), ("y", "z", "x"), ("z", "x", "y"))
COLS = ((0, 640), (640, 640), (1280, 768))
RATE, DELAY, AHEAD, STEP = 46700.0, 2.0, 1.0, 0.36


def sign_of(offset):
    return 1 if offset in (0, 1) else -1


def link_of(c, m):
    phase = int(m[0][1]) - 1
    return ORDERS[c][phase], m[-1] if m[0] in ("m1", "m2", "m3") else sign_of(m[-1])


def bytes_of(c, m):
    return 32.0 * COLS[c][1] * (2 if m == ("m1", 2) else 1)


def queue_of(c, m):
    d, s = link_of(c, m)
    return d, 1 if s == 2 else s


def gather_group(m):
    if m[0] == "f3":
        return ("f3",), 16
    if m[0] == "m3" and sign_of(m[2]) != m[3]:
        return ("m3", m[3]), 8
    return m, 1


def scatter_group(m):
    if m[0] in ("m2", "m3"):
        return m[:-1], 2
    return (("m1",), 3) if m[0] == "m1" else (m, 1)


def grouped(steps, group):
    seen, out = {}, []
    for _, _, kind, what in sorted(steps, key=lambda step: step[:2]):
        if kind == "receive":
            name, size = group(what[1])
            key = (what[0], name)
            seen[key] = seen.get(key, 0) + 1
            if seen[key] < size:
                continue
            what = key
        out.append((kind, *what))
    return out


def simulate(first, react, rank):
    queue, waiting, free, count = [], {}, {}, 0
    sent, came, ready = {}, {}, {}

    def push(t, kind, item):
        nonlocal count
        count += 1
        heapq.heappush(queue, (t, count, kind, item))

    for t, items in first:
        for item in items:
            push(t, "ready", item)
    while queue:
        t, _, kind, item = heapq.heappop(queue)
        if kind == "ready":
            ready[item] = t
            count += 1
            heapq.heappush(waiting.setdefault(queue_of(*item), []), (rank(item), count, item))
            links = [queue_of(*item)]
        elif kind == "free":
            links = [item]
        else:
            came[item] = t
            links = []
            for new in react(item):
                push(t, "ready", new)
        for k in links:
            if free.get(k, 0.0) <= t + 1e-9 and waiting.get(k):
                _, _, m = heapq.heappop(waiting[k])
                free[k] = t + bytes_of(*m) / RATE
                sent[m] = t
                push(free[k], "free", k)
                push(free[k] + (DELAY + 0.8 if m[1] == ("m1", 2) else DELAY), "came", m)
    steps = [(t, 0, "receive", m) for m, t in came.items()]
    steps += [(max(ready[m], t - AHEAD), 1, "send", m) for m, t in sent.items()]
    return steps, sent


def plan_gather():
    def present(c, o, q):
        new = [(c, ("m2", o, 1)), (c, ("m2", o, -1))] if q == 0 else []
        return new + [(c, ("m3", o, q, 1)), (c, ("m3", o, q, -1))]

    def react(item):
        c, m = item
        if m[0] == "m1":
            return present(c, {1: 3, -1: 1, 2: 2}[m[1]], 0)
        if m[0] == "m2":
            o, s = m[1:]
            new = [(c, ("f2", o))] if sign_of(o) == s else []
            return new + present(c, o, 3 if s == 1 else 1)
        if m[0] == "f2":
            return present(c, m[1], 2)
        if m[0] == "m3" and sign_of(m[2]) == m[3]:
            return [(c, ("f3", m[1], m[2]))]
        return []

    start = [(c, ("m1", s)) for s in (1, -1, 2) for c in range(3)]
    for c in range(3):
        start += present(c, 0, 0)
    rank = {"m1": 0, "m2": 1, "f2": 1, "m3": 2, "f3": 3}
    steps, sent = simulate([(0.0, start)], react, lambda item: rank[item[1][0]])
    return grouped(steps, gather_group), sent


def plan_scatter(sent):
    seen = {}

    def react(item):
        c, m = item

        def both(key):
            seen[c, key] = seen.get((c, key), 0) + 1
            return seen[c, key] == 2

        def level2(o, q):
            if q == 2:
                return [(c, ("f2", o))]
            if q == 0:
                return level1(o)
            s = -1 if q == 1 else 1
            return [(c, ("m2", o, s))] if sign_of(o) != s or both(("m2", o, s)) else []

        def level1(o):
            seen[c, "sum", o] = seen.get((c, "sum", o), 0) + 1
            if seen[c, "sum", o] < 3:
                return []
            return [(c, ("m1", {1: -1, 2: 2, 3: 1}[o]))] if o else []

        if m[0] == "f3":
            s = sign_of(m[2])
            return [(c, ("m3", m[1], m[2], s))] if both(("m3",) + m[1:] + (s,)) else []
        if m[0] == "m3":
            return level2(m[1], m[2]) if both(("sum3",) + m[1:3]) else []
        if m[0] == "f2":
            s = sign_of(m[1])
            return [(c, ("m2", m[1], s))] if both(("m2", m[1], s)) else []
        if m[0] == "m2":
            return level1(m[1])
        return []

    first, products, t = [], [], 0.0
    pairs = [(o, q) for o in range(4) for q in range(4)]
    for k in (2, 3, 1, 0):
        for c in range(3):
            products.append((t, 0, "product", (c, k)))
            t += STEP
            if k == 2:
                first.append((t, [(c, ("f3", o, q)) for o, q in pairs]))
            elif k in (1, 3):
                s = -1 if k == 1 else 1
                free = [(c, ("m3", o, q, s)) for o, q in pairs if sign_of(q) != s]
                first.append((t, free))
                for o, q in pairs:
                    if sign_of(q) == s:
                        seen[c, ("m3", o, q, s)] = 1
    last = max(sent.values())
    steps, _ = simulate(first, react, lambda item: last - sent[item])
    return grouped(steps + products, scatter_group)


def numbered(group):
    one = [("m1", s) for s in (1, -1, 2)]
    two = [("m2", o, s) for o in range(4) for s in (1, -1)] + [("f2", o) for o in range(4)]
    pairs = [(o, q) for o in range(4) for q in range(4)]
    three = [("m3", o, q, s) for o, q in pairs for s in (1, -1)] + [("f3", o, q) for o, q in pairs]
    names = dict.fromkeys(group(m)[0] for m in one + two + three)
    return {name: i for i, name in enumerate(names)}


GATHER_SLOT = numbered(gather_group)
SCATTER_SLOT = numbered(scatter_group)


def dot(a, b):
    return jnp.dot(a, b, preferred_element_type=F32)


def dot_nt(a, b):
    return lax.dot_general(a, b, (((1,), (1,)), ((), ())), preferred_element_type=F32)


def layer_kernel(
    tokens_hbm,
    state_hbm,
    norm_mix_hbm,
    w_drive_hbm,
    lam_real_hbm,
    lam_imag_hbm,
    log_step_hbm,
    b_real_hbm,
    b_imag_hbm,
    readout_real_hbm,
    readout_imag_hbm,
    d_skip_hbm,
    w_value_hbm,
    w_glugate_hbm,
    w_output_hbm,
    norm_ffn_hbm,
    group_hbm,
    router_hbm,
    ids_hbm,
    vector_hbm,
    gate_hbm,
    up_hbm,
    down_hbm,
    eg_hbm,
    eu_hbm,
    ed_hbm,
    out_ref,
    state_out,
    tokens_ref,
    state_ref,
    norms_ref,
    w_drive_ref,
    lam_ref,
    log_step_ref,
    maps_ref,
    d_skip_ref,
    glu_ref,
    w_output_ref,
    group_ref,
    router_ref,
    ids_ref,
    input_re,
    input_im,
    readout_re,
    readout_im,
    decay_rows,
    resid_ref,
    own,
    x,
    w_in,
    w_out,
    eg,
    eu,
    ed,
    ids_all,
    ids_own,
    sums,
    hc,
    picking,
    group_rows,
    p,
    r1,
    r2,
    r3,
    load_sem,
    local_sem,
    swap_send,
    swap_recv,
    id_send,
    id_recv,
    ag_send,
    ag_recv,
    rs_send,
    rs_recv,
):
    me = lax.axis_index("ep")
    core = lax.rem(me, 2)
    pos = {"x": lax.rem(me // 2, 4), "y": lax.rem(me // 8, 4), "z": me // 32}
    near = {d: [lax.rem(pos[d] + k, 4) for k in range(4)] for d in "xyz"}

    def device(at):
        return ((at["z"] * 4 + at["y"]) * 4 + at["x"]) * 2 + core

    def neighbour(d, s):
        at = dict(pos)
        at[d] = near[d][s % 4]
        return device(at)

    peers = {(d, s): neighbour(d, s) for d in "xyz" for s in (1, -1, 2)}
    partner = me + 1 - 2 * core

    barrier = pltpu.get_barrier_semaphore()
    for peer in [*peers.values(), partner]:
        pl.semaphore_signal(barrier, inc=1, device_id=(peer,), device_id_type=MESH)

    def await_bytes(ref, semaphore):
        pltpu.make_async_copy(ref, ref, semaphore).wait()

    loads = (
        ((lam_real_hbm, lam_imag_hbm), lam_ref),
        ((log_step_hbm,), log_step_ref),
        ((b_real_hbm, b_imag_hbm, readout_real_hbm, readout_imag_hbm), maps_ref),
        ((tokens_hbm,), tokens_ref),
        ((norm_mix_hbm, norm_ffn_hbm, vector_hbm), norms_ref),
        ((w_drive_hbm,), w_drive_ref),
        ((state_hbm,), state_ref),
        ((d_skip_hbm,), d_skip_ref),
        ((w_value_hbm, w_glugate_hbm), glu_ref),
        ((w_output_hbm,), w_output_ref),
        ((ids_hbm,), ids_ref),
        ((group_hbm,), group_ref),
        ((router_hbm,), router_ref),
    )
    for i, (sources, target) in enumerate(loads):
        for j, source in enumerate(sources):
            part = target.at[j] if len(sources) > 1 else target
            pltpu.make_async_copy(source, part, load_sem.at[i]).start()

    def loaded(begin, end):
        for i in range(begin, end):
            await_bytes(loads[i][1], load_sem.at[i])

    def rows(i):
        return pl.ds(pl.multiple_of(i * 64, 64), 64)

    weights = [
        (gate_hbm, w_in.at[rows(core)]),
        (up_hbm, w_in.at[rows(2 + core)]),
        (down_hbm, w_out.at[rows(core)]),
        (eg_hbm, eg.at[core]),
        (eu_hbm, eu.at[core]),
        (ed_hbm, ed.at[core]),
    ]
    group = (0, 0, 0, 1, 2, 3)
    for i, (s, t) in zip(group, weights):
        pltpu.make_async_copy(s, t, local_sem.at[i]).start()
    pieces = [(0, *pair) for pair in weights[:3]]
    for j, (s, t) in enumerate(weights[3:]):
        depth = s.shape[0] // 4
        for i in range(4):
            part = pl.ds(i * depth, depth)
            pieces.append((1 + j, s.at[part], t.at[part]))
    swaps = [
        pltpu.make_async_remote_copy(
            src_ref=s,
            dst_ref=t,
            send_sem=swap_send.at[i],
            recv_sem=swap_recv.at[i],
            device_id=(partner,),
            device_id_type=MESH,
        )
        for i, s, t in pieces
    ]
    swapped = (w_out.at[pl.ds(0, 192)], eg.at[0], eu.at[0], ed.at[0])

    def weights_wait(i):
        await_bytes(swapped[i], local_sem.at[i])
        await_bytes(swapped[i], swap_recv.at[i])

    for ref in (input_re, input_im, readout_re, readout_im):
        ref[...] = jnp.zeros((4, 128, 512), BF16)
    loaded(0, 3)
    square = lax.broadcasted_iota(jnp.int32, (32, 32), 0) == lax.broadcasted_iota(
        jnp.int32, (32, 32), 1
    )
    time_step = jnp.sum(
        jnp.where(square, jnp.exp(log_step_ref[...]), 0.0), axis=1, keepdims=True
    )
    lam_re = lam_ref[0]
    lam_im = lam_ref[1]
    magnitude = jnp.exp(lam_re * time_step)
    decay_re = magnitude * jnp.cos(lam_im * time_step)
    decay_im = magnitude * jnp.sin(lam_im * time_step)
    modulus = lam_re * lam_re + lam_im * lam_im
    factor_re = ((decay_re - 1.0) * lam_re + decay_im * lam_im) / modulus
    factor_im = (decay_im * lam_re - (decay_re - 1.0) * lam_im) / modulus
    for g in range(32):
        q, j = divmod(g, 8)
        at = (q, pl.ds(16 * j, 16), pl.ds(64 * j, 64))
        f_re = factor_re[g : g + 1]
        f_im = factor_im[g : g + 1]
        b_re = maps_ref[0, g]
        b_im = maps_ref[1, g]
        input_re[at] = (f_re * b_re - f_im * b_im).astype(BF16)
        input_im[at] = (f_re * b_im + f_im * b_re).astype(BF16)
        readout_re[at] = maps_ref[2, g].astype(BF16)
        readout_im[at] = maps_ref[3, g].astype(BF16)
        lane = pl.ds(64 * g, 64)
        decay_rows[pl.ds(0, 1), lane] = decay_re[g : g + 1]
        decay_rows[pl.ds(1, 1), lane] = decay_im[g : g + 1]

    pl.semaphore_wait(barrier, 10)
    for copy in swaps[:7]:
        copy.start()

    def rms_scale(values, gain):
        mean = jnp.mean(values * values, axis=1, keepdims=True)
        return (values * lax.rsqrt(mean + EPS) * gain).astype(BF16)

    loaded(3, 6)
    tokens = tokens_ref[...].astype(F32)
    drive = dot(rms_scale(tokens, norms_ref[0]), w_drive_ref[...]).astype(BF16)
    loaded(6, 8)
    projected = []
    for q in range(4):
        channels = drive[:, 128 * q : 128 * q + 128]
        cols = pl.ds(512 * q, 512)
        old_re = state_ref[0, :, cols]
        old_im = state_ref[1, :, cols]
        d_re = decay_rows[pl.ds(0, 1), cols]
        d_im = decay_rows[pl.ds(1, 1), cols]
        new_re = d_re * old_re - d_im * old_im + dot(channels, input_re[q])
        new_im = d_re * old_im + d_im * old_re + dot(channels, input_im[q])
        state_out[0, :, cols] = new_re
        state_out[1, :, cols] = new_im
        projected.append(
            dot_nt(new_re.astype(BF16), readout_re[q]) - dot_nt(new_im.astype(BF16), readout_im[q])
        )
    skipped = d_skip_ref[...] * drive.astype(F32)
    readout = jax.nn.gelu(jnp.concatenate(projected, axis=1) + skipped).astype(BF16)
    loaded(8, 10)
    value_part = dot(readout, glu_ref[0])
    gate_part = dot(readout, glu_ref[1])
    mixed = (value_part * jax.nn.sigmoid(gate_part)).astype(BF16)
    resid = (tokens + dot(mixed, w_output_ref[...])).astype(BF16)
    resid_ref[...] = resid
    loaded(10, 13)
    normed = rms_scale(resid.astype(F32), norms_ref[1])

    own[...] = normed

    ids = ids_ref[...].astype(F32)
    lanes = lax.broadcasted_iota(jnp.int32, (16, 128), 1)
    down = lax.broadcasted_iota(jnp.int32, (16, 128), 0)
    this = lax.broadcasted_iota(jnp.int32, (16, 16), 0)
    that = lax.broadcasted_iota(jnp.int32, (16, 16), 1)
    columns = [
        jnp.sum(jnp.where(this == that, ids[t : t + 1], 0.0), axis=1, keepdims=True)
        for t in range(6)
    ]
    chosen = jnp.zeros((16, 128), F32)
    for column in columns:
        chosen = chosen + jnp.where(column == lanes.astype(F32), 1.0, 0.0)
    earlier = jnp.where(that < this, 1.0, 0.0)
    ordinal = dot(earlier.astype(BF16), chosen.astype(BF16))
    branch = jax.nn.sigmoid(
        jnp.sum(normed.astype(F32) * norms_ref[2], axis=1, keepdims=True)
    )
    words = jnp.where(lanes == 96 + down, branch, 0.0)
    for t, column in enumerate(columns):
        rank = jnp.sum(
            jnp.where(column == lanes.astype(F32), ordinal, 0.0), axis=1, keepdims=True
        )
        words = words + jnp.where(lanes == 16 * t + down, column + 128.0 * rank, 0.0)
    words = jnp.sum(words, axis=0, keepdims=True)
    ids_own[...] = words
    ids_all[pos["z"], pos["y"], pos["x"]] = words
    x[pos["z"], pos["y"], pos["x"]] = normed

    def view(ref, colour, offsets, cols):
        at = {}
        for d, o in zip(ORDERS[colour], offsets):
            at[d] = slice(None) if o is None else near[d][o % 4]
        return ref.at[at["z"], at["y"], at["x"], :, cols]

    def whole(colour):
        return pl.ds(*COLS[colour])

    def gather_copy(colour, m):
        d, s = link_of(colour, m)
        where = {
            "m1": lambda: (0, 0, 0),
            "m2": lambda: (m[1], 0, 0),
            "f2": lambda: (m[1], -s, 0),
            "m3": lambda: (m[1], m[2], 0),
            "f3": lambda: (m[1], m[2], -s),
        }[m[0]]()
        target = view(x, colour, where, whole(colour))
        return pltpu.make_async_remote_copy(
            src_ref=own.at[:, whole(colour)] if where == (0, 0, 0) else target,
            dst_ref=target,
            send_sem=ag_send.at[colour, int(m[0][1]) - 1],
            recv_sem=ag_recv.at[colour, GATHER_SLOT[gather_group(m)[0]]],
            device_id=(peers[d, s],),
            device_id_type=MESH,
        )

    def gather_wait(colour, name):
        size = {("f3",): 16}.get(name, 8 if len(name) == 2 and name[0] == "m3" else 1)
        cols = whole(colour)
        ref = {16: x.at[0, :, :, :, cols], 8: x.at[0, pl.ds(0, 2), :, :, cols]}.get(
            size, x.at[0, 0, 0, :, cols]
        )
        await_bytes(ref, ag_recv.at[colour, GATHER_SLOT[name]])
        return size

    def ids_send(level):
        at = dict(pos)
        for axis in "xyz"[:level]:
            at[axis] = slice(None)
        target = ids_all.at[at["z"], at["y"], at["x"]]
        for s in (1, -1, 2):
            pltpu.make_async_remote_copy(
                src_ref=target if level else ids_own,
                dst_ref=target,
                send_sem=id_send.at[level],
                recv_sem=id_recv.at[level],
                device_id=(peers["xyz"[level], s],),
                device_id_type=MESH,
            ).start()

    def three(level):
        three = pl.ds(0, 3)
        return (ids_all.at[0, 0, three], ids_all.at[0, three], ids_all.at[three])[level]

    def ids_receive(level):
        await_bytes(three(level), id_recv.at[level])

    first = me - core

    def slab_of(ref, d, k, cols):
        i = near[d][k]
        if d == "z":
            return ref[i, :, :, :, cols]
        if d == "y":
            return ref[:, i, :, :, cols]
        return ref[:, :, i, :, cols]

    def slab_store(ref, d, k, cols, values):
        i = near[d][k]
        values = values.reshape(4, 4, 16, values.shape[-1])
        if d == "z":
            ref[i, :, :, :, cols] = values
        elif d == "y":
            ref[:, i, :, :, cols] = values
        else:
            ref[:, :, i, :, cols] = values

    tables = {}

    def read_ids():
        table = ids_all[...].reshape(64, 128)
        lane = lax.broadcasted_iota(jnp.int32, (64, 128), 1)
        sender = lax.broadcasted_iota(jnp.int32, (64, 128), 0)
        found = []
        for e in range(2):
            for k in range(2):
                wanted = (first + e + 128 * k).astype(F32)
                hit = (table == wanted) & (lane < 96)
                row = jnp.where(hit, lax.rem(lane, 16) + 16 * sender, -1)
                found.append(jnp.max(row.astype(F32), axis=1, keepdims=True))
        code = jnp.concatenate(found, axis=0)
        tables["code"] = code
        wide = jnp.broadcast_to(code, (256, 256))
        diagonal = lax.broadcasted_iota(jnp.int32, (256, 256), 0) == lax.broadcasted_iota(
            jnp.int32, (256, 256), 1
        )
        across = jnp.sum(jnp.where(diagonal, wide, 0.0), axis=0, keepdims=True)
        tables["across"] = across

    def slots_by_rows(z):
        number = z * 256 + lax.broadcasted_iota(jnp.int32, (256, 256), 0)
        hot = jnp.where(number.astype(F32) == tables["across"], 1.0, 0.0).astype(BF16)
        hc[z, :, :, :, pl.ds(128, 256)] = hot.reshape(4, 4, 16, 256)

    def read_choices():
        code = tables["code"]
        table = ids_all[...].reshape(64, 128)
        lane = lax.broadcasted_iota(jnp.int32, (64, 128), 1)
        slot = lax.broadcasted_iota(jnp.int32, (256, 64), 0)
        same = lax.rem(slot, 64) == lax.broadcasted_iota(jnp.int32, (256, 64), 1)
        choices = dot(
            jnp.where(same, 1.0, 0.0).astype(BF16), jnp.where(lane < 96, table, 0.0).astype(BF16)
        )
        lane = lax.broadcasted_iota(jnp.int32, (256, 128), 1)
        within = code - 16.0 * lax.rem(
            lax.broadcasted_iota(jnp.int32, (256, 1), 0), 64
        ).astype(F32)
        taken = jnp.zeros((256, 128), F32)
        for t in range(6):
            word = jnp.sum(
                jnp.where(lane.astype(F32) == within + 16.0 * t, choices, 0.0), axis=1, keepdims=True
            )
            expert = jnp.where(word >= 128.0, word - 128.0, word)
            hit = (expert == lane.astype(F32)) & (code >= 0.0)
            taken = jnp.where(hit, 1.0, taken)
        tables["taken"] = taken

    def use_slab(colour, k):
        start, width = COLS[colour]
        cols = pl.ds(start, width)
        d = ORDERS[colour][2]
        values = slab_of(x, d, k, cols).reshape(256, width)
        every = pl.ds(0, 256)
        total = slab_of(sums, d, k, every).reshape(256, 256) + dot_nt(values, w_in[:, cols])
        slab_store(sums, d, k, every, total)
        lane = lax.broadcasted_iota(jnp.int32, (1, 256), 1)
        a, b, r = lane // 64, lax.rem(lane // 16, 4), lax.rem(lane, 16)
        i = near[d][k]
        if d == "z":
            sender = i * 16 + a * 4 + b
        elif d == "y":
            sender = a * 16 + i * 4 + b
        else:
            sender = a * 16 + b * 4 + i
        number = (sender * 16 + r).astype(F32)
        hot = jnp.where(tables["code"] == number, 1.0, 0.0).astype(BF16)
        rows = dot(hot, values)
        if k == 0:
            picking[:, cols] = rows
        else:
            picking[:, cols] += rows

    for g in range(4):
        group_rows[pl.ds(32 * g, 32), :] = jnp.broadcast_to(
            group_ref[pl.ds(g, 1), :].astype(F32), (32, 2048)
        ).astype(BF16)
    sums[...] = jnp.zeros((4, 4, 4, 16, 256), F32)

    experts_in = {}

    def use_columns(colour):
        start, width = COLS[colour]
        cols = pl.ds(start, width)
        rows = picking[:, cols].astype(BF16)
        parts = [dot_nt(rows, group_rows[:, cols]), dot(rows, router_ref[cols, :])]
        for e in range(2):
            mine = rows[e * 128 : (e + 1) * 128]
            parts += [dot(mine, eg[e, cols, :]), dot(mine, eu[e, cols, :])]
        for i, part in enumerate(parts):
            experts_in[i] = experts_in[i] + part if i in experts_in else part

    gather_steps, gather_sent = plan_gather()
    scatter_steps = plan_scatter(gather_sent)
    ids_send(0)
    done = 0
    ready = []
    arrived = {}
    tasks = [
        (6, lambda: (ids_receive(0), ids_send(1))),
        (40, lambda: (ids_receive(1), ids_send(2))),
        (84, lambda: (ids_receive(2), read_ids(), weights_wait(0))),
        (88, lambda: slots_by_rows(0)),
        (92, lambda: slots_by_rows(1)),
        (96, lambda: slots_by_rows(2)),
        (100, lambda: slots_by_rows(3)),
        (104, read_choices),
    ]
    more = swaps[7:]
    for action, c, m in gather_steps:
        if action == "send":
            gather_copy(c, m).start()
            continue
        while tasks and done >= tasks[0][0]:
            tasks.pop(0)[1]()
        if more and done >= 12 * (8 - len(more)):
            more.pop(0).start()
        size = gather_wait(c, m)
        done += size
        k = 2 if m[0] == "f3" else (3 if m[-1] == 1 else 1) if m[0] == "m3" else 0
        arrived[c, k] = arrived.get((c, k), 1 if k == 0 else 0) + size
        if arrived[c, k] == 16:
            ready.append((c, k))
        while ready and done >= 88:
            c, k = ready.pop(0)
            if k == 2 and not experts_in:
                weights_wait(1)
                weights_wait(2)
            use_slab(c, k)
            if k == 2:
                use_columns(c)
    weights_wait(3)


    @pl.loop(0, 4)
    def _(zi):
        products = sums[zi].reshape(256, 256)
        words = jnp.broadcast_to(ids_all[zi], (4, 4, 16, 128)).reshape(256, 128)
        lane = lax.broadcasted_iota(jnp.int32, (256, 128), 1)
        row = lax.broadcasted_iota(jnp.int32, (256, 128), 0)
        own_word = lane == 96 + lax.rem(row, 16)
        scale = jnp.sum(jnp.where(own_word, words, 0.0), axis=1, keepdims=True)
        hidden = (scale * jax.nn.silu(products[:, :128]) * products[:, 128:]).astype(BF16)
        hc[zi, :, :, :, pl.ds(0, 128)] = hidden.reshape(4, 4, 16, 128)

    group_exp = jnp.exp(experts_in[0])
    inner_exp = jnp.exp(experts_in[1])
    lane = lax.broadcasted_iota(jnp.int32, (256, 128), 1)
    row = lax.broadcasted_iota(jnp.int32, (256, 128), 0)
    group_sum = jnp.sum(jnp.where(lax.rem(lane, 32) == 0, group_exp, 0.0), axis=1, keepdims=True)
    inner_sum = jnp.zeros((256, 128), F32)
    for g in range(4):
        inside = lane // 32 == g
        total = jnp.sum(jnp.where(inside, inner_exp, 0.0), axis=1, keepdims=True)
        inner_sum = jnp.where(inside, total, inner_sum)
    inner = inner_exp / inner_sum
    joint = (group_exp / group_sum) * inner
    mine = lane == first + row // 128
    numerator = jnp.sum(jnp.where(mine, joint, 0.0), axis=1, keepdims=True)
    denominator = jnp.sum(tables["taken"] * inner, axis=1, keepdims=True)
    live = tables["code"] >= 0.0
    gates = jnp.where(live, numerator / jnp.where(live, denominator, 1.0), 0.0)

    for e in range(2):
        hidden = (jax.nn.silu(experts_in[2 + 2 * e]) * experts_in[3 + 2 * e]).astype(BF16)
        result = dot(hidden, ed[e])
        weighted = result * gates[e * 128 : (e + 1) * 128]
        w_out[pl.ds(128 + e * 128, 128), :] = weighted.astype(BF16)

    def landing(colour, m):
        cols = pl.ds(0, COLS[colour][1])
        i = {1: 0, -1: 1, 2: 2}
        if m[0] == "m1":
            return r1.at[colour, i[m[1]], :, cols]
        if m[0] == "m2":
            return r2.at[colour, i[m[2]], m[1], :, cols]
        if m[0] == "f2":
            return r2.at[colour, 2, m[1], :, cols]
        if m[0] == "m3":
            return r3.at[colour, i[m[3]], m[1], m[2], :, cols]
        return r3.at[colour, 2, m[1], m[2], :, cols]

    def scatter_copy(colour, m):
        d, s = link_of(colour, m)
        where = {
            "m1": lambda: (-s, 0, 0),
            "m2": lambda: (m[1], -s, 0),
            "f2": lambda: (m[1], 2, 0),
            "m3": lambda: (m[1], m[2], -s),
            "f3": lambda: (m[1], m[2], 2),
        }[m[0]]()
        return pltpu.make_async_remote_copy(
            src_ref=view(p, colour, where, whole(colour)),
            dst_ref=landing(colour, m),
            send_sem=rs_send.at[colour, int(m[0][1]) - 1],
            recv_sem=rs_recv.at[colour, SCATTER_SLOT[scatter_group(m)[0]]],
            device_id=(peers[d, s if s == 2 else -s],),
            device_id_type=MESH,
        )

    def scatter_wait(colour, name):
        cols = pl.ds(0, COLS[colour][1])
        two = pl.ds(0, 2)
        if name[0] == "m1":
            ref = r1.at[colour, :, :, cols]
        elif name[0] == "m2":
            ref = r2.at[colour, two, name[1], :, cols]
        elif name[0] == "m3":
            ref = r3.at[colour, two, name[1], name[2], :, cols]
        else:
            ref = landing(colour, name)
        await_bytes(ref, rs_recv.at[colour, SCATTER_SLOT[name]])

    def product(colour, k):
        start, width = COLS[colour]
        cols = pl.ds(start, width)
        d = ORDERS[colour][2]
        left = slab_of(hc, d, k, pl.ds(0, 384)).reshape(256, 384)
        slab_store(p, d, k, cols, dot(left, w_out[:, cols]).astype(BF16))

    def add(colour, where, *messages):
        ref = view(p, colour, where, whole(colour))
        total = ref[...].astype(F32)
        for m in messages:
            total = total + landing(colour, m)[...].astype(F32)
        ref[...] = total.astype(BF16)

    done = 0
    for action, *what in scatter_steps:
        if action == "product":
            product(*what)
            continue
        c, m = what
        if action == "send":
            scatter_copy(c, m).start()
            continue
        done += 1
        scatter_wait(c, m)
        if m[0] == "f3":
            add(c, (m[1], m[2], -sign_of(m[2])), m)
        elif m[0] == "f2":
            add(c, (m[1], -sign_of(m[1]), 0), m)
        elif m[0] == "m3":
            add(c, (m[1], m[2], 0), (*m, 1), (*m, -1))
        elif m[0] == "m2":
            add(c, (m[1], 0, 0), (*m, 1), (*m, -1))
    for c in range(3):
        start, width = COLS[c]
        cols = pl.ds(start, width)
        total = resid_ref[:, cols].astype(F32) + view(p, c, (0, 0, 0), cols)[...].astype(F32)
        for k in range(3):
            total = total + r1[c, k, :, pl.ds(0, width)].astype(F32)
        out_ref[:, cols] = total.astype(BF16)

    for level in range(3):
        await_bytes(three(level), id_send.at[level])
    for i in range(4):
        await_bytes(swapped[i], swap_send.at[i])
    for c in range(3):
        cols = whole(c)
        three_blocks = pl.ds(0, 3)
        sent = (
            x.at[0, 0, three_blocks, :, cols],
            x.at[0, three_blocks, :, :, cols],
            x.at[three_blocks, :, :, :, cols],
        )
        for i in range(3):
            await_bytes(sent[i], ag_send.at[c, i])
            await_bytes(sent[i], rs_send.at[c, i])


def on_device(
    tokens,
    state,
    norm_mix,
    w_drive,
    lam_real,
    lam_imag,
    log_step,
    b_real,
    b_imag,
    readout_real,
    readout_imaginary,
    d_skip,
    w_value,
    w_glugate,
    w_output,
    norm_ffn,
    w_group,
    w_expert,
    route_ids,
    expert_gate,
    expert_up,
    expert_down,
    dense_vector,
    dense_gate,
    dense_up,
    dense_down,
):
    vmem = pl.BlockSpec(memory_space=pltpu.VMEM)
    hbm = pl.BlockSpec(memory_space=pltpu.HBM)
    return pl.pallas_call(
        layer_kernel,
        out_shape=(
            jax.ShapeDtypeStruct((16, 2048), BF16),
            jax.ShapeDtypeStruct((2, 16, 2048), F32),
        ),
        in_specs=[hbm] * 26,
        out_specs=(vmem, vmem),
        scratch_shapes=[
            pltpu.VMEM((16, 2048), BF16),
            pltpu.VMEM((2, 16, 2048), F32),
            pltpu.VMEM((3, 1, 2048), F32),
            pltpu.VMEM((2048, 512), BF16),
            pltpu.VMEM((2, 32, 64), F32),
            pltpu.VMEM((1, 32), F32),
            pltpu.VMEM((4, 32, 16, 64), F32),
            pltpu.VMEM((1, 512), F32),
            pltpu.VMEM((2, 512, 512), BF16),
            pltpu.VMEM((512, 2048), BF16),
            pltpu.VMEM((4, 2048), BF16),
            pltpu.VMEM((2048, 128), BF16),
            pltpu.VMEM((6, 16), jnp.int32),
            pltpu.VMEM((4, 128, 512), BF16),
            pltpu.VMEM((4, 128, 512), BF16),
            pltpu.VMEM((4, 128, 512), BF16),
            pltpu.VMEM((4, 128, 512), BF16),
            pltpu.VMEM((2, 2048), F32),
            pltpu.VMEM((16, 2048), BF16),
            pltpu.VMEM((16, 2048), BF16),
            pltpu.VMEM((4, 4, 4, 16, 2048), BF16),
            pltpu.VMEM((256, 2048), BF16),
            pltpu.VMEM((384, 2048), BF16),
            pltpu.VMEM((2, 2048, 512), BF16),
            pltpu.VMEM((2, 2048, 512), BF16),
            pltpu.VMEM((2, 512, 2048), BF16),
            pltpu.VMEM((4, 4, 4, 1, 128), F32),
            pltpu.VMEM((1, 128), F32),
            pltpu.VMEM((4, 4, 4, 16, 256), F32),
            pltpu.VMEM((4, 4, 4, 16, 384), BF16),
            pltpu.VMEM((256, 2048), F32),
            pltpu.VMEM((128, 2048), BF16),
            pltpu.VMEM((4, 4, 4, 16, 2048), BF16),
            pltpu.VMEM((3, 3, 16, 768), BF16),
            pltpu.VMEM((3, 3, 4, 16, 768), BF16),
            pltpu.VMEM((3, 3, 4, 4, 16, 768), BF16),
            pltpu.SemaphoreType.DMA((13,)),
            pltpu.SemaphoreType.DMA((4,)),
            pltpu.SemaphoreType.DMA((4,)),
            pltpu.SemaphoreType.DMA((4,)),
            pltpu.SemaphoreType.DMA((3,)),
            pltpu.SemaphoreType.DMA((3,)),
            pltpu.SemaphoreType.DMA((3, 3)),
            pltpu.SemaphoreType.DMA((3, len(GATHER_SLOT))),
            pltpu.SemaphoreType.DMA((3, 3)),
            pltpu.SemaphoreType.DMA((3, len(SCATTER_SLOT))),
        ],
        compiler_params=pltpu.CompilerParams(
            collective_id=0, has_side_effects=True, vmem_limit_bytes=47 * 1024 * 1024
        ),
        cost_estimate=pl.CostEstimate(
            flops=8_000_000_000, bytes_accessed=20_000_000, transcendentals=0
        ),
    )(*[pltpu.with_memory_space_constraint(a, pltpu.HBM) for a in (
        tokens,
        state,
        norm_mix.reshape(1, -1),
        w_drive,
        lam_real,
        lam_imag,
        log_step.reshape(1, -1),
        jnp.transpose(b_real, (0, 2, 1)),
        jnp.transpose(b_imag, (0, 2, 1)),
        readout_real,
        readout_imaginary,
        d_skip.reshape(1, -1),
        w_value,
        w_glugate,
        w_output,
        norm_ffn.reshape(1, -1),
        jnp.transpose(w_group),
        w_expert,
        jnp.transpose(route_ids),
        dense_vector.reshape(1, -1),
        jnp.transpose(dense_gate),
        jnp.transpose(dense_up),
        dense_down,
        expert_gate[0],
        expert_up[0],
        expert_down[0],
    )])


def solution(mesh):
    placed = (
        P("ep", None),
        P(None, "ep", None),
        P(),
        P(),
        P(),
        P(),
        P(),
        P(),
        P(),
        P(),
        P(),
        P(),
        P(),
        P(),
        P(),
        P(),
        P(),
        P(),
        P("ep", None),
        P("ep", None, None),
        P("ep", None, None),
        P("ep", None, None),
        P(),
        P(None, "ep"),
        P(None, "ep"),
        P("ep", None),
    )
    return jax.shard_map(
        on_device,
        mesh=mesh,
        in_specs=placed,
        out_specs=(P("ep", None), P(None, "ep", None)),
        check_vma=False,
    )
```

```python
import heapq

import jax
import jax.numpy as jnp
from jax import lax
from jax.experimental import pallas as pl
from jax.experimental.pallas import tpu as pltpu
from jax.sharding import PartitionSpec as P

EPS = 1e-05
F32 = jnp.float32
BF16 = jnp.bfloat16
MESH = pl.DeviceIdType.MESH
ORDERS = (("x", "y", "z"), ("y", "z", "x"), ("z", "x", "y"))
COLS = ((0, 640), (640, 640), (1280, 768))
RATE, DELAY, STEP = 46700.0, 2.9, 0.36
GATHER_AHEAD, SCATTER_AHEAD = (1.0, 0.3), (0.6, 0.3)
SLACK = 0.4


def sign_of(offset):
    return 1 if offset in (0, 1) else -1


def link_of(c, m):
    phase = int(m[0][1]) - 1
    return ORDERS[c][phase], m[-1] if m[0] in ("m1", "m2", "m3") else sign_of(m[-1])


def bytes_of(c, m):
    return 32.0 * COLS[c][1] * (2 if m == ("m1", 2) else 1)


def queue_of(c, m):
    d, s = link_of(c, m)
    return d, 1 if s == 2 else s


def gather_group(m):
    if m[0] == "f3":
        return ("f3",), 16
    if m[0] == "m3" and sign_of(m[2]) != m[3]:
        return ("m3", m[3]), 8
    return m, 1


def scatter_group(m):
    if m[0] in ("m2", "m3"):
        return m[:-1], 2
    return (("m1",), 3) if m[0] == "m1" else (m, 1)


def grouped(steps, group):
    seen, out = {}, []
    for _, _, kind, what in sorted(steps, key=lambda step: step[:2]):
        if kind == "receive":
            name, size = group(what[1])
            key = (what[0], name)
            seen[key] = seen.get(key, 0) + 1
            if seen[key] < size:
                continue
            what = key
        out.append((kind, *what))
    merged, place = [], {}
    since = 0
    for step in out:
        if not step[0].startswith("send"):
            since = len(merged)
        elif place.get(step[1:], -1) >= since:
            merged[place[step[1:]]] = ("send", *step[1:])
            continue
        else:
            place[step[1:]] = len(merged)
        merged.append(step)
    return merged


def simulate(first, react, rank, aheads):
    queue, waiting, free, count = [], {}, {}, 0
    sent, came, ready = {}, {}, {}

    def push(t, kind, item):
        nonlocal count
        count += 1
        heapq.heappush(queue, (t, count, kind, item))

    for t, items in first:
        for item in items:
            push(t, "ready", item)
    while queue:
        t, _, kind, item = heapq.heappop(queue)
        if kind == "ready":
            ready[item] = t
            count += 1
            heapq.heappush(waiting.setdefault(queue_of(*item), []), (rank(item), count, item))
            links = [queue_of(*item)]
        elif kind == "free":
            links = [item]
        else:
            came[item] = t
            links = []
            for new in react(item):
                push(t, "ready", new)
        for k in links:
            if free.get(k, 0.0) <= t + 1e-9 and waiting.get(k):
                _, _, m = heapq.heappop(waiting[k])
                free[k] = t + bytes_of(*m) / RATE
                sent[m] = t
                push(free[k], "free", k)
                push(free[k] + (DELAY + 0.8 if m[1] == ("m1", 2) else DELAY), "came", m)
    steps = [(t, 0, "receive", m) for m, t in came.items()]
    for core, ahead in enumerate(aheads):
        steps += [(max(ready[m], t - ahead), 1, "send%d" % core, m) for m, t in sent.items()]
    return steps, sent


def plan_gather():
    def present(c, o, q):
        new = [(c, ("m2", o, 1)), (c, ("m2", o, -1))] if q == 0 else []
        return new + [(c, ("m3", o, q, 1)), (c, ("m3", o, q, -1))]

    def react(item):
        c, m = item
        if m[0] == "m1":
            return present(c, {1: 3, -1: 1, 2: 2}[m[1]], 0)
        if m[0] == "m2":
            o, s = m[1:]
            new = [(c, ("f2", o))] if sign_of(o) == s else []
            return new + present(c, o, 3 if s == 1 else 1)
        if m[0] == "f2":
            return present(c, m[1], 2)
        if m[0] == "m3" and sign_of(m[2]) == m[3]:
            return [(c, ("f3", m[1], m[2]))]
        return []

    start = [(c, ("m1", s)) for s in (1, -1, 2) for c in range(3)]
    for c in range(3):
        start += present(c, 0, 0)
    rank = {"m1": 0, "m2": 1, "f2": 1, "m3": 2, "f3": 3}
    steps, sent = simulate([(0.0, start)], react, lambda item: rank[item[1][0]], GATHER_AHEAD)
    return with_tasks(grouped(steps, gather_group)), sent


def plan_scatter(sent):
    seen = {}

    def react(item):
        c, m = item

        def both(key):
            seen[c, key] = seen.get((c, key), 0) + 1
            return seen[c, key] == 2

        def level2(o, q):
            if q == 2:
                return [(c, ("f2", o))]
            if q == 0:
                return level1(o)
            s = -1 if q == 1 else 1
            return [(c, ("m2", o, s))] if sign_of(o) != s or both(("m2", o, s)) else []

        def level1(o):
            seen[c, "sum", o] = seen.get((c, "sum", o), 0) + 1
            if seen[c, "sum", o] < 3:
                return []
            return [(c, ("m1", {1: -1, 2: 2, 3: 1}[o]))] if o else []

        if m[0] == "f3":
            s = sign_of(m[2])
            return [(c, ("m3", m[1], m[2], s))] if both(("m3",) + m[1:] + (s,)) else []
        if m[0] == "m3":
            return level2(m[1], m[2]) if both(("sum3",) + m[1:3]) else []
        if m[0] == "f2":
            s = sign_of(m[1])
            return [(c, ("m2", m[1], s))] if both(("m2", m[1], s)) else []
        if m[0] == "m2":
            return level1(m[1])
        return []

    first, products, t = [], [], 0.0
    pairs = [(o, q) for o in range(4) for q in range(4)]
    for k in (2, 3, 1, 0):
        for c in range(3):
            products.append((t, 0, "product", (c, k)))
            t += STEP
            if k == 2:
                first.append((t, [(c, ("f3", o, q)) for o, q in pairs]))
            elif k in (1, 3):
                s = -1 if k == 1 else 1
                free = [(c, ("m3", o, q, s)) for o, q in pairs if sign_of(q) != s]
                first.append((t, free))
                for o, q in pairs:
                    if sign_of(q) == s:
                        seen[c, ("m3", o, q, s)] = 1
    last = max(sent.values())
    steps, _ = simulate(first, react, lambda item: last - sent[item], SCATTER_AHEAD)
    return grouped(steps + products, scatter_group)


def with_tasks(steps):
    free, came, out, waiting, arrived = {}, {}, [], [], {}
    t, done = 0.0, 0
    sends = sum(step[0] in ("send", "send0") for step in steps)
    held = [(("ids",), 0.5)] + [(("rows", z), 0.15) for z in range(4)] + [(("choices",), 0.4)]
    for step in steps:
        kind, c, m = step
        if kind != "receive":
            if kind != "send1":
                k = queue_of(c, m)
                free[k] = max(t, free.get(k, 0.0)) + bytes_of(c, m) / RATE
                key = (c, gather_group(m)[0])
                came[key] = max(came.get(key, 0.0), free[k] + DELAY)
                sends -= 1
            out.append(step)
            continue
        if done >= 84:
            waiting += held
            held = []
        while waiting and (sends == 0 or t + waiting[0][1] <= came[c, m] + SLACK):
            task, cost = waiting.pop(0)
            out.append(("task", task, None))
            t += cost
        t = max(t, came[c, m])
        out.append(step)
        size = gather_size(m)
        done += size
        k = 2 if m[0] == "f3" else (3 if m[-1] == 1 else 1) if m[0] == "m3" else 0
        arrived[c, k] = arrived.get((c, k), 1 if k == 0 else 0) + size
        if arrived[c, k] == 16:
            held += [(("hidden", c, k), 0.25), (("pick", c, k), 0.3)]
            if k == 2:
                held.append((("columns", c), 0.5))
    return out + [("task", task, None) for task, _ in waiting + held]


def gather_size(name):
    if name[0] == "f3":
        return 16
    return 8 if name[0] == "m3" and len(name) == 2 else 1


def numbered(group):
    one = [("m1", s) for s in (1, -1, 2)]
    two = [("m2", o, s) for o in range(4) for s in (1, -1)] + [("f2", o) for o in range(4)]
    pairs = [(o, q) for o in range(4) for q in range(4)]
    three = [("m3", o, q, s) for o, q in pairs for s in (1, -1)] + [("f3", o, q) for o, q in pairs]
    names = dict.fromkeys(group(m)[0] for m in one + two + three)
    return {name: i for i, name in enumerate(names)}


GATHER_SLOT = numbered(gather_group)
SCATTER_SLOT = numbered(scatter_group)


def dot(a, b):
    return jnp.dot(a, b, preferred_element_type=F32)


def dot_nt(a, b):
    return lax.dot_general(a, b, (((1,), (1,)), ((), ())), preferred_element_type=F32)


def layer_kernel(
    tokens_hbm,
    state_hbm,
    norm_mix_hbm,
    w_drive_hbm,
    lam_real_hbm,
    lam_imag_hbm,
    log_step_hbm,
    b_real_hbm,
    b_imag_hbm,
    readout_real_hbm,
    readout_imag_hbm,
    d_skip_hbm,
    w_value_hbm,
    w_glugate_hbm,
    w_output_hbm,
    norm_ffn_hbm,
    group_hbm,
    router_hbm,
    ids_hbm,
    vector_hbm,
    gate_hbm,
    up_hbm,
    down_hbm,
    eg_hbm,
    eu_hbm,
    ed_hbm,
    out_ref,
    state_out,
    tokens_ref,
    state_ref,
    norms_ref,
    w_drive_ref,
    lam_ref,
    log_step_ref,
    maps_ref,
    d_skip_ref,
    glu_ref,
    w_output_ref,
    group_ref,
    router_ref,
    ids_ref,
    input_re,
    input_im,
    readout_re,
    readout_im,
    decay_rows,
    resid_ref,
    own,
    x,
    w_in,
    w_out,
    eg,
    eu,
    ed,
    ids_all,
    ids_own,
    sums,
    hc,
    picking,
    group_rows,
    p,
    r1,
    r2,
    r3,
    load_sem,
    local_sem,
    swap_send,
    swap_recv,
    id_send,
    id_recv,
    ag_send,
    ag_recv,
    rs_send,
    rs_recv,
):
    me = lax.axis_index("ep")
    core = lax.rem(me, 2)
    pos = {"x": lax.rem(me // 2, 4), "y": lax.rem(me // 8, 4), "z": me // 32}
    near = {d: [lax.rem(pos[d] + k, 4) for k in range(4)] for d in "xyz"}

    def device(at):
        return ((at["z"] * 4 + at["y"]) * 4 + at["x"]) * 2 + core

    def neighbour(d, s):
        at = dict(pos)
        at[d] = near[d][s % 4]
        return device(at)

    peers = {(d, s): neighbour(d, s) for d in "xyz" for s in (1, -1, 2)}
    partner = me + 1 - 2 * core

    barrier = pltpu.get_barrier_semaphore()
    for peer in [*peers.values(), partner]:
        pl.semaphore_signal(barrier, inc=1, device_id=(peer,), device_id_type=MESH)

    def send(action, copy):
        if action == "send":
            copy.start()
            return

        @pl.when(core == int(action[-1]))
        def _():
            copy.start()

    def await_bytes(ref, semaphore):
        pltpu.make_async_copy(ref, ref, semaphore).wait()

    loads = (
        ((lam_real_hbm, lam_imag_hbm), lam_ref),
        ((log_step_hbm,), log_step_ref),
        ((b_real_hbm, b_imag_hbm, readout_real_hbm, readout_imag_hbm), maps_ref),
        ((tokens_hbm,), tokens_ref),
        ((norm_mix_hbm, norm_ffn_hbm, vector_hbm), norms_ref),
        ((w_drive_hbm,), w_drive_ref),
        ((state_hbm,), state_ref),
        ((d_skip_hbm,), d_skip_ref),
        ((w_value_hbm, w_glugate_hbm), glu_ref),
        ((w_output_hbm,), w_output_ref),
        ((ids_hbm,), ids_ref),
        ((group_hbm,), group_ref),
        ((router_hbm,), router_ref),
    )
    for i, (sources, target) in enumerate(loads):
        for j, source in enumerate(sources):
            part = target.at[j] if len(sources) > 1 else target
            pltpu.make_async_copy(source, part, load_sem.at[i]).start()

    def loaded(begin, end):
        for i in range(begin, end):
            await_bytes(loads[i][1], load_sem.at[i])

    def rows(i):
        return pl.ds(pl.multiple_of(i * 64, 64), 64)

    weights = [
        (gate_hbm, w_in.at[rows(core)]),
        (up_hbm, w_in.at[rows(2 + core)]),
        (down_hbm, w_out.at[rows(core)]),
        (eg_hbm, eg.at[core]),
        (eu_hbm, eu.at[core]),
        (ed_hbm, ed.at[core]),
    ]
    group = (0, 0, 0, 1, 2, 3)
    for i, (s, t) in zip(group, weights):
        pltpu.make_async_copy(s, t, local_sem.at[i]).start()
    pieces = [(0, *pair) for pair in weights[:3]]
    for j, (s, t) in enumerate(weights[3:]):
        depth = s.shape[0] // 4
        for i in range(4):
            part = pl.ds(i * depth, depth)
            pieces.append((1 + j, s.at[part], t.at[part]))
    swaps = [
        pltpu.make_async_remote_copy(
            src_ref=s,
            dst_ref=t,
            send_sem=swap_send.at[i],
            recv_sem=swap_recv.at[i],
            device_id=(partner,),
            device_id_type=MESH,
        )
        for i, s, t in pieces
    ]
    swapped = (w_out.at[pl.ds(0, 192)], eg.at[0], eu.at[0], ed.at[0])

    def weights_wait(i):
        await_bytes(swapped[i], local_sem.at[i])
        await_bytes(swapped[i], swap_recv.at[i])

    for ref in (input_re, input_im, readout_re, readout_im):
        ref[...] = jnp.zeros((4, 128, 512), BF16)
    loaded(0, 6)
    pl.semaphore_wait(barrier, 10)
    for copy in swaps[:7]:
        copy.start()
    square = lax.broadcasted_iota(jnp.int32, (32, 32), 0) == lax.broadcasted_iota(
        jnp.int32, (32, 32), 1
    )
    time_step = jnp.sum(
        jnp.where(square, jnp.exp(log_step_ref[...]), 0.0), axis=1, keepdims=True
    )
    lam_re = lam_ref[0]
    lam_im = lam_ref[1]
    magnitude = jnp.exp(lam_re * time_step)
    decay_re = magnitude * jnp.cos(lam_im * time_step)
    decay_im = magnitude * jnp.sin(lam_im * time_step)
    modulus = lam_re * lam_re + lam_im * lam_im
    factor_re = ((decay_re - 1.0) * lam_re + decay_im * lam_im) / modulus
    factor_im = (decay_im * lam_re - (decay_re - 1.0) * lam_im) / modulus
    for g in range(32):
        q, j = divmod(g, 8)
        at = (q, pl.ds(16 * j, 16), pl.ds(64 * j, 64))
        f_re = factor_re[g : g + 1]
        f_im = factor_im[g : g + 1]
        b_re = maps_ref[0, g]
        b_im = maps_ref[1, g]
        input_re[at] = (f_re * b_re - f_im * b_im).astype(BF16)
        input_im[at] = (f_re * b_im + f_im * b_re).astype(BF16)
        readout_re[at] = maps_ref[2, g].astype(BF16)
        readout_im[at] = maps_ref[3, g].astype(BF16)
        lane = pl.ds(64 * g, 64)
        decay_rows[pl.ds(0, 1), lane] = decay_re[g : g + 1]
        decay_rows[pl.ds(1, 1), lane] = decay_im[g : g + 1]

    def rms_scale(values, gain):
        mean = jnp.mean(values * values, axis=1, keepdims=True)
        return (values * lax.rsqrt(mean + EPS) * gain).astype(BF16)

    tokens = tokens_ref[...].astype(F32)
    drive = dot(rms_scale(tokens, norms_ref[0]), w_drive_ref[...]).astype(BF16)
    loaded(6, 8)
    projected = []
    for q in range(4):
        channels = drive[:, 128 * q : 128 * q + 128]
        cols = pl.ds(512 * q, 512)
        old_re = state_ref[0, :, cols]
        old_im = state_ref[1, :, cols]
        d_re = decay_rows[pl.ds(0, 1), cols]
        d_im = decay_rows[pl.ds(1, 1), cols]
        new_re = d_re * old_re - d_im * old_im + dot(channels, input_re[q])
        new_im = d_re * old_im + d_im * old_re + dot(channels, input_im[q])
        state_out[0, :, cols] = new_re
        state_out[1, :, cols] = new_im
        projected.append(
            dot_nt(new_re.astype(BF16), readout_re[q]) - dot_nt(new_im.astype(BF16), readout_im[q])
        )
    skipped = d_skip_ref[...] * drive.astype(F32)
    readout = jax.nn.gelu(jnp.concatenate(projected, axis=1) + skipped).astype(BF16)
    loaded(8, 10)
    value_part = dot(readout, glu_ref[0])
    gate_part = dot(readout, glu_ref[1])
    mixed = (value_part * jax.nn.sigmoid(gate_part)).astype(BF16)
    resid = (tokens + dot(mixed, w_output_ref[...])).astype(BF16)
    resid_ref[...] = resid
    loaded(10, 13)
    normed = rms_scale(resid.astype(F32), norms_ref[1])

    own[...] = normed

    ids = ids_ref[...].astype(F32)
    lanes = lax.broadcasted_iota(jnp.int32, (16, 128), 1)
    down = lax.broadcasted_iota(jnp.int32, (16, 128), 0)
    this = lax.broadcasted_iota(jnp.int32, (16, 16), 0)
    that = lax.broadcasted_iota(jnp.int32, (16, 16), 1)
    columns = [
        jnp.sum(jnp.where(this == that, ids[t : t + 1], 0.0), axis=1, keepdims=True)
        for t in range(6)
    ]
    chosen = jnp.zeros((16, 128), F32)
    for column in columns:
        chosen = chosen + jnp.where(column == lanes.astype(F32), 1.0, 0.0)
    earlier = jnp.where(that < this, 1.0, 0.0)
    ordinal = dot(earlier.astype(BF16), chosen.astype(BF16))
    branch = jax.nn.sigmoid(
        jnp.sum(normed.astype(F32) * norms_ref[2], axis=1, keepdims=True)
    )
    words = jnp.where(lanes == 96 + down, branch, 0.0)
    for t, column in enumerate(columns):
        rank = jnp.sum(
            jnp.where(column == lanes.astype(F32), ordinal, 0.0), axis=1, keepdims=True
        )
        words = words + jnp.where(lanes == 16 * t + down, column + 128.0 * rank, 0.0)
    words = jnp.sum(words, axis=0, keepdims=True)
    ids_own[...] = words
    ids_all[pos["z"], pos["y"], pos["x"]] = words
    x[pos["z"], pos["y"], pos["x"]] = normed

    def view(ref, colour, offsets, cols):
        at = {}
        for d, o in zip(ORDERS[colour], offsets):
            at[d] = slice(None) if o is None else near[d][o % 4]
        return ref.at[at["z"], at["y"], at["x"], :, cols]

    def whole(colour):
        return pl.ds(*COLS[colour])

    def gather_copy(colour, m):
        d, s = link_of(colour, m)
        where = {
            "m1": lambda: (0, 0, 0),
            "m2": lambda: (m[1], 0, 0),
            "f2": lambda: (m[1], -s, 0),
            "m3": lambda: (m[1], m[2], 0),
            "f3": lambda: (m[1], m[2], -s),
        }[m[0]]()
        target = view(x, colour, where, whole(colour))
        return pltpu.make_async_remote_copy(
            src_ref=own.at[:, whole(colour)] if where == (0, 0, 0) else target,
            dst_ref=target,
            send_sem=ag_send.at[colour, int(m[0][1]) - 1],
            recv_sem=ag_recv.at[colour, GATHER_SLOT[gather_group(m)[0]]],
            device_id=(peers[d, s],),
            device_id_type=MESH,
        )

    def gather_wait(colour, name):
        size = gather_size(name)
        cols = whole(colour)
        ref = {16: x.at[0, :, :, :, cols], 8: x.at[0, pl.ds(0, 2), :, :, cols]}.get(
            size, x.at[0, 0, 0, :, cols]
        )
        await_bytes(ref, ag_recv.at[colour, GATHER_SLOT[name]])
        return size

    def ids_send(level):
        at = dict(pos)
        for axis in "xyz"[:level]:
            at[axis] = slice(None)
        target = ids_all.at[at["z"], at["y"], at["x"]]
        for s in (1, -1, 2):
            pltpu.make_async_remote_copy(
                src_ref=target if level else ids_own,
                dst_ref=target,
                send_sem=id_send.at[level],
                recv_sem=id_recv.at[level],
                device_id=(peers["xyz"[level], s],),
                device_id_type=MESH,
            ).start()

    def three(level):
        three = pl.ds(0, 3)
        return (ids_all.at[0, 0, three], ids_all.at[0, three], ids_all.at[three])[level]

    def ids_receive(level):
        await_bytes(three(level), id_recv.at[level])

    first = me - core

    def slab_of(ref, d, k, cols):
        i = near[d][k]
        if d == "z":
            return ref[i, :, :, :, cols]
        if d == "y":
            return ref[:, i, :, :, cols]
        return ref[:, :, i, :, cols]

    def slab_store(ref, d, k, cols, values):
        i = near[d][k]
        values = values.reshape(4, 4, 16, values.shape[-1])
        if d == "z":
            ref[i, :, :, :, cols] = values
        elif d == "y":
            ref[:, i, :, :, cols] = values
        else:
            ref[:, :, i, :, cols] = values

    tables = {}

    def read_ids():
        table = ids_all[...].reshape(64, 128)
        lane = lax.broadcasted_iota(jnp.int32, (64, 128), 1)
        sender = lax.broadcasted_iota(jnp.int32, (64, 128), 0)
        found = []
        for e in range(2):
            for k in range(2):
                wanted = (first + e + 128 * k).astype(F32)
                hit = (table == wanted) & (lane < 96)
                row = jnp.where(hit, lax.rem(lane, 16) + 16 * sender, -1)
                found.append(jnp.max(row.astype(F32), axis=1, keepdims=True))
        code = jnp.concatenate(found, axis=0)
        tables["code"] = code
        wide = jnp.broadcast_to(code, (256, 256))
        diagonal = lax.broadcasted_iota(jnp.int32, (256, 256), 0) == lax.broadcasted_iota(
            jnp.int32, (256, 256), 1
        )
        across = jnp.sum(jnp.where(diagonal, wide, 0.0), axis=0, keepdims=True)
        tables["across"] = across

    def slots_by_rows(z):
        number = z * 256 + lax.broadcasted_iota(jnp.int32, (256, 256), 0)
        hot = jnp.where(number.astype(F32) == tables["across"], 1.0, 0.0).astype(BF16)
        hc[z, :, :, :, pl.ds(128, 256)] = hot.reshape(4, 4, 16, 256)

    def read_choices():
        code = tables["code"]
        table = ids_all[...].reshape(64, 128)
        lane = lax.broadcasted_iota(jnp.int32, (64, 128), 1)
        slot = lax.broadcasted_iota(jnp.int32, (256, 64), 0)
        same = lax.rem(slot, 64) == lax.broadcasted_iota(jnp.int32, (256, 64), 1)
        choices = dot(
            jnp.where(same, 1.0, 0.0).astype(BF16), jnp.where(lane < 96, table, 0.0).astype(BF16)
        )
        lane = lax.broadcasted_iota(jnp.int32, (256, 128), 1)
        within = code - 16.0 * lax.rem(
            lax.broadcasted_iota(jnp.int32, (256, 1), 0), 64
        ).astype(F32)
        taken = jnp.zeros((256, 128), F32)
        for t in range(6):
            word = jnp.sum(
                jnp.where(lane.astype(F32) == within + 16.0 * t, choices, 0.0), axis=1, keepdims=True
            )
            expert = jnp.where(word >= 128.0, word - 128.0, word)
            hit = (expert == lane.astype(F32)) & (code >= 0.0)
            taken = jnp.where(hit, 1.0, taken)
        tables["taken"] = taken

    def slab_rows(colour, k):
        return slab_of(x, ORDERS[colour][2], k, whole(colour)).reshape(256, COLS[colour][1])

    def use_hidden(colour, k):
        d = ORDERS[colour][2]
        every = pl.ds(0, 256)
        total = slab_of(sums, d, k, every).reshape(256, 256)
        total = total + dot_nt(slab_rows(colour, k), w_in[:, whole(colour)])
        slab_store(sums, d, k, every, total)

    def use_pick(colour, k):
        d = ORDERS[colour][2]
        cols = whole(colour)
        lane = lax.broadcasted_iota(jnp.int32, (1, 256), 1)
        a, b, r = lane // 64, lax.rem(lane // 16, 4), lax.rem(lane, 16)
        i = near[d][k]
        if d == "z":
            sender = i * 16 + a * 4 + b
        elif d == "y":
            sender = a * 16 + i * 4 + b
        else:
            sender = a * 16 + b * 4 + i
        number = (sender * 16 + r).astype(F32)
        hot = jnp.where(tables["code"] == number, 1.0, 0.0).astype(BF16)
        rows = dot(hot, slab_rows(colour, k))
        if k == 0:
            picking[:, cols] = rows
        else:
            picking[:, cols] += rows

    for g in range(4):
        group_rows[pl.ds(32 * g, 32), :] = jnp.broadcast_to(
            group_ref[pl.ds(g, 1), :].astype(F32), (32, 2048)
        ).astype(BF16)
    sums[...] = jnp.zeros((4, 4, 4, 16, 256), F32)

    experts_in = {}

    def use_columns(colour):
        start, width = COLS[colour]
        cols = pl.ds(start, width)
        rows = picking[:, cols].astype(BF16)
        parts = [dot_nt(rows, group_rows[:, cols]), dot(rows, router_ref[cols, :])]
        for e in range(2):
            mine = rows[e * 128 : (e + 1) * 128]
            parts += [dot(mine, eg[e, cols, :]), dot(mine, eu[e, cols, :])]
        for i, part in enumerate(parts):
            experts_in[i] = experts_in[i] + part if i in experts_in else part

    gather_steps, gather_sent = plan_gather()
    scatter_steps = plan_scatter(gather_sent)
    ids_send(0)
    done = 0
    tasks = [
        (6, lambda: (ids_receive(0), ids_send(1))),
        (40, lambda: (ids_receive(1), ids_send(2))),
    ]
    more = swaps[7:]
    for action, c, m in gather_steps:
        if action == "task":
            name, *what = c
            if name == "ids":
                ids_receive(2)
                read_ids()
                weights_wait(0)
            elif name == "rows":
                slots_by_rows(*what)
            elif name == "choices":
                read_choices()
            elif name == "hidden":
                use_hidden(*what)
            elif name == "pick":
                use_pick(*what)
            else:
                if not experts_in:
                    weights_wait(1)
                    weights_wait(2)
                use_columns(*what)
            continue
        if action != "receive":
            send(action, gather_copy(c, m))
            continue
        while tasks and done >= tasks[0][0]:
            tasks.pop(0)[1]()
        if more and done >= 12 * (8 - len(more)):
            more.pop(0).start()
        done += gather_wait(c, m)
    weights_wait(3)


    for zi in range(4):
        products = sums[zi].reshape(256, 256)
        words = jnp.broadcast_to(ids_all[zi], (4, 4, 16, 128)).reshape(256, 128)
        lane = lax.broadcasted_iota(jnp.int32, (256, 128), 1)
        row = lax.broadcasted_iota(jnp.int32, (256, 128), 0)
        own_word = lane == 96 + lax.rem(row, 16)
        scale = jnp.sum(jnp.where(own_word, words, 0.0), axis=1, keepdims=True)
        hidden = (scale * jax.nn.silu(products[:, :128]) * products[:, 128:]).astype(BF16)
        hc[zi, :, :, :, pl.ds(0, 128)] = hidden.reshape(4, 4, 16, 128)

    group_exp = jnp.exp(experts_in[0])
    inner_exp = jnp.exp(experts_in[1])
    lane = lax.broadcasted_iota(jnp.int32, (256, 128), 1)
    row = lax.broadcasted_iota(jnp.int32, (256, 128), 0)
    group_sum = jnp.sum(jnp.where(lax.rem(lane, 32) == 0, group_exp, 0.0), axis=1, keepdims=True)
    inner_sum = jnp.zeros((256, 128), F32)
    for g in range(4):
        inside = lane // 32 == g
        total = jnp.sum(jnp.where(inside, inner_exp, 0.0), axis=1, keepdims=True)
        inner_sum = jnp.where(inside, total, inner_sum)
    inner = inner_exp / inner_sum
    joint = (group_exp / group_sum) * inner
    mine = lane == first + row // 128
    numerator = jnp.sum(jnp.where(mine, joint, 0.0), axis=1, keepdims=True)
    denominator = jnp.sum(tables["taken"] * inner, axis=1, keepdims=True)
    live = tables["code"] >= 0.0
    gates = jnp.where(live, numerator / jnp.where(live, denominator, 1.0), 0.0)

    for e in range(2):
        hidden = (jax.nn.silu(experts_in[2 + 2 * e]) * experts_in[3 + 2 * e]).astype(BF16)
        result = dot(hidden, ed[e])
        weighted = result * gates[e * 128 : (e + 1) * 128]
        w_out[pl.ds(128 + e * 128, 128), :] = weighted.astype(BF16)

    def landing(colour, m):
        cols = pl.ds(0, COLS[colour][1])
        i = {1: 0, -1: 1, 2: 2}
        if m[0] == "m1":
            return r1.at[colour, i[m[1]], :, cols]
        if m[0] == "m2":
            return r2.at[colour, i[m[2]], m[1], :, cols]
        if m[0] == "f2":
            return r2.at[colour, 2, m[1], :, cols]
        if m[0] == "m3":
            return r3.at[colour, i[m[3]], m[1], m[2], :, cols]
        return r3.at[colour, 2, m[1], m[2], :, cols]

    def scatter_copy(colour, m):
        d, s = link_of(colour, m)
        where = {
            "m1": lambda: (-s, 0, 0),
            "m2": lambda: (m[1], -s, 0),
            "f2": lambda: (m[1], 2, 0),
            "m3": lambda: (m[1], m[2], -s),
            "f3": lambda: (m[1], m[2], 2),
        }[m[0]]()
        return pltpu.make_async_remote_copy(
            src_ref=view(p, colour, where, whole(colour)),
            dst_ref=landing(colour, m),
            send_sem=rs_send.at[colour, int(m[0][1]) - 1],
            recv_sem=rs_recv.at[colour, SCATTER_SLOT[scatter_group(m)[0]]],
            device_id=(peers[d, s if s == 2 else -s],),
            device_id_type=MESH,
        )

    def scatter_wait(colour, name):
        cols = pl.ds(0, COLS[colour][1])
        two = pl.ds(0, 2)
        if name[0] == "m1":
            ref = r1.at[colour, :, :, cols]
        elif name[0] == "m2":
            ref = r2.at[colour, two, name[1], :, cols]
        elif name[0] == "m3":
            ref = r3.at[colour, two, name[1], name[2], :, cols]
        else:
            ref = landing(colour, name)
        await_bytes(ref, rs_recv.at[colour, SCATTER_SLOT[name]])

    def product(colour, k):
        start, width = COLS[colour]
        cols = pl.ds(start, width)
        d = ORDERS[colour][2]
        left = slab_of(hc, d, k, pl.ds(0, 384)).reshape(256, 384)
        slab_store(p, d, k, cols, dot(left, w_out[:, cols]).astype(BF16))

    def add(colour, where, *messages):
        ref = view(p, colour, where, whole(colour))
        total = ref[...].astype(F32)
        for m in messages:
            total = total + landing(colour, m)[...].astype(F32)
        ref[...] = total.astype(BF16)

    done = 0
    for action, *what in scatter_steps:
        if action == "product":
            product(*what)
            continue
        c, m = what
        if action != "receive":
            send(action, scatter_copy(c, m))
            continue
        done += 1
        scatter_wait(c, m)
        if m[0] == "f3":
            add(c, (m[1], m[2], -sign_of(m[2])), m)
        elif m[0] == "f2":
            add(c, (m[1], -sign_of(m[1]), 0), m)
        elif m[0] == "m3":
            add(c, (m[1], m[2], 0), (*m, 1), (*m, -1))
        elif m[0] == "m2":
            add(c, (m[1], 0, 0), (*m, 1), (*m, -1))
    for c in range(3):
        start, width = COLS[c]
        cols = pl.ds(start, width)
        total = resid_ref[:, cols].astype(F32) + view(p, c, (0, 0, 0), cols)[...].astype(F32)
        for k in range(3):
            total = total + r1[c, k, :, pl.ds(0, width)].astype(F32)
        out_ref[:, cols] = total.astype(BF16)

    for level in range(3):
        await_bytes(three(level), id_send.at[level])
    for i in range(4):
        await_bytes(swapped[i], swap_send.at[i])
    for c in range(3):
        cols = whole(c)
        three_blocks = pl.ds(0, 3)
        sent = (
            x.at[0, 0, three_blocks, :, cols],
            x.at[0, three_blocks, :, :, cols],
            x.at[three_blocks, :, :, :, cols],
        )
        for i in range(3):
            await_bytes(sent[i], ag_send.at[c, i])
            await_bytes(sent[i], rs_send.at[c, i])


def finish_kernel(rows_ref, state_ref, rows_out, state_out, sem):
    copies = (
        pltpu.make_async_copy(rows_ref, rows_out, sem.at[0]),
        pltpu.make_async_copy(state_ref, state_out, sem.at[1]),
    )
    for copy in copies:
        copy.start()
    for copy in copies:
        copy.wait()


def finish(rows, state):
    return pl.pallas_call(
        finish_kernel,
        out_shape=(
            jax.ShapeDtypeStruct(rows.shape, rows.dtype),
            jax.ShapeDtypeStruct(state.shape, state.dtype),
        ),
        in_specs=[pl.BlockSpec(memory_space=pltpu.VMEM)] * 2,
        out_specs=[pl.BlockSpec(memory_space=pl.ANY)] * 2,
        scratch_shapes=[pltpu.SemaphoreType.DMA((2,))],
        compiler_params=pltpu.CompilerParams(vmem_limit_bytes=4 * 1024 * 1024),
    )(rows, state)


def on_device(
    tokens,
    state,
    norm_mix,
    w_drive,
    lam_real,
    lam_imag,
    log_step,
    b_real,
    b_imag,
    readout_real,
    readout_imaginary,
    d_skip,
    w_value,
    w_glugate,
    w_output,
    norm_ffn,
    w_group,
    w_expert,
    route_ids,
    expert_gate,
    expert_up,
    expert_down,
    dense_vector,
    dense_gate,
    dense_up,
    dense_down,
):
    vmem = pl.BlockSpec(memory_space=pltpu.VMEM)
    hbm = pl.BlockSpec(memory_space=pltpu.HBM)
    rows, new_state = pl.pallas_call(
        layer_kernel,
        out_shape=(
            jax.ShapeDtypeStruct((16, 2048), BF16),
            jax.ShapeDtypeStruct((2, 16, 2048), F32),
        ),
        in_specs=[hbm] * 26,
        out_specs=(vmem, vmem),
        scratch_shapes=[
            pltpu.VMEM((16, 2048), BF16),
            pltpu.VMEM((2, 16, 2048), F32),
            pltpu.VMEM((3, 1, 2048), F32),
            pltpu.VMEM((2048, 512), BF16),
            pltpu.VMEM((2, 32, 64), F32),
            pltpu.VMEM((1, 32), F32),
            pltpu.VMEM((4, 32, 16, 64), F32),
            pltpu.VMEM((1, 512), F32),
            pltpu.VMEM((2, 512, 512), BF16),
            pltpu.VMEM((512, 2048), BF16),
            pltpu.VMEM((4, 2048), BF16),
            pltpu.VMEM((2048, 128), BF16),
            pltpu.VMEM((6, 16), jnp.int32),
            pltpu.VMEM((4, 128, 512), BF16),
            pltpu.VMEM((4, 128, 512), BF16),
            pltpu.VMEM((4, 128, 512), BF16),
            pltpu.VMEM((4, 128, 512), BF16),
            pltpu.VMEM((2, 2048), F32),
            pltpu.VMEM((16, 2048), BF16),
            pltpu.VMEM((16, 2048), BF16),
            pltpu.VMEM((4, 4, 4, 16, 2048), BF16),
            pltpu.VMEM((256, 2048), BF16),
            pltpu.VMEM((384, 2048), BF16),
            pltpu.VMEM((2, 2048, 512), BF16),
            pltpu.VMEM((2, 2048, 512), BF16),
            pltpu.VMEM((2, 512, 2048), BF16),
            pltpu.VMEM((4, 4, 4, 1, 128), F32),
            pltpu.VMEM((1, 128), F32),
            pltpu.VMEM((4, 4, 4, 16, 256), F32),
            pltpu.VMEM((4, 4, 4, 16, 384), BF16),
            pltpu.VMEM((256, 2048), F32),
            pltpu.VMEM((128, 2048), BF16),
            pltpu.VMEM((4, 4, 4, 16, 2048), BF16),
            pltpu.VMEM((3, 3, 16, 768), BF16),
            pltpu.VMEM((3, 3, 4, 16, 768), BF16),
            pltpu.VMEM((3, 3, 4, 4, 16, 768), BF16),
            pltpu.SemaphoreType.DMA((13,)),
            pltpu.SemaphoreType.DMA((4,)),
            pltpu.SemaphoreType.DMA((4,)),
            pltpu.SemaphoreType.DMA((4,)),
            pltpu.SemaphoreType.DMA((3,)),
            pltpu.SemaphoreType.DMA((3,)),
            pltpu.SemaphoreType.DMA((3, 3)),
            pltpu.SemaphoreType.DMA((3, len(GATHER_SLOT))),
            pltpu.SemaphoreType.DMA((3, 3)),
            pltpu.SemaphoreType.DMA((3, len(SCATTER_SLOT))),
        ],
        compiler_params=pltpu.CompilerParams(
            collective_id=0, has_side_effects=True, vmem_limit_bytes=47 * 1024 * 1024
        ),
        cost_estimate=pl.CostEstimate(
            flops=8_000_000_000, bytes_accessed=20_000_000, transcendentals=0
        ),
    )(*[pltpu.with_memory_space_constraint(a, pltpu.HBM) for a in (
        tokens,
        state,
        norm_mix.reshape(1, -1),
        w_drive,
        lam_real,
        lam_imag,
        log_step.reshape(1, -1),
        jnp.transpose(b_real, (0, 2, 1)),
        jnp.transpose(b_imag, (0, 2, 1)),
        readout_real,
        readout_imaginary,
        d_skip.reshape(1, -1),
        w_value,
        w_glugate,
        w_output,
        norm_ffn.reshape(1, -1),
        jnp.transpose(w_group),
        w_expert,
        jnp.transpose(route_ids),
        dense_vector.reshape(1, -1),
        jnp.transpose(dense_gate),
        jnp.transpose(dense_up),
        dense_down,
        expert_gate[0],
        expert_up[0],
        expert_down[0],
    )])
    return finish(rows, new_state)


def solution(mesh):
    placed = (
        P("ep", None),
        P(None, "ep", None),
        P(),
        P(),
        P(),
        P(),
        P(),
        P(),
        P(),
        P(),
        P(),
        P(),
        P(),
        P(),
        P(),
        P(),
        P(),
        P(),
        P("ep", None),
        P("ep", None, None),
        P("ep", None, None),
        P("ep", None, None),
        P(),
        P(None, "ep"),
        P(None, "ep"),
        P("ep", None),
    )
    return jax.shard_map(
        on_device,
        mesh=mesh,
        in_specs=placed,
        out_specs=(P("ep", None), P(None, "ep", None)),
        check_vma=False,
    )
```

```python
import heapq

import jax
import jax.numpy as jnp
from jax import lax
from jax.experimental import pallas as pl
from jax.experimental.pallas import tpu as pltpu
from jax.sharding import PartitionSpec as P

EPS = 1e-05
F32 = jnp.float32
BF16 = jnp.bfloat16
MESH = pl.DeviceIdType.MESH
ORDERS = (("x", "y", "z"), ("y", "z", "x"), ("z", "x", "y"))
COLS = ((0, 640), (640, 640), (1280, 768))
RATE, DELAY, STEP = 46700.0, 2.9, 0.36
GATHER_AHEAD, SCATTER_AHEAD = (1.0, 0.3), (0.6, 0.3)
SLACK = 0.4


def sign_of(offset):
    return 1 if offset in (0, 1) else -1


def link_of(c, m):
    phase = int(m[0][1]) - 1
    return ORDERS[c][phase], m[-1] if m[0] in ("m1", "m2", "m3") else sign_of(m[-1])


def bytes_of(c, m):
    return 32.0 * COLS[c][1] * (2 if m == ("m1", 2) else 1)


def queue_of(c, m):
    d, s = link_of(c, m)
    return d, 1 if s == 2 else s


def gather_group(m):
    if m[0] == "f3":
        return ("f3",), 16
    if m[0] == "m3" and sign_of(m[2]) != m[3]:
        return ("m3", m[3]), 8
    return m, 1


def scatter_group(m):
    if m[0] in ("m2", "m3"):
        return m[:-1], 2
    return (("m1",), 3) if m[0] == "m1" else (m, 1)


def grouped(steps, group):
    seen, out = {}, []
    for _, _, kind, what in sorted(steps, key=lambda step: step[:2]):
        if kind == "receive":
            name, size = group(what[1])
            key = (what[0], name)
            seen[key] = seen.get(key, 0) + 1
            if seen[key] < size:
                continue
            what = key
        out.append((kind, *what))
    merged, place = [], {}
    since = 0
    for step in out:
        if not step[0].startswith("send"):
            since = len(merged)
        elif place.get(step[1:], -1) >= since:
            merged[place[step[1:]]] = ("send", *step[1:])
            continue
        else:
            place[step[1:]] = len(merged)
        merged.append(step)
    return merged


def simulate(first, react, rank, aheads):
    queue, waiting, free, count = [], {}, {}, 0
    sent, came, ready = {}, {}, {}

    def push(t, kind, item):
        nonlocal count
        count += 1
        heapq.heappush(queue, (t, count, kind, item))

    for t, items in first:
        for item in items:
            push(t, "ready", item)
    while queue:
        t, _, kind, item = heapq.heappop(queue)
        if kind == "ready":
            ready[item] = t
            count += 1
            heapq.heappush(waiting.setdefault(queue_of(*item), []), (rank(item), count, item))
            links = [queue_of(*item)]
        elif kind == "free":
            links = [item]
        else:
            came[item] = t
            links = []
            for new in react(item):
                push(t, "ready", new)
        for k in links:
            if free.get(k, 0.0) <= t + 1e-9 and waiting.get(k):
                _, _, m = heapq.heappop(waiting[k])
                free[k] = t + bytes_of(*m) / RATE
                sent[m] = t
                push(free[k], "free", k)
                push(free[k] + (DELAY + 0.8 if m[1] == ("m1", 2) else DELAY), "came", m)
    steps = [(t, 0, "receive", m) for m, t in came.items()]
    for core, ahead in enumerate(aheads):
        steps += [(max(ready[m], t - ahead), 1, "send%d" % core, m) for m, t in sent.items()]
    return steps, sent


def plan_gather():
    def present(c, o, q):
        new = [(c, ("m2", o, 1)), (c, ("m2", o, -1))] if q == 0 else []
        return new + [(c, ("m3", o, q, 1)), (c, ("m3", o, q, -1))]

    def react(item):
        c, m = item
        if m[0] == "m1":
            return present(c, {1: 3, -1: 1, 2: 2}[m[1]], 0)
        if m[0] == "m2":
            o, s = m[1:]
            new = [(c, ("f2", o))] if sign_of(o) == s else []
            return new + present(c, o, 3 if s == 1 else 1)
        if m[0] == "f2":
            return present(c, m[1], 2)
        if m[0] == "m3" and sign_of(m[2]) == m[3]:
            return [(c, ("f3", m[1], m[2]))]
        return []

    start = [(c, ("m1", s)) for s in (1, -1, 2) for c in range(3)]
    for c in range(3):
        start += present(c, 0, 0)
    rank = {"m1": 0, "m2": 1, "f2": 1, "m3": 2, "f3": 3}
    steps, sent = simulate([(0.0, start)], react, lambda item: rank[item[1][0]], GATHER_AHEAD)
    return with_tasks(grouped(steps, gather_group)), sent


def plan_scatter(sent):
    seen = {}

    def react(item):
        c, m = item

        def both(key):
            seen[c, key] = seen.get((c, key), 0) + 1
            return seen[c, key] == 2

        def level2(o, q):
            if q == 2:
                return [(c, ("f2", o))]
            if q == 0:
                return level1(o)
            s = -1 if q == 1 else 1
            return [(c, ("m2", o, s))] if sign_of(o) != s or both(("m2", o, s)) else []

        def level1(o):
            seen[c, "sum", o] = seen.get((c, "sum", o), 0) + 1
            if seen[c, "sum", o] < 3:
                return []
            return [(c, ("m1", {1: -1, 2: 2, 3: 1}[o]))] if o else []

        if m[0] == "f3":
            s = sign_of(m[2])
            return [(c, ("m3", m[1], m[2], s))] if both(("m3",) + m[1:] + (s,)) else []
        if m[0] == "m3":
            return level2(m[1], m[2]) if both(("sum3",) + m[1:3]) else []
        if m[0] == "f2":
            s = sign_of(m[1])
            return [(c, ("m2", m[1], s))] if both(("m2", m[1], s)) else []
        if m[0] == "m2":
            return level1(m[1])
        return []

    first, products, t = [], [], 0.0
    pairs = [(o, q) for o in range(4) for q in range(4)]
    for k in (2, 3, 1, 0):
        for c in range(3):
            products.append((t, 0, "product", (c, k)))
            t += STEP
            if k == 2:
                first.append((t, [(c, ("f3", o, q)) for o, q in pairs]))
            elif k in (1, 3):
                s = -1 if k == 1 else 1
                free = [(c, ("m3", o, q, s)) for o, q in pairs if sign_of(q) != s]
                first.append((t, free))
                for o, q in pairs:
                    if sign_of(q) == s:
                        seen[c, ("m3", o, q, s)] = 1
    last = max(sent.values())
    steps, _ = simulate(first, react, lambda item: last - sent[item], SCATTER_AHEAD)
    return grouped(steps + products, scatter_group)


def with_tasks(steps):
    free, came, out, waiting, arrived = {}, {}, [], [], {}
    t, done = 0.0, 0
    sends = sum(step[0] in ("send", "send0") for step in steps)
    held = [(("ids",), 0.3)] + [(("rows", z), 0.1) for z in range(4)]
    for step in steps:
        kind, c, m = step
        if kind != "receive":
            if kind != "send1":
                k = queue_of(c, m)
                free[k] = max(t, free.get(k, 0.0)) + bytes_of(c, m) / RATE
                key = (c, gather_group(m)[0])
                came[key] = max(came.get(key, 0.0), free[k] + DELAY)
                sends -= 1
            out.append(step)
            continue
        if done >= 84:
            waiting += held
            held = []
        while waiting and (sends == 0 or t + waiting[0][1] <= came[c, m] + SLACK):
            task, cost = waiting.pop(0)
            out.append(("task", task, None))
            t += cost
        t = max(t, came[c, m])
        out.append(step)
        size = gather_size(m)
        done += size
        k = 2 if m[0] == "f3" else (3 if m[-1] == 1 else 1) if m[0] == "m3" else 0
        arrived[c, k] = arrived.get((c, k), 1 if k == 0 else 0) + size
        if arrived[c, k] == 16:
            waiting.append((("hidden", c, k), 0.3))
            held.append((("pick", c, k), 0.3))
            if k == 2:
                held.append((("columns", c), 0.8))
    return out + [("task", task, None) for task, _ in waiting + held]


def gather_size(name):
    if name[0] == "f3":
        return 16
    return 8 if name[0] == "m3" and len(name) == 2 else 1


def numbered(group):
    one = [("m1", s) for s in (1, -1, 2)]
    two = [("m2", o, s) for o in range(4) for s in (1, -1)] + [("f2", o) for o in range(4)]
    pairs = [(o, q) for o in range(4) for q in range(4)]
    three = [("m3", o, q, s) for o, q in pairs for s in (1, -1)] + [("f3", o, q) for o, q in pairs]
    names = dict.fromkeys(group(m)[0] for m in one + two + three)
    return {name: i for i, name in enumerate(names)}


GATHER_SLOT = numbered(gather_group)
SCATTER_SLOT = numbered(scatter_group)


def dot(a, b):
    return jnp.dot(a, b, preferred_element_type=F32)


def dot_nt(a, b):
    return lax.dot_general(a, b, (((1,), (1,)), ((), ())), preferred_element_type=F32)


def layer_kernel(
    tokens_hbm,
    state_hbm,
    norm_mix_hbm,
    w_drive_hbm,
    lam_real_hbm,
    lam_imag_hbm,
    log_step_hbm,
    b_real_hbm,
    b_imag_hbm,
    readout_real_hbm,
    readout_imag_hbm,
    d_skip_hbm,
    w_value_hbm,
    w_glugate_hbm,
    w_output_hbm,
    norm_ffn_hbm,
    group_hbm,
    router_hbm,
    ids_hbm,
    vector_hbm,
    gate_hbm,
    up_hbm,
    down_hbm,
    eg_hbm,
    eu_hbm,
    ed_hbm,
    out_ref,
    state_out,
    tokens_ref,
    state_ref,
    norms_ref,
    w_drive_ref,
    lam_ref,
    log_step_ref,
    maps_ref,
    d_skip_ref,
    glu_ref,
    w_output_ref,
    group_ref,
    router_ref,
    ids_ref,
    input_re,
    input_im,
    readout_re,
    readout_im,
    decay_rows,
    resid_ref,
    own,
    x,
    w_in,
    w_out,
    eg,
    eu,
    ed,
    ids_all,
    ids_own,
    sums,
    hc,
    picking,
    w_turned,
    p,
    r1,
    r2,
    r3,
    load_sem,
    local_sem,
    swap_send,
    swap_recv,
    id_send,
    id_recv,
    ag_send,
    ag_recv,
    rs_send,
    rs_recv,
):
    me = lax.axis_index("ep")
    core = lax.rem(me, 2)
    pos = {"x": lax.rem(me // 2, 4), "y": lax.rem(me // 8, 4), "z": me // 32}
    near = {d: [lax.rem(pos[d] + k, 4) for k in range(4)] for d in "xyz"}

    def device(at):
        return ((at["z"] * 4 + at["y"]) * 4 + at["x"]) * 2 + core

    def neighbour(d, s):
        at = dict(pos)
        at[d] = near[d][s % 4]
        return device(at)

    peers = {(d, s): neighbour(d, s) for d in "xyz" for s in (1, -1, 2)}
    partner = me + 1 - 2 * core

    barrier = pltpu.get_barrier_semaphore()
    for peer in [*peers.values(), partner]:
        pl.semaphore_signal(barrier, inc=1, device_id=(peer,), device_id_type=MESH)

    def send(action, copy):
        if action == "send":
            copy.start()
            return

        @pl.when(core == int(action[-1]))
        def _():
            copy.start()

    def await_bytes(ref, semaphore):
        pltpu.make_async_copy(ref, ref, semaphore).wait()

    loads = (
        ((lam_real_hbm, lam_imag_hbm), lam_ref),
        ((log_step_hbm,), log_step_ref),
        ((b_real_hbm, b_imag_hbm, readout_real_hbm, readout_imag_hbm), maps_ref),
        ((tokens_hbm,), tokens_ref),
        ((norm_mix_hbm, norm_ffn_hbm, vector_hbm), norms_ref),
        ((w_drive_hbm,), w_drive_ref),
        ((state_hbm,), state_ref),
        ((d_skip_hbm,), d_skip_ref),
        ((w_value_hbm, w_glugate_hbm), glu_ref),
        ((w_output_hbm,), w_output_ref),
        ((ids_hbm,), ids_ref),
        ((group_hbm,), group_ref),
        ((router_hbm,), router_ref),
    )
    for i, (sources, target) in enumerate(loads):
        for j, source in enumerate(sources):
            part = target.at[j] if len(sources) > 1 else target
            pltpu.make_async_copy(source, part, load_sem.at[i]).start()

    def loaded(begin, end):
        for i in range(begin, end):
            await_bytes(loads[i][1], load_sem.at[i])

    def rows(i):
        return pl.ds(pl.multiple_of(i * 64, 64), 64)

    weights = [
        (gate_hbm, w_in.at[rows(core)]),
        (up_hbm, w_in.at[rows(2 + core)]),
        (down_hbm, w_out.at[rows(core)]),
        (eg_hbm, eg.at[core]),
        (eu_hbm, eu.at[core]),
        (ed_hbm, ed.at[core]),
    ]
    group = (0, 0, 0, 1, 2, 3)
    for i, (s, t) in zip(group, weights):
        pltpu.make_async_copy(s, t, local_sem.at[i]).start()
    pieces = [(0, *pair) for pair in weights[:3]]
    for j, (s, t) in enumerate(weights[3:]):
        depth = s.shape[0] // 4
        for i in range(4):
            part = pl.ds(i * depth, depth)
            pieces.append((1 + j, s.at[part], t.at[part]))
    swaps = [
        pltpu.make_async_remote_copy(
            src_ref=s,
            dst_ref=t,
            send_sem=swap_send.at[i],
            recv_sem=swap_recv.at[i],
            device_id=(partner,),
            device_id_type=MESH,
        )
        for i, s, t in pieces
    ]
    swapped = (w_out.at[pl.ds(0, 192)], eg.at[0], eu.at[0], ed.at[0])

    def weights_wait(i):
        await_bytes(swapped[i], local_sem.at[i])
        await_bytes(swapped[i], swap_recv.at[i])

    for ref in (input_re, input_im, readout_re, readout_im):
        ref[...] = jnp.zeros((4, 128, 512), BF16)
    loaded(0, 6)
    pl.semaphore_wait(barrier, 10)
    for copy in swaps[:7]:
        copy.start()
    square = lax.broadcasted_iota(jnp.int32, (32, 32), 0) == lax.broadcasted_iota(
        jnp.int32, (32, 32), 1
    )
    time_step = jnp.sum(
        jnp.where(square, jnp.exp(log_step_ref[...]), 0.0), axis=1, keepdims=True
    )
    lam_re = lam_ref[0]
    lam_im = lam_ref[1]
    magnitude = jnp.exp(lam_re * time_step)
    decay_re = magnitude * jnp.cos(lam_im * time_step)
    decay_im = magnitude * jnp.sin(lam_im * time_step)
    modulus = lam_re * lam_re + lam_im * lam_im
    factor_re = ((decay_re - 1.0) * lam_re + decay_im * lam_im) / modulus
    factor_im = (decay_im * lam_re - (decay_re - 1.0) * lam_im) / modulus
    for g in range(32):
        q, j = divmod(g, 8)
        at = (q, pl.ds(16 * j, 16), pl.ds(64 * j, 64))
        f_re = factor_re[g : g + 1]
        f_im = factor_im[g : g + 1]
        b_re = maps_ref[0, g]
        b_im = maps_ref[1, g]
        input_re[at] = (f_re * b_re - f_im * b_im).astype(BF16)
        input_im[at] = (f_re * b_im + f_im * b_re).astype(BF16)
        readout_re[at] = maps_ref[2, g].astype(BF16)
        readout_im[at] = maps_ref[3, g].astype(BF16)
        lane = pl.ds(64 * g, 64)
        decay_rows[pl.ds(0, 1), lane] = decay_re[g : g + 1]
        decay_rows[pl.ds(1, 1), lane] = decay_im[g : g + 1]

    def rms_scale(values, gain):
        mean = jnp.mean(values * values, axis=1, keepdims=True)
        return (values * lax.rsqrt(mean + EPS) * gain).astype(BF16)

    tokens = tokens_ref[...].astype(F32)
    drive = dot(rms_scale(tokens, norms_ref[0]), w_drive_ref[...]).astype(BF16)
    loaded(6, 8)
    projected = []
    for q in range(4):
        channels = drive[:, 128 * q : 128 * q + 128]
        cols = pl.ds(512 * q, 512)
        old_re = state_ref[0, :, cols]
        old_im = state_ref[1, :, cols]
        d_re = decay_rows[pl.ds(0, 1), cols]
        d_im = decay_rows[pl.ds(1, 1), cols]
        new_re = d_re * old_re - d_im * old_im + dot(channels, input_re[q])
        new_im = d_re * old_im + d_im * old_re + dot(channels, input_im[q])
        state_out[0, :, cols] = new_re
        state_out[1, :, cols] = new_im
        projected.append(
            dot_nt(new_re.astype(BF16), readout_re[q]) - dot_nt(new_im.astype(BF16), readout_im[q])
        )
    skipped = d_skip_ref[...] * drive.astype(F32)
    readout = jax.nn.gelu(jnp.concatenate(projected, axis=1) + skipped).astype(BF16)
    loaded(8, 10)
    value_part = dot(readout, glu_ref[0])
    gate_part = dot(readout, glu_ref[1])
    mixed = (value_part * jax.nn.sigmoid(gate_part)).astype(BF16)
    resid = (tokens + dot(mixed, w_output_ref[...])).astype(BF16)
    resid_ref[...] = resid
    loaded(10, 13)
    normed = rms_scale(resid.astype(F32), norms_ref[1])

    own[...] = normed

    x[pos["z"], pos["y"], pos["x"]] = normed

    def write_words():
        normed = own[...]
        ids = ids_ref[...].astype(F32)
        lanes = lax.broadcasted_iota(jnp.int32, (16, 128), 1)
        down = lax.broadcasted_iota(jnp.int32, (16, 128), 0)
        this = lax.broadcasted_iota(jnp.int32, (16, 16), 0)
        that = lax.broadcasted_iota(jnp.int32, (16, 16), 1)
        hits = []
        columns = []
        for t in range(6):
            column = jnp.sum(jnp.where(this == that, ids[t : t + 1], 0.0), axis=1, keepdims=True)
            columns.append(column)
            hits.append(column == lanes.astype(F32))
        chosen = jnp.zeros((16, 128), F32)
        for hit in hits:
            chosen = chosen + jnp.where(hit, 1.0, 0.0)
        earlier = jnp.where(that < this, 1.0, 0.0)
        ordinal = dot(earlier.astype(BF16), chosen.astype(BF16))
        branch = jax.nn.sigmoid(
            jnp.sum(normed.astype(F32) * norms_ref[2], axis=1, keepdims=True)
        )
        group_exp = jnp.exp(dot_nt(normed, group_ref[...]))
        group_prob = group_exp / jnp.sum(group_exp, axis=1, keepdims=True)
        inner_exp = jnp.exp(dot(normed, router_ref[...]))
        inner_sum = jnp.zeros((16, 128), F32)
        outer = jnp.zeros((16, 128), F32)
        for g in range(4):
            inside = lanes // 32 == g
            total = jnp.sum(jnp.where(inside, inner_exp, 0.0), axis=1, keepdims=True)
            inner_sum = jnp.where(inside, total, inner_sum)
            outer = jnp.where(inside, group_prob[:, g : g + 1], outer)
        inner = inner_exp / inner_sum
        joint = outer * inner
        divisor = jnp.sum(jnp.where(chosen > 0.0, inner, 0.0), axis=1, keepdims=True)
        words = jnp.where(lanes == 96 + down, branch, 0.0)
        gates = jnp.zeros((16, 128), F32)
        for t in range(6):
            place = lanes == 16 * t + down
            rank = jnp.sum(jnp.where(hits[t], ordinal, 0.0), axis=1, keepdims=True)
            gate = jnp.sum(jnp.where(hits[t], joint, 0.0), axis=1, keepdims=True) / divisor
            words = words + jnp.where(place, columns[t] + 128.0 * rank, 0.0)
            gates = gates + jnp.where(place, gate, 0.0)
        words = jnp.sum(words, axis=0, keepdims=True)
        gates = jnp.sum(gates, axis=0, keepdims=True)
        for ref in (ids_own, ids_all.at[pos["z"], pos["y"], pos["x"]]):
            ref[pl.ds(0, 1), :] = words
            ref[pl.ds(1, 1), :] = gates

    def view(ref, colour, offsets, cols):
        at = {}
        for d, o in zip(ORDERS[colour], offsets):
            at[d] = slice(None) if o is None else near[d][o % 4]
        return ref.at[at["z"], at["y"], at["x"], :, cols]

    def whole(colour):
        return pl.ds(*COLS[colour])

    def gather_copy(colour, m):
        d, s = link_of(colour, m)
        where = {
            "m1": lambda: (0, 0, 0),
            "m2": lambda: (m[1], 0, 0),
            "f2": lambda: (m[1], -s, 0),
            "m3": lambda: (m[1], m[2], 0),
            "f3": lambda: (m[1], m[2], -s),
        }[m[0]]()
        target = view(x, colour, where, whole(colour))
        return pltpu.make_async_remote_copy(
            src_ref=own.at[:, whole(colour)] if where == (0, 0, 0) else target,
            dst_ref=target,
            send_sem=ag_send.at[colour, int(m[0][1]) - 1],
            recv_sem=ag_recv.at[colour, GATHER_SLOT[gather_group(m)[0]]],
            device_id=(peers[d, s],),
            device_id_type=MESH,
        )

    def gather_wait(colour, name):
        size = gather_size(name)
        cols = whole(colour)
        ref = {16: x.at[0, :, :, :, cols], 8: x.at[0, pl.ds(0, 2), :, :, cols]}.get(
            size, x.at[0, 0, 0, :, cols]
        )
        await_bytes(ref, ag_recv.at[colour, GATHER_SLOT[name]])
        return size

    def ids_send(level):
        at = dict(pos)
        for axis in "xyz"[:level]:
            at[axis] = slice(None)
        target = ids_all.at[at["z"], at["y"], at["x"]]
        for s in (1, -1, 2):
            pltpu.make_async_remote_copy(
                src_ref=target if level else ids_own,
                dst_ref=target,
                send_sem=id_send.at[level],
                recv_sem=id_recv.at[level],
                device_id=(peers["xyz"[level], s],),
                device_id_type=MESH,
            ).start()

    def three(level):
        three = pl.ds(0, 3)
        return (ids_all.at[0, 0, three], ids_all.at[0, three], ids_all.at[three])[level]

    def ids_receive(level):
        await_bytes(three(level), id_recv.at[level])

    first = me - core

    def slab_of(ref, d, k, cols):
        i = near[d][k]
        if d == "z":
            return ref[i, :, :, :, cols]
        if d == "y":
            return ref[:, i, :, :, cols]
        return ref[:, :, i, :, cols]

    def slab_store(ref, d, k, cols, values):
        i = near[d][k]
        values = values.reshape(4, 4, 16, values.shape[-1])
        if d == "z":
            ref[i, :, :, :, cols] = values
        elif d == "y":
            ref[:, i, :, :, cols] = values
        else:
            ref[:, :, i, :, cols] = values

    tables = {}

    def read_ids():
        table = ids_all[:, :, :, pl.ds(0, 1), :].reshape(64, 128)
        all_gates = ids_all[:, :, :, pl.ds(1, 1), :].reshape(64, 128)
        lane = lax.broadcasted_iota(jnp.int32, (64, 128), 1)
        sender = lax.broadcasted_iota(jnp.int32, (64, 128), 0)
        found, gates = [], []
        for e in range(2):
            for k in range(2):
                wanted = (first + e + 128 * k).astype(F32)
                hit = (table == wanted) & (lane < 96)
                row = jnp.where(hit, lax.rem(lane, 16) + 16 * sender, -1)
                found.append(jnp.max(row.astype(F32), axis=1, keepdims=True))
                gates.append(jnp.sum(jnp.where(hit, all_gates, 0.0), axis=1, keepdims=True))
        code = jnp.concatenate(found, axis=0)
        tables["code"] = code
        tables["gates"] = jnp.concatenate(gates, axis=0)
        wide = jnp.broadcast_to(code, (256, 256))
        diagonal = lax.broadcasted_iota(jnp.int32, (256, 256), 0) == lax.broadcasted_iota(
            jnp.int32, (256, 256), 1
        )
        across = jnp.sum(jnp.where(diagonal, wide, 0.0), axis=0, keepdims=True)
        tables["across"] = across

    def slots_by_rows(z):
        number = z * 256 + lax.broadcasted_iota(jnp.int32, (256, 256), 0)
        hot = jnp.where(number.astype(F32) == tables["across"], 1.0, 0.0).astype(BF16)
        hc[z, :, :, :, pl.ds(128, 256)] = hot.reshape(4, 4, 16, 256)

    def slab_rows(colour, k):
        return slab_of(x, ORDERS[colour][2], k, whole(colour)).reshape(256, COLS[colour][1])

    def use_hidden(colour, k):
        d = ORDERS[colour][2]
        every = pl.ds(0, 256)
        total = slab_of(sums, d, k, every).reshape(256, 256)
        total = total + dot(slab_rows(colour, k), w_turned[whole(colour), :])
        slab_store(sums, d, k, every, total)

    def use_pick(colour, k):
        d = ORDERS[colour][2]
        cols = whole(colour)
        lane = lax.broadcasted_iota(jnp.int32, (1, 256), 1)
        a, b, r = lane // 64, lax.rem(lane // 16, 4), lax.rem(lane, 16)
        i = near[d][k]
        if d == "z":
            sender = i * 16 + a * 4 + b
        elif d == "y":
            sender = a * 16 + i * 4 + b
        else:
            sender = a * 16 + b * 4 + i
        number = (sender * 16 + r).astype(F32)
        hot = jnp.where(tables["code"] == number, 1.0, 0.0).astype(BF16)
        rows = dot(hot, slab_rows(colour, k))
        if k == 0:
            picking[:, cols] = rows
        else:
            picking[:, cols] += rows

    sums[...] = jnp.zeros((4, 4, 4, 16, 256), F32)

    experts_in = {}

    def turn_weights():
        weights_wait(0)
        for i in range(8):
            part = pl.ds(256 * i, 256)
            w_turned[part, :] = w_in[:, part].T

    def use_columns(colour):
        start, width = COLS[colour]
        cols = pl.ds(start, width)
        rows = picking[:, cols].astype(BF16)
        parts = []
        for e in range(2):
            mine = rows[e * 128 : (e + 1) * 128]
            parts += [dot(mine, eg[e, cols, :]), dot(mine, eu[e, cols, :])]
        for i, part in enumerate(parts):
            experts_in[i] = experts_in[i] + part if i in experts_in else part

    gather_steps, gather_sent = plan_gather()
    scatter_steps = plan_scatter(gather_sent)
    done = 0
    tasks = [
        (0, lambda: (write_words(), ids_send(0))),
        (14, lambda: (ids_receive(0), ids_send(1))),
        (24, turn_weights),
        (44, lambda: (ids_receive(1), ids_send(2))),
    ]
    more = swaps[7:]
    for action, c, m in gather_steps:
        if action == "task":
            name, *what = c
            if name == "ids":
                ids_receive(2)
                read_ids()
            elif name == "rows":
                slots_by_rows(*what)
            elif name == "hidden":
                use_hidden(*what)
            elif name == "pick":
                use_pick(*what)
            else:
                if not experts_in:
                    weights_wait(1)
                    weights_wait(2)
                use_columns(*what)
            continue
        if action != "receive":
            send(action, gather_copy(c, m))
            continue
        while tasks and done >= tasks[0][0]:
            tasks.pop(0)[1]()
        if more and done >= 12 * (8 - len(more)):
            more.pop(0).start()
        done += gather_wait(c, m)
    weights_wait(3)


    for zi in range(4):
        products = sums[zi].reshape(256, 256)
        words = jnp.broadcast_to(ids_all[zi, :, :, pl.ds(0, 1), :], (4, 4, 16, 128)).reshape(256, 128)
        lane = lax.broadcasted_iota(jnp.int32, (256, 128), 1)
        row = lax.broadcasted_iota(jnp.int32, (256, 128), 0)
        own_word = lane == 96 + lax.rem(row, 16)
        scale = jnp.sum(jnp.where(own_word, words, 0.0), axis=1, keepdims=True)
        hidden = (scale * jax.nn.silu(products[:, :128]) * products[:, 128:]).astype(BF16)
        hc[zi, :, :, :, pl.ds(0, 128)] = hidden.reshape(4, 4, 16, 128)

    for e in range(2):
        hidden = (jax.nn.silu(experts_in[2 * e]) * experts_in[2 * e + 1]).astype(BF16)
        result = dot(hidden, ed[e])
        weighted = result * tables["gates"][e * 128 : (e + 1) * 128]
        w_out[pl.ds(128 + e * 128, 128), :] = weighted.astype(BF16)

    def landing(colour, m):
        cols = pl.ds(0, COLS[colour][1])
        i = {1: 0, -1: 1, 2: 2}
        if m[0] == "m1":
            return r1.at[colour, i[m[1]], :, cols]
        if m[0] == "m2":
            return r2.at[colour, i[m[2]], m[1], :, cols]
        if m[0] == "f2":
            return r2.at[colour, 2, m[1], :, cols]
        if m[0] == "m3":
            return r3.at[colour, i[m[3]], m[1], m[2], :, cols]
        return r3.at[colour, 2, m[1], m[2], :, cols]

    def scatter_copy(colour, m):
        d, s = link_of(colour, m)
        where = {
            "m1": lambda: (-s, 0, 0),
            "m2": lambda: (m[1], -s, 0),
            "f2": lambda: (m[1], 2, 0),
            "m3": lambda: (m[1], m[2], -s),
            "f3": lambda: (m[1], m[2], 2),
        }[m[0]]()
        return pltpu.make_async_remote_copy(
            src_ref=view(p, colour, where, whole(colour)),
            dst_ref=landing(colour, m),
            send_sem=rs_send.at[colour, int(m[0][1]) - 1],
            recv_sem=rs_recv.at[colour, SCATTER_SLOT[scatter_group(m)[0]]],
            device_id=(peers[d, s if s == 2 else -s],),
            device_id_type=MESH,
        )

    def scatter_wait(colour, name):
        cols = pl.ds(0, COLS[colour][1])
        two = pl.ds(0, 2)
        if name[0] == "m1":
            ref = r1.at[colour, :, :, cols]
        elif name[0] == "m2":
            ref = r2.at[colour, two, name[1], :, cols]
        elif name[0] == "m3":
            ref = r3.at[colour, two, name[1], name[2], :, cols]
        else:
            ref = landing(colour, name)
        await_bytes(ref, rs_recv.at[colour, SCATTER_SLOT[name]])

    def product(colour, k):
        start, width = COLS[colour]
        cols = pl.ds(start, width)
        d = ORDERS[colour][2]
        left = slab_of(hc, d, k, pl.ds(0, 384)).reshape(256, 384)
        slab_store(p, d, k, cols, dot(left, w_out[:, cols]).astype(BF16))

    def add(colour, where, *messages):
        ref = view(p, colour, where, whole(colour))
        total = ref[...].astype(F32)
        for m in messages:
            total = total + landing(colour, m)[...].astype(F32)
        ref[...] = total.astype(BF16)

    done = 0
    for action, *what in scatter_steps:
        if action == "product":
            product(*what)
            continue
        c, m = what
        if action != "receive":
            send(action, scatter_copy(c, m))
            continue
        done += 1
        scatter_wait(c, m)
        if m[0] == "f3":
            add(c, (m[1], m[2], -sign_of(m[2])), m)
        elif m[0] == "f2":
            add(c, (m[1], -sign_of(m[1]), 0), m)
        elif m[0] == "m3":
            add(c, (m[1], m[2], 0), (*m, 1), (*m, -1))
        elif m[0] == "m2":
            add(c, (m[1], 0, 0), (*m, 1), (*m, -1))
    for c in range(3):
        start, width = COLS[c]
        cols = pl.ds(start, width)
        total = resid_ref[:, cols].astype(F32) + view(p, c, (0, 0, 0), cols)[...].astype(F32)
        for k in range(3):
            total = total + r1[c, k, :, pl.ds(0, width)].astype(F32)
        out_ref[:, cols] = total.astype(BF16)

    for level in range(3):
        await_bytes(three(level), id_send.at[level])
    for i in range(4):
        await_bytes(swapped[i], swap_send.at[i])
    for c in range(3):
        cols = whole(c)
        three_blocks = pl.ds(0, 3)
        sent = (
            x.at[0, 0, three_blocks, :, cols],
            x.at[0, three_blocks, :, :, cols],
            x.at[three_blocks, :, :, :, cols],
        )
        for i in range(3):
            await_bytes(sent[i], ag_send.at[c, i])
            await_bytes(sent[i], rs_send.at[c, i])


def finish_kernel(rows_ref, state_ref, rows_out, state_out, sem):
    copies = (
        pltpu.make_async_copy(rows_ref, rows_out, sem.at[0]),
        pltpu.make_async_copy(state_ref, state_out, sem.at[1]),
    )
    for copy in copies:
        copy.start()
    for copy in copies:
        copy.wait()


def finish(rows, state):
    return pl.pallas_call(
        finish_kernel,
        out_shape=(
            jax.ShapeDtypeStruct(rows.shape, rows.dtype),
            jax.ShapeDtypeStruct(state.shape, state.dtype),
        ),
        in_specs=[pl.BlockSpec(memory_space=pltpu.VMEM)] * 2,
        out_specs=[pl.BlockSpec(memory_space=pl.ANY)] * 2,
        scratch_shapes=[pltpu.SemaphoreType.DMA((2,))],
        compiler_params=pltpu.CompilerParams(vmem_limit_bytes=4 * 1024 * 1024),
    )(rows, state)


def on_device(
    tokens,
    state,
    norm_mix,
    w_drive,
    lam_real,
    lam_imag,
    log_step,
    b_real,
    b_imag,
    readout_real,
    readout_imaginary,
    d_skip,
    w_value,
    w_glugate,
    w_output,
    norm_ffn,
    w_group,
    w_expert,
    route_ids,
    expert_gate,
    expert_up,
    expert_down,
    dense_vector,
    dense_gate,
    dense_up,
    dense_down,
):
    vmem = pl.BlockSpec(memory_space=pltpu.VMEM)
    hbm = pl.BlockSpec(memory_space=pltpu.HBM)
    rows, new_state = pl.pallas_call(
        layer_kernel,
        out_shape=(
            jax.ShapeDtypeStruct((16, 2048), BF16),
            jax.ShapeDtypeStruct((2, 16, 2048), F32),
        ),
        in_specs=[hbm] * 26,
        out_specs=(vmem, vmem),
        scratch_shapes=[
            pltpu.VMEM((16, 2048), BF16),
            pltpu.VMEM((2, 16, 2048), F32),
            pltpu.VMEM((3, 1, 2048), F32),
            pltpu.VMEM((2048, 512), BF16),
            pltpu.VMEM((2, 32, 64), F32),
            pltpu.VMEM((1, 32), F32),
            pltpu.VMEM((4, 32, 16, 64), F32),
            pltpu.VMEM((1, 512), F32),
            pltpu.VMEM((2, 512, 512), BF16),
            pltpu.VMEM((512, 2048), BF16),
            pltpu.VMEM((4, 2048), BF16),
            pltpu.VMEM((2048, 128), BF16),
            pltpu.VMEM((6, 16), jnp.int32),
            pltpu.VMEM((4, 128, 512), BF16),
            pltpu.VMEM((4, 128, 512), BF16),
            pltpu.VMEM((4, 128, 512), BF16),
            pltpu.VMEM((4, 128, 512), BF16),
            pltpu.VMEM((2, 2048), F32),
            pltpu.VMEM((16, 2048), BF16),
            pltpu.VMEM((16, 2048), BF16),
            pltpu.VMEM((4, 4, 4, 16, 2048), BF16),
            pltpu.VMEM((256, 2048), BF16),
            pltpu.VMEM((384, 2048), BF16),
            pltpu.VMEM((2, 2048, 512), BF16),
            pltpu.VMEM((2, 2048, 512), BF16),
            pltpu.VMEM((2, 512, 2048), BF16),
            pltpu.VMEM((4, 4, 4, 2, 128), F32),
            pltpu.VMEM((2, 128), F32),
            pltpu.VMEM((4, 4, 4, 16, 256), F32),
            pltpu.VMEM((4, 4, 4, 16, 384), BF16),
            pltpu.VMEM((256, 2048), F32),
            pltpu.VMEM((2048, 256), BF16),
            pltpu.VMEM((4, 4, 4, 16, 2048), BF16),
            pltpu.VMEM((3, 3, 16, 768), BF16),
            pltpu.VMEM((3, 3, 4, 16, 768), BF16),
            pltpu.VMEM((3, 3, 4, 4, 16, 768), BF16),
            pltpu.SemaphoreType.DMA((13,)),
            pltpu.SemaphoreType.DMA((4,)),
            pltpu.SemaphoreType.DMA((4,)),
            pltpu.SemaphoreType.DMA((4,)),
            pltpu.SemaphoreType.DMA((3,)),
            pltpu.SemaphoreType.DMA((3,)),
            pltpu.SemaphoreType.DMA((3, 3)),
            pltpu.SemaphoreType.DMA((3, len(GATHER_SLOT))),
            pltpu.SemaphoreType.DMA((3, 3)),
            pltpu.SemaphoreType.DMA((3, len(SCATTER_SLOT))),
        ],
        compiler_params=pltpu.CompilerParams(
            collective_id=0, has_side_effects=True, vmem_limit_bytes=47 * 1024 * 1024
        ),
        cost_estimate=pl.CostEstimate(
            flops=8_000_000_000, bytes_accessed=20_000_000, transcendentals=0
        ),
    )(*[pltpu.with_memory_space_constraint(a, pltpu.HBM) for a in (
        tokens,
        state,
        norm_mix.reshape(1, -1),
        w_drive,
        lam_real,
        lam_imag,
        log_step.reshape(1, -1),
        jnp.transpose(b_real, (0, 2, 1)),
        jnp.transpose(b_imag, (0, 2, 1)),
        readout_real,
        readout_imaginary,
        d_skip.reshape(1, -1),
        w_value,
        w_glugate,
        w_output,
        norm_ffn.reshape(1, -1),
        jnp.transpose(w_group),
        w_expert,
        jnp.transpose(route_ids),
        dense_vector.reshape(1, -1),
        jnp.transpose(dense_gate),
        jnp.transpose(dense_up),
        dense_down,
        expert_gate[0],
        expert_up[0],
        expert_down[0],
    )])
    return finish(rows, new_state)


def solution(mesh):
    placed = (
        P("ep", None),
        P(None, "ep", None),
        P(),
        P(),
        P(),
        P(),
        P(),
        P(),
        P(),
        P(),
        P(),
        P(),
        P(),
        P(),
        P(),
        P(),
        P(),
        P(),
        P("ep", None),
        P("ep", None, None),
        P("ep", None, None),
        P("ep", None, None),
        P(),
        P(None, "ep"),
        P(None, "ep"),
        P("ep", None),
    )
    return jax.shard_map(
        on_device,
        mesh=mesh,
        in_specs=placed,
        out_specs=(P("ep", None), P(None, "ep", None)),
        check_vma=False,
    )
```

```python
import heapq

import jax
import jax.numpy as jnp
from jax import lax
from jax.experimental import pallas as pl
from jax.experimental.pallas import tpu as pltpu
from jax.sharding import PartitionSpec as P

EPS = 1e-05
F32 = jnp.float32
BF16 = jnp.bfloat16
MESH = pl.DeviceIdType.MESH
ORDERS = (("x", "y", "z"), ("y", "z", "x"), ("z", "x", "y"))
COLS = ((0, 640), (640, 640), (1280, 768))
RATE, DELAY, STEP = 46700.0, 2.9, 0.36
GATHER_AHEAD, SCATTER_AHEAD = (1.0, 0.3), (0.6, 0.3)
SLACK = 0.4


def sign_of(offset):
    return 1 if offset in (0, 1) else -1


def link_of(c, m):
    phase = int(m[0][1]) - 1
    return ORDERS[c][phase], m[-1] if m[0] in ("m1", "m2", "m3") else sign_of(m[-1])


def bytes_of(c, m):
    return 32.0 * COLS[c][1] * (2 if m == ("m1", 2) else 1)


def queue_of(c, m):
    d, s = link_of(c, m)
    return d, 1 if s == 2 else s


def gather_group(m):
    if m[0] == "f3":
        return ("f3",), 16
    if m[0] == "m3" and sign_of(m[2]) != m[3]:
        return ("m3", m[3]), 8
    return m, 1


def scatter_group(m):
    if m[0] in ("m2", "m3"):
        return m[:-1], 2
    return (("m1",), 3) if m[0] == "m1" else (m, 1)


def grouped(steps, group):
    seen, out = {}, []
    for _, _, kind, what in sorted(steps, key=lambda step: step[:2]):
        if kind == "receive":
            name, size = group(what[1])
            key = (what[0], name)
            seen[key] = seen.get(key, 0) + 1
            if seen[key] < size:
                continue
            what = key
        out.append((kind, *what))
    merged, place = [], {}
    since = 0
    for step in out:
        if not step[0].startswith("send"):
            since = len(merged)
        elif place.get(step[1:], -1) >= since:
            merged[place[step[1:]]] = ("send", *step[1:])
            continue
        else:
            place[step[1:]] = len(merged)
        merged.append(step)
    return merged


def simulate(first, react, rank, aheads):
    queue, waiting, free, count = [], {}, {}, 0
    sent, came, ready = {}, {}, {}

    def push(t, kind, item):
        nonlocal count
        count += 1
        heapq.heappush(queue, (t, count, kind, item))

    for t, items in first:
        for item in items:
            push(t, "ready", item)
    while queue:
        t, _, kind, item = heapq.heappop(queue)
        if kind == "ready":
            ready[item] = t
            count += 1
            heapq.heappush(waiting.setdefault(queue_of(*item), []), (rank(item), count, item))
            links = [queue_of(*item)]
        elif kind == "free":
            links = [item]
        else:
            came[item] = t
            links = []
            for new in react(item):
                push(t, "ready", new)
        for k in links:
            if free.get(k, 0.0) <= t + 1e-9 and waiting.get(k):
                _, _, m = heapq.heappop(waiting[k])
                free[k] = t + bytes_of(*m) / RATE
                sent[m] = t
                push(free[k], "free", k)
                push(free[k] + (DELAY + 0.8 if m[1] == ("m1", 2) else DELAY), "came", m)
    steps = [(t, 0, "receive", m) for m, t in came.items()]
    for core, ahead in enumerate(aheads):
        steps += [(max(ready[m], t - ahead), 1, "send%d" % core, m) for m, t in sent.items()]
    return steps, sent


def plan_gather():
    def present(c, o, q):
        new = [(c, ("m2", o, 1)), (c, ("m2", o, -1))] if q == 0 else []
        return new + [(c, ("m3", o, q, 1)), (c, ("m3", o, q, -1))]

    def react(item):
        c, m = item
        if m[0] == "m1":
            return present(c, {1: 3, -1: 1, 2: 2}[m[1]], 0)
        if m[0] == "m2":
            o, s = m[1:]
            new = [(c, ("f2", o))] if sign_of(o) == s else []
            return new + present(c, o, 3 if s == 1 else 1)
        if m[0] == "f2":
            return present(c, m[1], 2)
        if m[0] == "m3" and sign_of(m[2]) == m[3]:
            return [(c, ("f3", m[1], m[2]))]
        return []

    start = [(c, ("m1", s)) for s in (1, -1, 2) for c in range(3)]
    for c in range(3):
        start += present(c, 0, 0)
    rank = {"m1": 0, "m2": 1, "f2": 1, "m3": 2, "f3": 3}
    steps, sent = simulate([(0.0, start)], react, lambda item: rank[item[1][0]], GATHER_AHEAD)
    return with_tasks(grouped(steps, gather_group)), sent


def plan_scatter(sent):
    seen = {}

    def react(item):
        c, m = item

        def both(key):
            seen[c, key] = seen.get((c, key), 0) + 1
            return seen[c, key] == 2

        def level2(o, q):
            if q == 2:
                return [(c, ("f2", o))]
            if q == 0:
                return level1(o)
            s = -1 if q == 1 else 1
            return [(c, ("m2", o, s))] if sign_of(o) != s or both(("m2", o, s)) else []

        def level1(o):
            seen[c, "sum", o] = seen.get((c, "sum", o), 0) + 1
            if seen[c, "sum", o] < 3:
                return []
            return [(c, ("m1", {1: -1, 2: 2, 3: 1}[o]))] if o else []

        if m[0] == "f3":
            s = sign_of(m[2])
            return [(c, ("m3", m[1], m[2], s))] if both(("m3",) + m[1:] + (s,)) else []
        if m[0] == "m3":
            return level2(m[1], m[2]) if both(("sum3",) + m[1:3]) else []
        if m[0] == "f2":
            s = sign_of(m[1])
            return [(c, ("m2", m[1], s))] if both(("m2", m[1], s)) else []
        if m[0] == "m2":
            return level1(m[1])
        return []

    first, products, t = [], [], 0.0
    pairs = [(o, q) for o in range(4) for q in range(4)]
    for ks in ((2,), (3, 1), (0,)):
        for c in range(3):
            products.append((t, 0, "product", (c, ks)))
            t += STEP * (0.5 + 0.5 * len(ks))
            if ks == (2,):
                first.append((t, [(c, ("f3", o, q)) for o, q in pairs]))
            for k in (1, 3):
                if k in ks:
                    s = -1 if k == 1 else 1
                    free = [(c, ("m3", o, q, s)) for o, q in pairs if sign_of(q) != s]
                    first.append((t, free))
                    for o, q in pairs:
                        if sign_of(q) == s:
                            seen[c, ("m3", o, q, s)] = 1
    last = max(sent.values())
    steps, _ = simulate(first, react, lambda item: last - sent[item], SCATTER_AHEAD)
    return grouped(steps + products, scatter_group)


def with_tasks(steps):
    free, came, out, waiting, arrived = {}, {}, [], [], {}
    t, done = 0.0, 0
    sends = sum(step[0] in ("send", "send0") for step in steps)
    held = [(("ids",), 0.3)] + [(("rows", z), 0.1) for z in range(4)]
    for step in steps:
        kind, c, m = step
        if kind != "receive":
            if kind != "send1":
                k = queue_of(c, m)
                free[k] = max(t, free.get(k, 0.0)) + bytes_of(c, m) / RATE
                key = (c, gather_group(m)[0])
                came[key] = max(came.get(key, 0.0), free[k] + DELAY)
                sends -= 1
            out.append(step)
            continue
        if done >= 84:
            waiting += held
            held = []
        while waiting and (sends == 0 or t + waiting[0][1] <= came[c, m] + SLACK):
            task, cost = waiting.pop(0)
            out.append(("task", task, None))
            t += cost
        t = max(t, came[c, m])
        out.append(step)
        size = gather_size(m)
        done += size
        k = 2 if m[0] == "f3" else (3 if m[-1] == 1 else 1) if m[0] == "m3" else 0
        arrived[c, k] = arrived.get((c, k), 1 if k == 0 else 0) + size
        if arrived[c, k] == 16 and (k in (0, 2) or arrived.get((c, 4 - k)) == 16):
            both = (1, 3) if k in (1, 3) else (k,)
            waiting.append((("hidden", c, both), 0.3 * len(both)))
            held.append((("pick", c, both), 0.3 * len(both)))
            if k == 2:
                held.append((("columns", c), 0.8))
    return out + [("task", task, None) for task, _ in waiting + held]


def gather_size(name):
    if name[0] == "f3":
        return 16
    return 8 if name[0] == "m3" and len(name) == 2 else 1


def numbered(group):
    one = [("m1", s) for s in (1, -1, 2)]
    two = [("m2", o, s) for o in range(4) for s in (1, -1)] + [("f2", o) for o in range(4)]
    pairs = [(o, q) for o in range(4) for q in range(4)]
    three = [("m3", o, q, s) for o, q in pairs for s in (1, -1)] + [("f3", o, q) for o, q in pairs]
    names = dict.fromkeys(group(m)[0] for m in one + two + three)
    return {name: i for i, name in enumerate(names)}


def receive_slots(steps):
    names = [(c, name) for c in range(3) for name in numbered(gather_group)]
    gather = {key: i for i, key in enumerate(names)}
    last = {}
    for at, (kind, c, m) in enumerate(steps):
        if kind.startswith("send") and link_of(c, m)[1] != 2:
            for core in (0, 1):
                if kind in ("send", "send%d" % core):
                    last[core, link_of(c, m)] = at
    early = steps[: min(last.values())]
    free = [gather[step[1:]] for step in early if step[0] == "receive"]
    scatter, count = {}, len(gather)
    for c in range(3):
        for name in numbered(scatter_group):
            if free and name[0] != "m1":
                scatter[c, name] = free.pop()
            else:
                scatter[c, name] = count
                count += 1
    return gather, scatter, count


GATHER_STEPS, GATHER_SENT = plan_gather()
SCATTER_STEPS = plan_scatter(GATHER_SENT)
GATHER_SLOT, SCATTER_SLOT, RECEIVE_SLOTS = receive_slots(GATHER_STEPS)


def dot(a, b):
    return jnp.dot(a, b, preferred_element_type=F32)


def dot_nt(a, b):
    return lax.dot_general(a, b, (((1,), (1,)), ((), ())), preferred_element_type=F32)


def layer_kernel(
    tokens_hbm,
    state_hbm,
    norm_mix_hbm,
    w_drive_hbm,
    lam_real_hbm,
    lam_imag_hbm,
    log_step_hbm,
    b_real_hbm,
    b_imag_hbm,
    readout_real_hbm,
    readout_imag_hbm,
    d_skip_hbm,
    w_value_hbm,
    w_glugate_hbm,
    w_output_hbm,
    norm_ffn_hbm,
    group_hbm,
    router_hbm,
    ids_hbm,
    vector_hbm,
    gate_hbm,
    up_hbm,
    down_hbm,
    eg_hbm,
    eu_hbm,
    ed_hbm,
    out_ref,
    state_out,
    tokens_ref,
    state_ref,
    norms_ref,
    w_drive_ref,
    lam_ref,
    log_step_ref,
    maps_ref,
    d_skip_ref,
    glu_ref,
    w_output_ref,
    group_ref,
    router_ref,
    ids_ref,
    input_re,
    input_im,
    readout_re,
    readout_im,
    decay_rows,
    resid_ref,
    own,
    x,
    w_in,
    w_out,
    eg,
    eu,
    ed,
    ids_all,
    ids_own,
    sums,
    hc,
    picking,
    w_turned,
    p,
    r1,
    r2,
    r3,
    load_sem,
    local_sem,
    swap_send,
    swap_recv,
    id_send,
    id_recv,
    ag_send,
    rs_send,
    receive_sem,
):
    me = lax.axis_index("ep")
    core = lax.rem(me, 2)
    pos = {"x": lax.rem(me // 2, 4), "y": lax.rem(me // 8, 4), "z": me // 32}
    near = {d: [lax.rem(pos[d] + k, 4) for k in range(4)] for d in "xyz"}

    def device(at):
        return ((at["z"] * 4 + at["y"]) * 4 + at["x"]) * 2 + core

    def neighbour(d, s):
        at = dict(pos)
        at[d] = near[d][s % 4]
        return device(at)

    peers = {(d, s): neighbour(d, s) for d in "xyz" for s in (1, -1, 2)}
    partner = me + 1 - 2 * core

    barrier = pltpu.get_barrier_semaphore()
    for peer in [*peers.values(), partner]:
        pl.semaphore_signal(barrier, inc=1, device_id=(peer,), device_id_type=MESH)

    def send(action, copy):
        if action == "send":
            copy.start()
            return

        @pl.when(core == int(action[-1]))
        def _():
            copy.start()

    def await_bytes(ref, semaphore):
        pltpu.make_async_copy(ref, ref, semaphore).wait()

    loads = (
        ((lam_real_hbm, lam_imag_hbm), lam_ref),
        ((log_step_hbm,), log_step_ref),
        ((b_real_hbm, b_imag_hbm, readout_real_hbm, readout_imag_hbm), maps_ref),
        ((tokens_hbm,), tokens_ref),
        ((norm_mix_hbm, norm_ffn_hbm, vector_hbm), norms_ref),
        ((w_drive_hbm,), w_drive_ref),
        ((state_hbm,), state_ref),
        ((d_skip_hbm,), d_skip_ref),
        ((w_value_hbm, w_glugate_hbm), glu_ref),
        ((w_output_hbm,), w_output_ref),
        ((ids_hbm,), ids_ref),
        ((group_hbm,), group_ref),
        ((router_hbm,), router_ref),
    )
    for i, (sources, target) in enumerate(loads):
        for j, source in enumerate(sources):
            part = target.at[j] if len(sources) > 1 else target
            pltpu.make_async_copy(source, part, load_sem.at[i]).start()

    def loaded(begin, end):
        for i in range(begin, end):
            await_bytes(loads[i][1], load_sem.at[i])

    def rows(i):
        return pl.ds(pl.multiple_of(i * 64, 64), 64)

    weights = [
        (gate_hbm, w_in.at[rows(core)]),
        (up_hbm, w_in.at[rows(2 + core)]),
        (down_hbm, w_out.at[rows(core)]),
        (eg_hbm, eg.at[core]),
        (eu_hbm, eu.at[core]),
        (ed_hbm, ed.at[core]),
    ]
    group = (0, 0, 0, 1, 2, 3)
    for i, (s, t) in zip(group, weights):
        pltpu.make_async_copy(s, t, local_sem.at[i]).start()
    pieces = [(0, *pair) for pair in weights[:3]]
    for j, (s, t) in enumerate(weights[3:]):
        depth = s.shape[0] // 4
        for i in range(4):
            part = pl.ds(i * depth, depth)
            pieces.append((1 + j, s.at[part], t.at[part]))
    swaps = [
        pltpu.make_async_remote_copy(
            src_ref=s,
            dst_ref=t,
            send_sem=swap_send.at[i],
            recv_sem=swap_recv.at[i],
            device_id=(partner,),
            device_id_type=MESH,
        )
        for i, s, t in pieces
    ]
    swapped = (w_out.at[pl.ds(0, 192)], eg.at[0], eu.at[0], ed.at[0])

    def weights_wait(i):
        await_bytes(swapped[i], local_sem.at[i])
        await_bytes(swapped[i], swap_recv.at[i])

    for ref in (input_re, input_im, readout_re, readout_im):
        ref[...] = jnp.zeros((4, 128, 512), BF16)
    loaded(0, 3)
    square = lax.broadcasted_iota(jnp.int32, (32, 32), 0) == lax.broadcasted_iota(
        jnp.int32, (32, 32), 1
    )
    time_step = jnp.sum(
        jnp.where(square, jnp.exp(log_step_ref[...]), 0.0), axis=1, keepdims=True
    )
    lam_re = lam_ref[0]
    lam_im = lam_ref[1]
    magnitude = jnp.exp(lam_re * time_step)
    decay_re = magnitude * jnp.cos(lam_im * time_step)
    decay_im = magnitude * jnp.sin(lam_im * time_step)
    modulus = lam_re * lam_re + lam_im * lam_im
    factor_re = ((decay_re - 1.0) * lam_re + decay_im * lam_im) / modulus
    factor_im = (decay_im * lam_re - (decay_re - 1.0) * lam_im) / modulus
    for g in range(32):
        q, j = divmod(g, 8)
        at = (q, pl.ds(16 * j, 16), pl.ds(64 * j, 64))
        f_re = factor_re[g : g + 1]
        f_im = factor_im[g : g + 1]
        b_re = maps_ref[0, g]
        b_im = maps_ref[1, g]
        input_re[at] = (f_re * b_re - f_im * b_im).astype(BF16)
        input_im[at] = (f_re * b_im + f_im * b_re).astype(BF16)
        readout_re[at] = maps_ref[2, g].astype(BF16)
        readout_im[at] = maps_ref[3, g].astype(BF16)
        lane = pl.ds(64 * g, 64)
        decay_rows[pl.ds(0, 1), lane] = decay_re[g : g + 1]
        decay_rows[pl.ds(1, 1), lane] = decay_im[g : g + 1]

    pl.semaphore_wait(barrier, 10)
    for copy in swaps[:7]:
        copy.start()


    def rms_scale(values, gain):
        mean = jnp.mean(values * values, axis=1, keepdims=True)
        return (values * lax.rsqrt(mean + EPS) * gain).astype(BF16)

    loaded(3, 6)
    tokens = tokens_ref[...].astype(F32)
    drive = dot(rms_scale(tokens, norms_ref[0]), w_drive_ref[...]).astype(BF16)
    loaded(6, 8)
    projected = []
    for q in range(4):
        channels = drive[:, 128 * q : 128 * q + 128]
        cols = pl.ds(512 * q, 512)
        old_re = state_ref[0, :, cols]
        old_im = state_ref[1, :, cols]
        d_re = decay_rows[pl.ds(0, 1), cols]
        d_im = decay_rows[pl.ds(1, 1), cols]
        new_re = d_re * old_re - d_im * old_im + dot(channels, input_re[q])
        new_im = d_re * old_im + d_im * old_re + dot(channels, input_im[q])
        state_out[0, :, cols] = new_re
        state_out[1, :, cols] = new_im
        projected.append(
            dot_nt(new_re.astype(BF16), readout_re[q]) - dot_nt(new_im.astype(BF16), readout_im[q])
        )
    skipped = d_skip_ref[...] * drive.astype(F32)
    readout = jax.nn.gelu(jnp.concatenate(projected, axis=1) + skipped).astype(BF16)
    loaded(8, 10)
    value_part = dot(readout, glu_ref[0])
    gate_part = dot(readout, glu_ref[1])
    mixed = (value_part * jax.nn.sigmoid(gate_part)).astype(BF16)
    resid = (tokens + dot(mixed, w_output_ref[...])).astype(BF16)
    resid_ref[...] = resid
    loaded(10, 13)
    normed = rms_scale(resid.astype(F32), norms_ref[1])

    own[...] = normed

    x[pos["z"], pos["y"], pos["x"]] = normed

    def write_words():
        sums[...] = jnp.zeros((4, 4, 4, 16, 256), F32)
        normed = own[...]
        ids = ids_ref[...].astype(F32)
        lanes = lax.broadcasted_iota(jnp.int32, (16, 128), 1)
        down = lax.broadcasted_iota(jnp.int32, (16, 128), 0)
        this = lax.broadcasted_iota(jnp.int32, (16, 16), 0)
        that = lax.broadcasted_iota(jnp.int32, (16, 16), 1)
        hits = []
        columns = []
        for t in range(6):
            column = jnp.sum(jnp.where(this == that, ids[t : t + 1], 0.0), axis=1, keepdims=True)
            columns.append(column)
            hits.append(column == lanes.astype(F32))
        chosen = jnp.zeros((16, 128), F32)
        for hit in hits:
            chosen = chosen + jnp.where(hit, 1.0, 0.0)
        earlier = jnp.where(that < this, 1.0, 0.0)
        ordinal = dot(earlier.astype(BF16), chosen.astype(BF16))
        branch = jax.nn.sigmoid(
            jnp.sum(normed.astype(F32) * norms_ref[2], axis=1, keepdims=True)
        )
        group_exp = jnp.exp(dot_nt(normed, group_ref[...]))
        group_prob = group_exp / jnp.sum(group_exp, axis=1, keepdims=True)
        inner_exp = jnp.exp(dot(normed, router_ref[...]))
        inner_sum = jnp.zeros((16, 128), F32)
        outer = jnp.zeros((16, 128), F32)
        for g in range(4):
            inside = lanes // 32 == g
            total = jnp.sum(jnp.where(inside, inner_exp, 0.0), axis=1, keepdims=True)
            inner_sum = jnp.where(inside, total, inner_sum)
            outer = jnp.where(inside, group_prob[:, g : g + 1], outer)
        inner = inner_exp / inner_sum
        joint = outer * inner
        divisor = jnp.sum(jnp.where(chosen > 0.0, inner, 0.0), axis=1, keepdims=True)
        words = jnp.where(lanes == 96 + down, branch, 0.0)
        gates = jnp.zeros((16, 128), F32)
        for t in range(6):
            place = lanes == 16 * t + down
            rank = jnp.sum(jnp.where(hits[t], ordinal, 0.0), axis=1, keepdims=True)
            gate = jnp.sum(jnp.where(hits[t], joint, 0.0), axis=1, keepdims=True) / divisor
            words = words + jnp.where(place, columns[t] + 128.0 * rank, 0.0)
            gates = gates + jnp.where(place, gate, 0.0)
        words = jnp.sum(words, axis=0, keepdims=True)
        gates = jnp.sum(gates, axis=0, keepdims=True)
        for ref in (ids_own, ids_all.at[pos["z"], pos["y"], pos["x"]]):
            ref[pl.ds(0, 1), :] = words
            ref[pl.ds(1, 1), :] = gates

    def view(ref, colour, offsets, cols):
        at = {}
        for d, o in zip(ORDERS[colour], offsets):
            at[d] = slice(None) if o is None else near[d][o % 4]
        return ref.at[at["z"], at["y"], at["x"], :, cols]

    def whole(colour):
        return pl.ds(*COLS[colour])

    def gather_copy(colour, m):
        d, s = link_of(colour, m)
        where = {
            "m1": lambda: (0, 0, 0),
            "m2": lambda: (m[1], 0, 0),
            "f2": lambda: (m[1], -s, 0),
            "m3": lambda: (m[1], m[2], 0),
            "f3": lambda: (m[1], m[2], -s),
        }[m[0]]()
        target = view(x, colour, where, whole(colour))
        return pltpu.make_async_remote_copy(
            src_ref=own.at[:, whole(colour)] if where == (0, 0, 0) else target,
            dst_ref=target,
            send_sem=ag_send.at[colour, int(m[0][1]) - 1],
            recv_sem=receive_sem.at[GATHER_SLOT[colour, gather_group(m)[0]]],
            device_id=(peers[d, s],),
            device_id_type=MESH,
        )

    def gather_wait(colour, name):
        size = gather_size(name)
        cols = whole(colour)
        ref = {16: x.at[0, :, :, :, cols], 8: x.at[0, pl.ds(0, 2), :, :, cols]}.get(
            size, x.at[0, 0, 0, :, cols]
        )
        await_bytes(ref, receive_sem.at[GATHER_SLOT[colour, name]])
        return size

    def ids_send(level):
        at = dict(pos)
        for axis in "xyz"[:level]:
            at[axis] = slice(None)
        target = ids_all.at[at["z"], at["y"], at["x"]]
        for s in (1, -1, 2):
            pltpu.make_async_remote_copy(
                src_ref=target if level else ids_own,
                dst_ref=target,
                send_sem=id_send.at[level],
                recv_sem=id_recv.at[level],
                device_id=(peers["xyz"[level], s],),
                device_id_type=MESH,
            ).start()

    def three(level):
        three = pl.ds(0, 3)
        return (ids_all.at[0, 0, three], ids_all.at[0, three], ids_all.at[three])[level]

    def ids_receive(level):
        await_bytes(three(level), id_recv.at[level])

    first = me - core

    def slab_of(ref, d, k, cols):
        i = near[d][k]
        if d == "z":
            return ref[i, :, :, :, cols]
        if d == "y":
            return ref[:, i, :, :, cols]
        return ref[:, :, i, :, cols]

    def slab_store(ref, d, k, cols, values):
        i = near[d][k]
        values = values.reshape(4, 4, 16, values.shape[-1])
        if d == "z":
            ref[i, :, :, :, cols] = values
        elif d == "y":
            ref[:, i, :, :, cols] = values
        else:
            ref[:, :, i, :, cols] = values

    tables = {}

    def read_ids():
        table = ids_all[:, :, :, pl.ds(0, 1), :].reshape(64, 128)
        all_gates = ids_all[:, :, :, pl.ds(1, 1), :].reshape(64, 128)
        lane = lax.broadcasted_iota(jnp.int32, (64, 128), 1)
        sender = lax.broadcasted_iota(jnp.int32, (64, 128), 0)
        found, gates = [], []
        for e in range(2):
            for k in range(2):
                wanted = (first + e + 128 * k).astype(F32)
                hit = (table == wanted) & (lane < 96)
                row = jnp.where(hit, lax.rem(lane, 16) + 16 * sender, -1)
                found.append(jnp.max(row.astype(F32), axis=1, keepdims=True))
                gates.append(jnp.sum(jnp.where(hit, all_gates, 0.0), axis=1, keepdims=True))
        code = jnp.concatenate(found, axis=0)
        tables["code"] = code
        tables["gates"] = jnp.concatenate(gates, axis=0)
        wide = jnp.broadcast_to(code, (256, 256))
        diagonal = lax.broadcasted_iota(jnp.int32, (256, 256), 0) == lax.broadcasted_iota(
            jnp.int32, (256, 256), 1
        )
        across = jnp.sum(jnp.where(diagonal, wide, 0.0), axis=0, keepdims=True)
        tables["across"] = across

    def slots_by_rows(z):
        number = z * 256 + lax.broadcasted_iota(jnp.int32, (256, 256), 0)
        hot = jnp.where(number.astype(F32) == tables["across"], 1.0, 0.0).astype(BF16)
        hc[z, :, :, :, pl.ds(128, 256)] = hot.reshape(4, 4, 16, 256)

    def slab_rows(colour, ks):
        d, cols = ORDERS[colour][2], whole(colour)
        slabs = [slab_of(x, d, k, cols).reshape(256, COLS[colour][1]) for k in ks]
        return jnp.concatenate(slabs, axis=0) if len(slabs) > 1 else slabs[0]

    def use_hidden(colour, ks):
        d = ORDERS[colour][2]
        every = pl.ds(0, 256)
        products = dot(slab_rows(colour, ks), w_turned[whole(colour), :])
        for i, k in enumerate(ks):
            total = slab_of(sums, d, k, every).reshape(256, 256)
            slab_store(sums, d, k, every, total + products[256 * i : 256 * i + 256])

    def use_pick(colour, ks):
        d = ORDERS[colour][2]
        cols = whole(colour)
        lane = lax.broadcasted_iota(jnp.int32, (1, 256), 1)
        a, b, r = lane // 64, lax.rem(lane // 16, 4), lax.rem(lane, 16)
        hots = []
        for k in ks:
            i = near[d][k]
            if d == "z":
                sender = i * 16 + a * 4 + b
            elif d == "y":
                sender = a * 16 + i * 4 + b
            else:
                sender = a * 16 + b * 4 + i
            number = (sender * 16 + r).astype(F32)
            hots.append(jnp.where(tables["code"] == number, 1.0, 0.0).astype(BF16))
        hot = jnp.concatenate(hots, axis=1) if len(hots) > 1 else hots[0]
        rows = dot(hot, slab_rows(colour, ks))
        if ks == (0,):
            picking[:, cols] = rows
        else:
            picking[:, cols] += rows


    experts_in = {}

    def turn_weights():
        weights_wait(0)
        for i in range(8):
            part = pl.ds(256 * i, 256)
            w_turned[part, :] = w_in[:, part].T

    def use_columns(colour):
        start, width = COLS[colour]
        cols = pl.ds(start, width)
        rows = picking[:, cols].astype(BF16)
        parts = []
        for e in range(2):
            mine = rows[e * 128 : (e + 1) * 128]
            parts += [dot(mine, eg[e, cols, :]), dot(mine, eu[e, cols, :])]
        for i, part in enumerate(parts):
            experts_in[i] = experts_in[i] + part if i in experts_in else part

    done = 0
    tasks = [
        (0, lambda: (write_words(), ids_send(0))),
        (14, lambda: (ids_receive(0), ids_send(1))),
        (24, turn_weights),
        (44, lambda: (ids_receive(1), ids_send(2))),
    ]
    more = swaps[7:]
    for action, c, m in GATHER_STEPS:
        if action == "task":
            name, *what = c
            if name == "ids":
                ids_receive(2)
                read_ids()
            elif name == "rows":
                slots_by_rows(*what)
            elif name == "hidden":
                use_hidden(*what)
            elif name == "pick":
                use_pick(*what)
            else:
                if not experts_in:
                    weights_wait(1)
                    weights_wait(2)
                use_columns(*what)
            continue
        if action != "receive":
            send(action, gather_copy(c, m))
            continue
        while tasks and done >= tasks[0][0]:
            tasks.pop(0)[1]()
        if more and done >= 12 * (8 - len(more)):
            more.pop(0).start()
        done += gather_wait(c, m)
    weights_wait(3)


    for zi in range(4):
        products = sums[zi].reshape(256, 256)
        words = jnp.broadcast_to(ids_all[zi, :, :, pl.ds(0, 1), :], (4, 4, 16, 128)).reshape(256, 128)
        lane = lax.broadcasted_iota(jnp.int32, (256, 128), 1)
        row = lax.broadcasted_iota(jnp.int32, (256, 128), 0)
        own_word = lane == 96 + lax.rem(row, 16)
        scale = jnp.sum(jnp.where(own_word, words, 0.0), axis=1, keepdims=True)
        hidden = (scale * jax.nn.silu(products[:, :128]) * products[:, 128:]).astype(BF16)
        hc[zi, :, :, :, pl.ds(0, 128)] = hidden.reshape(4, 4, 16, 128)

    for e in range(2):
        hidden = (jax.nn.silu(experts_in[2 * e]) * experts_in[2 * e + 1]).astype(BF16)
        result = dot(hidden, ed[e])
        weighted = result * tables["gates"][e * 128 : (e + 1) * 128]
        w_out[pl.ds(128 + e * 128, 128), :] = weighted.astype(BF16)

    def landing(colour, m):
        cols = pl.ds(0, COLS[colour][1])
        i = {1: 0, -1: 1, 2: 2}
        if m[0] == "m1":
            return r1.at[colour, i[m[1]], :, cols]
        if m[0] == "m2":
            return r2.at[colour, i[m[2]], m[1], :, cols]
        if m[0] == "f2":
            return r2.at[colour, 2, m[1], :, cols]
        if m[0] == "m3":
            return r3.at[colour, i[m[3]], m[1], m[2], :, cols]
        return r3.at[colour, 2, m[1], m[2], :, cols]

    def scatter_copy(colour, m):
        d, s = link_of(colour, m)
        where = {
            "m1": lambda: (-s, 0, 0),
            "m2": lambda: (m[1], -s, 0),
            "f2": lambda: (m[1], 2, 0),
            "m3": lambda: (m[1], m[2], -s),
            "f3": lambda: (m[1], m[2], 2),
        }[m[0]]()
        return pltpu.make_async_remote_copy(
            src_ref=view(p, colour, where, whole(colour)),
            dst_ref=landing(colour, m),
            send_sem=rs_send.at[colour, int(m[0][1]) - 1],
            recv_sem=receive_sem.at[SCATTER_SLOT[colour, scatter_group(m)[0]]],
            device_id=(peers[d, s if s == 2 else -s],),
            device_id_type=MESH,
        )

    def scatter_wait(colour, name):
        cols = pl.ds(0, COLS[colour][1])
        two = pl.ds(0, 2)
        if name[0] == "m1":
            ref = r1.at[colour, :, :, cols]
        elif name[0] == "m2":
            ref = r2.at[colour, two, name[1], :, cols]
        elif name[0] == "m3":
            ref = r3.at[colour, two, name[1], name[2], :, cols]
        else:
            ref = landing(colour, name)
        await_bytes(ref, receive_sem.at[SCATTER_SLOT[colour, name]])

    def product(colour, ks):
        d, cols = ORDERS[colour][2], whole(colour)
        left = [slab_of(hc, d, k, pl.ds(0, 384)).reshape(256, 384) for k in ks]
        left = jnp.concatenate(left, axis=0) if len(left) > 1 else left[0]
        values = dot(left, w_out[:, cols]).astype(BF16)
        for i, k in enumerate(ks):
            slab_store(p, d, k, cols, values[256 * i : 256 * i + 256])

    def add(colour, where, *messages):
        ref = view(p, colour, where, whole(colour))
        total = ref[...].astype(F32)
        for m in messages:
            total = total + landing(colour, m)[...].astype(F32)
        ref[...] = total.astype(BF16)

    done = 0
    for action, *what in SCATTER_STEPS:
        if action == "product":
            product(*what)
            continue
        c, m = what
        if action != "receive":
            send(action, scatter_copy(c, m))
            continue
        done += 1
        scatter_wait(c, m)
        if m[0] == "f3":
            add(c, (m[1], m[2], -sign_of(m[2])), m)
        elif m[0] == "f2":
            add(c, (m[1], -sign_of(m[1]), 0), m)
        elif m[0] == "m3":
            add(c, (m[1], m[2], 0), (*m, 1), (*m, -1))
        elif m[0] == "m2":
            add(c, (m[1], 0, 0), (*m, 1), (*m, -1))
    for c in range(3):
        start, width = COLS[c]
        cols = pl.ds(start, width)
        total = resid_ref[:, cols].astype(F32) + view(p, c, (0, 0, 0), cols)[...].astype(F32)
        for k in range(3):
            total = total + r1[c, k, :, pl.ds(0, width)].astype(F32)
        out_ref[:, cols] = total.astype(BF16)

    for level in range(3):
        await_bytes(three(level), id_send.at[level])
    for i in range(4):
        await_bytes(swapped[i], swap_send.at[i])
    for c in range(3):
        cols = whole(c)
        three_blocks = pl.ds(0, 3)
        sent = (
            x.at[0, 0, three_blocks, :, cols],
            x.at[0, three_blocks, :, :, cols],
            x.at[three_blocks, :, :, :, cols],
        )
        for i in range(3):
            await_bytes(sent[i], ag_send.at[c, i])
            await_bytes(sent[i], rs_send.at[c, i])


def finish_kernel(rows_ref, state_ref, rows_out, state_out, sem):
    copies = (
        pltpu.make_async_copy(rows_ref, rows_out, sem.at[0]),
        pltpu.make_async_copy(state_ref, state_out, sem.at[1]),
    )
    for copy in copies:
        copy.start()
    for copy in copies:
        copy.wait()


def finish(rows, state):
    return pl.pallas_call(
        finish_kernel,
        out_shape=(
            jax.ShapeDtypeStruct(rows.shape, rows.dtype),
            jax.ShapeDtypeStruct(state.shape, state.dtype),
        ),
        in_specs=[pl.BlockSpec(memory_space=pltpu.VMEM)] * 2,
        out_specs=[pl.BlockSpec(memory_space=pl.ANY)] * 2,
        scratch_shapes=[pltpu.SemaphoreType.DMA((2,))],
        compiler_params=pltpu.CompilerParams(vmem_limit_bytes=4 * 1024 * 1024),
    )(rows, state)


def on_device(
    tokens,
    state,
    norm_mix,
    w_drive,
    lam_real,
    lam_imag,
    log_step,
    b_real,
    b_imag,
    readout_real,
    readout_imaginary,
    d_skip,
    w_value,
    w_glugate,
    w_output,
    norm_ffn,
    w_group,
    w_expert,
    route_ids,
    expert_gate,
    expert_up,
    expert_down,
    dense_vector,
    dense_gate,
    dense_up,
    dense_down,
):
    vmem = pl.BlockSpec(memory_space=pltpu.VMEM)
    hbm = pl.BlockSpec(memory_space=pltpu.HBM)
    rows, new_state = pl.pallas_call(
        layer_kernel,
        out_shape=(
            jax.ShapeDtypeStruct((16, 2048), BF16),
            jax.ShapeDtypeStruct((2, 16, 2048), F32),
        ),
        in_specs=[hbm] * 26,
        out_specs=(vmem, vmem),
        scratch_shapes=[
            pltpu.VMEM((16, 2048), BF16),
            pltpu.VMEM((2, 16, 2048), F32),
            pltpu.VMEM((3, 1, 2048), F32),
            pltpu.VMEM((2048, 512), BF16),
            pltpu.VMEM((2, 32, 64), F32),
            pltpu.VMEM((1, 32), F32),
            pltpu.VMEM((4, 32, 16, 64), F32),
            pltpu.VMEM((1, 512), F32),
            pltpu.VMEM((2, 512, 512), BF16),
            pltpu.VMEM((512, 2048), BF16),
            pltpu.VMEM((4, 2048), BF16),
            pltpu.VMEM((2048, 128), BF16),
            pltpu.VMEM((6, 16), jnp.int32),
            pltpu.VMEM((4, 128, 512), BF16),
            pltpu.VMEM((4, 128, 512), BF16),
            pltpu.VMEM((4, 128, 512), BF16),
            pltpu.VMEM((4, 128, 512), BF16),
            pltpu.VMEM((2, 2048), F32),
            pltpu.VMEM((16, 2048), BF16),
            pltpu.VMEM((16, 2048), BF16),
            pltpu.VMEM((4, 4, 4, 16, 2048), BF16),
            pltpu.VMEM((256, 2048), BF16),
            pltpu.VMEM((384, 2048), BF16),
            pltpu.VMEM((2, 2048, 512), BF16),
            pltpu.VMEM((2, 2048, 512), BF16),
            pltpu.VMEM((2, 512, 2048), BF16),
            pltpu.VMEM((4, 4, 4, 2, 128), F32),
            pltpu.VMEM((2, 128), F32),
            pltpu.VMEM((4, 4, 4, 16, 256), F32),
            pltpu.VMEM((4, 4, 4, 16, 384), BF16),
            pltpu.VMEM((256, 2048), F32),
            pltpu.VMEM((2048, 256), BF16),
            pltpu.VMEM((4, 4, 4, 16, 2048), BF16),
            pltpu.VMEM((3, 3, 16, 768), BF16),
            pltpu.VMEM((3, 3, 4, 16, 768), BF16),
            pltpu.VMEM((3, 3, 4, 4, 16, 768), BF16),
            pltpu.SemaphoreType.DMA((13,)),
            pltpu.SemaphoreType.DMA((4,)),
            pltpu.SemaphoreType.DMA((4,)),
            pltpu.SemaphoreType.DMA((4,)),
            pltpu.SemaphoreType.DMA((3,)),
            pltpu.SemaphoreType.DMA((3,)),
            pltpu.SemaphoreType.DMA((3, 3)),
            pltpu.SemaphoreType.DMA((3, 3)),
            pltpu.SemaphoreType.DMA((RECEIVE_SLOTS,)),
        ],
        compiler_params=pltpu.CompilerParams(
            collective_id=0, has_side_effects=True, vmem_limit_bytes=47 * 1024 * 1024
        ),
        cost_estimate=pl.CostEstimate(
            flops=8_000_000_000, bytes_accessed=20_000_000, transcendentals=0
        ),
    )(*[pltpu.with_memory_space_constraint(a, pltpu.HBM) for a in (
        tokens,
        state,
        norm_mix.reshape(1, -1),
        w_drive,
        lam_real,
        lam_imag,
        log_step.reshape(1, -1),
        jnp.transpose(b_real, (0, 2, 1)),
        jnp.transpose(b_imag, (0, 2, 1)),
        readout_real,
        readout_imaginary,
        d_skip.reshape(1, -1),
        w_value,
        w_glugate,
        w_output,
        norm_ffn.reshape(1, -1),
        jnp.transpose(w_group),
        w_expert,
        jnp.transpose(route_ids),
        dense_vector.reshape(1, -1),
        jnp.transpose(dense_gate),
        jnp.transpose(dense_up),
        dense_down,
        expert_gate[0],
        expert_up[0],
        expert_down[0],
    )])
    return finish(rows, new_state)


def solution(mesh):
    placed = (
        P("ep", None),
        P(None, "ep", None),
        P(),
        P(),
        P(),
        P(),
        P(),
        P(),
        P(),
        P(),
        P(),
        P(),
        P(),
        P(),
        P(),
        P(),
        P(),
        P(),
        P("ep", None),
        P("ep", None, None),
        P("ep", None, None),
        P("ep", None, None),
        P(),
        P(None, "ep"),
        P(None, "ep"),
        P("ep", None),
    )
    return jax.shard_map(
        on_device,
        mesh=mesh,
        in_specs=placed,
        out_specs=(P("ep", None), P(None, "ep", None)),
        check_vma=False,
    )
```

```python
import heapq

import jax
import jax.numpy as jnp
from jax import lax
from jax.experimental import pallas as pl
from jax.experimental.pallas import tpu as pltpu
from jax.sharding import PartitionSpec as P

EPS = 1e-05
F32 = jnp.float32
BF16 = jnp.bfloat16
MESH = pl.DeviceIdType.MESH
ORDERS = (("x", "y", "z"), ("y", "z", "x"), ("z", "x", "y"))
COLS = ((0, 640), (640, 640), (1280, 768))
RATE, DELAY, STEP = 46700.0, 2.9, 0.36
GATHER_AHEAD, SCATTER_AHEAD = (1.0, 0.3), (0.6, 0.3)
SLACK = 0.4


def sign_of(offset):
    return 1 if offset in (0, 1) else -1


def link_of(c, m):
    phase = int(m[0][1]) - 1
    return ORDERS[c][phase], m[-1] if m[0] in ("m1", "m2", "m3") else sign_of(m[-1])


def bytes_of(c, m):
    return 32.0 * COLS[c][1] * (2 if m == ("m1", 2) else 1)


def queue_of(c, m):
    d, s = link_of(c, m)
    return d, 1 if s == 2 else s


def gather_group(m):
    if m[0] == "f3":
        return ("f3",), 16
    if m[0] == "m3" and sign_of(m[2]) != m[3]:
        return ("m3", m[3]), 8
    return m, 1


def scatter_group(m):
    if m[0] in ("m2", "m3"):
        return m[:-1], 2
    return (("m1",), 3) if m[0] == "m1" else (m, 1)


def grouped(steps, group):
    seen, out = {}, []
    for _, _, kind, what in sorted(steps, key=lambda step: step[:2]):
        if kind == "receive":
            name, size = group(what[1])
            key = (what[0], name)
            seen[key] = seen.get(key, 0) + 1
            if seen[key] < size:
                continue
            what = key
        out.append((kind, *what))
    merged, place = [], {}
    since = 0
    for step in out:
        if not step[0].startswith("send"):
            since = len(merged)
        elif place.get(step[1:], -1) >= since:
            merged[place[step[1:]]] = ("send", *step[1:])
            continue
        else:
            place[step[1:]] = len(merged)
        merged.append(step)
    return merged


def simulate(first, react, rank, aheads):
    queue, waiting, free, count = [], {}, {}, 0
    sent, came, ready = {}, {}, {}

    def push(t, kind, item):
        nonlocal count
        count += 1
        heapq.heappush(queue, (t, count, kind, item))

    for t, items in first:
        for item in items:
            push(t, "ready", item)
    while queue:
        t, _, kind, item = heapq.heappop(queue)
        if kind == "ready":
            ready[item] = t
            count += 1
            heapq.heappush(waiting.setdefault(queue_of(*item), []), (rank(item), count, item))
            links = [queue_of(*item)]
        elif kind == "free":
            links = [item]
        else:
            came[item] = t
            links = []
            for new in react(item):
                push(t, "ready", new)
        for k in links:
            if free.get(k, 0.0) <= t + 1e-9 and waiting.get(k):
                _, _, m = heapq.heappop(waiting[k])
                free[k] = t + bytes_of(*m) / RATE
                sent[m] = t
                push(free[k], "free", k)
                push(free[k] + (DELAY + 0.8 if m[1] == ("m1", 2) else DELAY), "came", m)
    steps = [(t, 0, "receive", m) for m, t in came.items()]
    for core, ahead in enumerate(aheads):
        steps += [(max(ready[m], t - ahead), 1, "send%d" % core, m) for m, t in sent.items()]
    return steps, sent


def plan_gather():
    def present(c, o, q):
        new = [(c, ("m2", o, 1)), (c, ("m2", o, -1))] if q == 0 else []
        return new + [(c, ("m3", o, q, 1)), (c, ("m3", o, q, -1))]

    def react(item):
        c, m = item
        if m[0] == "m1":
            return present(c, {1: 3, -1: 1, 2: 2}[m[1]], 0)
        if m[0] == "m2":
            o, s = m[1:]
            new = [(c, ("f2", o))] if sign_of(o) == s else []
            return new + present(c, o, 3 if s == 1 else 1)
        if m[0] == "f2":
            return present(c, m[1], 2)
        if m[0] == "m3" and sign_of(m[2]) == m[3]:
            return [(c, ("f3", m[1], m[2]))]
        return []

    start = [(c, ("m1", s)) for s in (1, -1, 2) for c in range(3)]
    for c in range(3):
        start += present(c, 0, 0)
    rank = {"m1": 0, "m2": 1, "f2": 1, "m3": 2, "f3": 3}
    steps, sent = simulate([(0.0, start)], react, lambda item: rank[item[1][0]], GATHER_AHEAD)
    return with_tasks(grouped(steps, gather_group)), sent


def plan_scatter(sent):
    seen = {}

    def react(item):
        c, m = item

        def both(key):
            seen[c, key] = seen.get((c, key), 0) + 1
            return seen[c, key] == 2

        def level2(o, q):
            if q == 2:
                return [(c, ("f2", o))]
            if q == 0:
                return level1(o)
            s = -1 if q == 1 else 1
            return [(c, ("m2", o, s))] if sign_of(o) != s or both(("m2", o, s)) else []

        def level1(o):
            seen[c, "sum", o] = seen.get((c, "sum", o), 0) + 1
            if seen[c, "sum", o] < 3:
                return []
            return [(c, ("m1", {1: -1, 2: 2, 3: 1}[o]))] if o else []

        if m[0] == "f3":
            s = sign_of(m[2])
            return [(c, ("m3", m[1], m[2], s))] if both(("m3",) + m[1:] + (s,)) else []
        if m[0] == "m3":
            return level2(m[1], m[2]) if both(("sum3",) + m[1:3]) else []
        if m[0] == "f2":
            s = sign_of(m[1])
            return [(c, ("m2", m[1], s))] if both(("m2", m[1], s)) else []
        if m[0] == "m2":
            return level1(m[1])
        return []

    first, products, t = [], [], 0.0
    pairs = [(o, q) for o in range(4) for q in range(4)]
    for ks in ((2,), (3, 1), (0,)):
        for c in range(3):
            products.append((t, 0, "product", (c, ks)))
            t += STEP * (0.5 + 0.5 * len(ks))
            if ks == (2,):
                first.append((t, [(c, ("f3", o, q)) for o, q in pairs]))
            for k in (1, 3):
                if k in ks:
                    s = -1 if k == 1 else 1
                    free = [(c, ("m3", o, q, s)) for o, q in pairs if sign_of(q) != s]
                    first.append((t, free))
                    for o, q in pairs:
                        if sign_of(q) == s:
                            seen[c, ("m3", o, q, s)] = 1
    last = max(sent.values())
    steps, _ = simulate(first, react, lambda item: last - sent[item], SCATTER_AHEAD)
    return grouped(steps + products, scatter_group)


def with_tasks(steps):
    free, came, out, waiting, arrived = {}, {}, [], [], {}
    t, done = 0.0, 0
    sends = sum(step[0] in ("send", "send0") for step in steps)
    held = [(("ids",), 0.3)] + [(("rows", z), 0.1) for z in range(4)]
    for step in steps:
        kind, c, m = step
        if kind != "receive":
            if kind != "send1":
                k = queue_of(c, m)
                free[k] = max(t, free.get(k, 0.0)) + bytes_of(c, m) / RATE
                key = (c, gather_group(m)[0])
                came[key] = max(came.get(key, 0.0), free[k] + DELAY)
                sends -= 1
            out.append(step)
            continue
        if done >= 84:
            waiting += held
            held = []
        while waiting and (sends == 0 or t + waiting[0][1] <= came[c, m] + SLACK):
            task, cost = waiting.pop(0)
            out.append(("task", task, None))
            t += cost
        t = max(t, came[c, m])
        out.append(step)
        size = gather_size(m)
        done += size
        k = 2 if m[0] == "f3" else (3 if m[-1] == 1 else 1) if m[0] == "m3" else 0
        arrived[c, k] = arrived.get((c, k), 1 if k == 0 else 0) + size
        if arrived[c, k] == 16 and (k in (0, 2) or arrived.get((c, 4 - k)) == 16):
            both = (1, 3) if k in (1, 3) else (k,)
            waiting.append((("hidden", c, both), 0.3 * len(both)))
            held.append((("pick", c, both), 0.3 * len(both)))
            if k == 2:
                held.append((("columns", c), 0.8))
    return out + [("task", task, None) for task, _ in waiting + held]


def gather_size(name):
    if name[0] == "f3":
        return 16
    return 8 if name[0] == "m3" and len(name) == 2 else 1


def numbered(group):
    one = [("m1", s) for s in (1, -1, 2)]
    two = [("m2", o, s) for o in range(4) for s in (1, -1)] + [("f2", o) for o in range(4)]
    pairs = [(o, q) for o in range(4) for q in range(4)]
    three = [("m3", o, q, s) for o, q in pairs for s in (1, -1)] + [("f3", o, q) for o, q in pairs]
    names = dict.fromkeys(group(m)[0] for m in one + two + three)
    return {name: i for i, name in enumerate(names)}


def receive_slots(steps):
    names = [(c, name) for c in range(3) for name in numbered(gather_group)]
    gather = {key: i for i, key in enumerate(names)}
    last = {}
    for at, (kind, c, m) in enumerate(steps):
        if kind.startswith("send") and link_of(c, m)[1] != 2:
            for core in (0, 1):
                if kind in ("send", "send%d" % core):
                    last[core, link_of(c, m)] = at
    waited = [(at, gather[step[1:]]) for at, step in enumerate(steps) if step[0] == "receive"]
    limits = []
    for c in range(3):
        for name in numbered(scatter_group):
            if name[0] == "m1":
                limits.append((-1, c, name))
                continue
            d = ORDERS[c][int(name[0][1]) - 1]
            ways = (sign_of(name[-1]),) if name[0] in ("f2", "f3") else (1, -1)
            limits.append((min(last[core, (d, s)] for core in (0, 1) for s in ways), c, name))
    scatter, count = {}, len(gather)
    for limit, c, name in sorted(limits):
        fit = [pair for pair in waited if pair[0] < limit]
        if fit:
            waited.remove(fit[-1])
            scatter[c, name] = fit[-1][1]
        else:
            scatter[c, name] = count
            count += 1
    return gather, scatter, count


GATHER_STEPS, GATHER_SENT = plan_gather()
SCATTER_STEPS = plan_scatter(GATHER_SENT)
GATHER_SLOT, SCATTER_SLOT, RECEIVE_SLOTS = receive_slots(GATHER_STEPS)


def dot(a, b):
    return jnp.dot(a, b, preferred_element_type=F32)


def dot_nt(a, b):
    return lax.dot_general(a, b, (((1,), (1,)), ((), ())), preferred_element_type=F32)


def layer_kernel(
    tokens_hbm,
    state_hbm,
    norm_mix_hbm,
    w_drive_hbm,
    lam_real_hbm,
    lam_imag_hbm,
    log_step_hbm,
    b_real_hbm,
    b_imag_hbm,
    readout_real_hbm,
    readout_imag_hbm,
    d_skip_hbm,
    w_value_hbm,
    w_glugate_hbm,
    w_output_hbm,
    norm_ffn_hbm,
    group_hbm,
    router_hbm,
    ids_hbm,
    vector_hbm,
    gate_hbm,
    up_hbm,
    down_hbm,
    eg_hbm,
    eu_hbm,
    ed_hbm,
    out_ref,
    state_out,
    tokens_ref,
    state_ref,
    norms_ref,
    w_drive_ref,
    lam_ref,
    log_step_ref,
    maps_ref,
    d_skip_ref,
    glu_ref,
    w_output_ref,
    group_ref,
    router_ref,
    ids_ref,
    input_re,
    input_im,
    readout_re,
    readout_im,
    decay_rows,
    resid_ref,
    own,
    x,
    w_in,
    w_out,
    eg,
    eu,
    ed,
    ids_all,
    ids_own,
    sums,
    hc,
    picking,
    w_turned,
    p,
    r1,
    r2,
    r3,
    load_sem,
    local_sem,
    swap_send,
    swap_recv,
    id_send,
    id_recv,
    ag_send,
    rs_send,
    receive_sem,
):
    me = lax.axis_index("ep")
    core = lax.rem(me, 2)
    pos = {"x": lax.rem(me // 2, 4), "y": lax.rem(me // 8, 4), "z": me // 32}
    near = {d: [lax.rem(pos[d] + k, 4) for k in range(4)] for d in "xyz"}

    def device(at):
        return ((at["z"] * 4 + at["y"]) * 4 + at["x"]) * 2 + core

    def neighbour(d, s):
        at = dict(pos)
        at[d] = near[d][s % 4]
        return device(at)

    peers = {(d, s): neighbour(d, s) for d in "xyz" for s in (1, -1, 2)}
    partner = me + 1 - 2 * core

    barrier = pltpu.get_barrier_semaphore()
    for peer in [*peers.values(), partner]:
        pl.semaphore_signal(barrier, inc=1, device_id=(peer,), device_id_type=MESH)

    def send(action, copy):
        if action == "send":
            copy.start()
            return

        @pl.when(core == int(action[-1]))
        def _():
            copy.start()

    def await_bytes(ref, semaphore):
        pltpu.make_async_copy(ref, ref, semaphore).wait()

    loads = (
        ((lam_real_hbm, lam_imag_hbm), lam_ref),
        ((log_step_hbm,), log_step_ref),
        ((b_real_hbm, b_imag_hbm, readout_real_hbm, readout_imag_hbm), maps_ref),
        ((tokens_hbm,), tokens_ref),
        ((norm_mix_hbm, norm_ffn_hbm, vector_hbm), norms_ref),
        ((w_drive_hbm,), w_drive_ref),
        ((state_hbm,), state_ref),
        ((d_skip_hbm,), d_skip_ref),
        ((w_value_hbm, w_glugate_hbm), glu_ref),
        ((w_output_hbm,), w_output_ref),
        ((ids_hbm,), ids_ref),
        ((group_hbm,), group_ref),
        ((router_hbm,), router_ref),
    )
    for i, (sources, target) in enumerate(loads):
        for j, source in enumerate(sources):
            part = target.at[j] if len(sources) > 1 else target
            pltpu.make_async_copy(source, part, load_sem.at[i]).start()

    def loaded(begin, end):
        for i in range(begin, end):
            await_bytes(loads[i][1], load_sem.at[i])

    def rows(i):
        return pl.ds(pl.multiple_of(i * 64, 64), 64)

    weights = [
        (gate_hbm, w_in.at[rows(core)]),
        (up_hbm, w_in.at[rows(2 + core)]),
        (down_hbm, w_out.at[rows(core)]),
        (eg_hbm, eg.at[core]),
        (eu_hbm, eu.at[core]),
        (ed_hbm, ed.at[core]),
    ]
    group = (0, 0, 0, 1, 2, 3)
    for i, (s, t) in zip(group, weights):
        pltpu.make_async_copy(s, t, local_sem.at[i]).start()
    pieces = [(0, *pair) for pair in weights[:3]]
    for j, (s, t) in enumerate(weights[3:]):
        depth = s.shape[0] // 4
        for i in range(4):
            part = pl.ds(i * depth, depth)
            pieces.append((1 + j, s.at[part], t.at[part]))
    swaps = [
        pltpu.make_async_remote_copy(
            src_ref=s,
            dst_ref=t,
            send_sem=swap_send.at[i],
            recv_sem=swap_recv.at[i],
            device_id=(partner,),
            device_id_type=MESH,
        )
        for i, s, t in pieces
    ]
    swapped = (w_out.at[pl.ds(0, 192)], eg.at[0], eu.at[0], ed.at[0])

    def weights_wait(i):
        await_bytes(swapped[i], local_sem.at[i])
        await_bytes(swapped[i], swap_recv.at[i])

    for ref in (input_re, input_im, readout_re, readout_im):
        ref[...] = jnp.zeros((4, 128, 512), BF16)
    loaded(0, 3)
    square = lax.broadcasted_iota(jnp.int32, (32, 32), 0) == lax.broadcasted_iota(
        jnp.int32, (32, 32), 1
    )
    time_step = jnp.sum(
        jnp.where(square, jnp.exp(log_step_ref[...]), 0.0), axis=1, keepdims=True
    )
    lam_re = lam_ref[0]
    lam_im = lam_ref[1]
    magnitude = jnp.exp(lam_re * time_step)
    decay_re = magnitude * jnp.cos(lam_im * time_step)
    decay_im = magnitude * jnp.sin(lam_im * time_step)
    modulus = lam_re * lam_re + lam_im * lam_im
    factor_re = ((decay_re - 1.0) * lam_re + decay_im * lam_im) / modulus
    factor_im = (decay_im * lam_re - (decay_re - 1.0) * lam_im) / modulus
    for g in range(32):
        q, j = divmod(g, 8)
        at = (q, pl.ds(16 * j, 16), pl.ds(64 * j, 64))
        f_re = factor_re[g : g + 1]
        f_im = factor_im[g : g + 1]
        b_re = maps_ref[0, g]
        b_im = maps_ref[1, g]
        input_re[at] = (f_re * b_re - f_im * b_im).astype(BF16)
        input_im[at] = (f_re * b_im + f_im * b_re).astype(BF16)
        readout_re[at] = maps_ref[2, g].astype(BF16)
        readout_im[at] = maps_ref[3, g].astype(BF16)
        lane = pl.ds(64 * g, 64)
        decay_rows[pl.ds(0, 1), lane] = decay_re[g : g + 1]
        decay_rows[pl.ds(1, 1), lane] = decay_im[g : g + 1]

    pl.semaphore_wait(barrier, 10)
    for copy in swaps[:7]:
        copy.start()


    def rms_scale(values, gain):
        mean = jnp.mean(values * values, axis=1, keepdims=True)
        return (values * lax.rsqrt(mean + EPS) * gain).astype(BF16)

    loaded(3, 6)
    tokens = tokens_ref[...].astype(F32)
    drive = dot(rms_scale(tokens, norms_ref[0]), w_drive_ref[...]).astype(BF16)
    loaded(6, 8)
    projected = []
    for q in range(4):
        channels = drive[:, 128 * q : 128 * q + 128]
        cols = pl.ds(512 * q, 512)
        old_re = state_ref[0, :, cols]
        old_im = state_ref[1, :, cols]
        d_re = decay_rows[pl.ds(0, 1), cols]
        d_im = decay_rows[pl.ds(1, 1), cols]
        new_re = d_re * old_re - d_im * old_im + dot(channels, input_re[q])
        new_im = d_re * old_im + d_im * old_re + dot(channels, input_im[q])
        state_out[0, :, cols] = new_re
        state_out[1, :, cols] = new_im
        projected.append(
            dot_nt(new_re.astype(BF16), readout_re[q]) - dot_nt(new_im.astype(BF16), readout_im[q])
        )
    skipped = d_skip_ref[...] * drive.astype(F32)
    readout = jax.nn.gelu(jnp.concatenate(projected, axis=1) + skipped).astype(BF16)
    loaded(8, 10)
    value_part = dot(readout, glu_ref[0])
    gate_part = dot(readout, glu_ref[1])
    mixed = (value_part * jax.nn.sigmoid(gate_part)).astype(BF16)
    resid = (tokens + dot(mixed, w_output_ref[...])).astype(BF16)
    resid_ref[...] = resid
    loaded(10, 13)
    normed = rms_scale(resid.astype(F32), norms_ref[1])

    own[...] = normed

    x[pos["z"], pos["y"], pos["x"]] = normed

    def write_words():
        sums[...] = jnp.zeros((4, 4, 4, 16, 256), F32)
        normed = own[...]
        ids = ids_ref[...].astype(F32)
        lanes = lax.broadcasted_iota(jnp.int32, (16, 128), 1)
        down = lax.broadcasted_iota(jnp.int32, (16, 128), 0)
        this = lax.broadcasted_iota(jnp.int32, (16, 16), 0)
        that = lax.broadcasted_iota(jnp.int32, (16, 16), 1)
        hits = []
        columns = []
        for t in range(6):
            column = jnp.sum(jnp.where(this == that, ids[t : t + 1], 0.0), axis=1, keepdims=True)
            columns.append(column)
            hits.append(column == lanes.astype(F32))
        chosen = jnp.zeros((16, 128), F32)
        for hit in hits:
            chosen = chosen + jnp.where(hit, 1.0, 0.0)
        earlier = jnp.where(that < this, 1.0, 0.0)
        ordinal = dot(earlier.astype(BF16), chosen.astype(BF16))
        branch = jax.nn.sigmoid(
            jnp.sum(normed.astype(F32) * norms_ref[2], axis=1, keepdims=True)
        )
        group_exp = jnp.exp(dot_nt(normed, group_ref[...]))
        group_prob = group_exp / jnp.sum(group_exp, axis=1, keepdims=True)
        inner_exp = jnp.exp(dot(normed, router_ref[...]))
        inner_sum = jnp.zeros((16, 128), F32)
        outer = jnp.zeros((16, 128), F32)
        for g in range(4):
            inside = lanes // 32 == g
            total = jnp.sum(jnp.where(inside, inner_exp, 0.0), axis=1, keepdims=True)
            inner_sum = jnp.where(inside, total, inner_sum)
            outer = jnp.where(inside, group_prob[:, g : g + 1], outer)
        inner = inner_exp / inner_sum
        joint = outer * inner
        divisor = jnp.sum(jnp.where(chosen > 0.0, inner, 0.0), axis=1, keepdims=True)
        words = jnp.where(lanes == 96 + down, branch, 0.0)
        gates = jnp.zeros((16, 128), F32)
        for t in range(6):
            place = lanes == 16 * t + down
            rank = jnp.sum(jnp.where(hits[t], ordinal, 0.0), axis=1, keepdims=True)
            gate = jnp.sum(jnp.where(hits[t], joint, 0.0), axis=1, keepdims=True) / divisor
            words = words + jnp.where(place, columns[t] + 128.0 * rank, 0.0)
            gates = gates + jnp.where(place, gate, 0.0)
        words = jnp.sum(words, axis=0, keepdims=True)
        gates = jnp.sum(gates, axis=0, keepdims=True)
        for ref in (ids_own, ids_all.at[pos["z"], pos["y"], pos["x"]]):
            ref[pl.ds(0, 1), :] = words
            ref[pl.ds(1, 1), :] = gates

    def view(ref, colour, offsets, cols):
        at = {}
        for d, o in zip(ORDERS[colour], offsets):
            at[d] = slice(None) if o is None else near[d][o % 4]
        return ref.at[at["z"], at["y"], at["x"], :, cols]

    def whole(colour):
        return pl.ds(*COLS[colour])

    def gather_copy(colour, m):
        d, s = link_of(colour, m)
        where = {
            "m1": lambda: (0, 0, 0),
            "m2": lambda: (m[1], 0, 0),
            "f2": lambda: (m[1], -s, 0),
            "m3": lambda: (m[1], m[2], 0),
            "f3": lambda: (m[1], m[2], -s),
        }[m[0]]()
        target = view(x, colour, where, whole(colour))
        return pltpu.make_async_remote_copy(
            src_ref=own.at[:, whole(colour)] if where == (0, 0, 0) else target,
            dst_ref=target,
            send_sem=ag_send.at[colour, int(m[0][1]) - 1],
            recv_sem=receive_sem.at[GATHER_SLOT[colour, gather_group(m)[0]]],
            device_id=(peers[d, s],),
            device_id_type=MESH,
        )

    def gather_wait(colour, name):
        size = gather_size(name)
        cols = whole(colour)
        ref = {16: x.at[0, :, :, :, cols], 8: x.at[0, pl.ds(0, 2), :, :, cols]}.get(
            size, x.at[0, 0, 0, :, cols]
        )
        await_bytes(ref, receive_sem.at[GATHER_SLOT[colour, name]])
        return size

    def ids_send(level):
        at = dict(pos)
        for axis in "xyz"[:level]:
            at[axis] = slice(None)
        target = ids_all.at[at["z"], at["y"], at["x"]]
        for s in (1, -1, 2):
            pltpu.make_async_remote_copy(
                src_ref=target if level else ids_own,
                dst_ref=target,
                send_sem=id_send.at[level],
                recv_sem=id_recv.at[level],
                device_id=(peers["xyz"[level], s],),
                device_id_type=MESH,
            ).start()

    def three(level):
        three = pl.ds(0, 3)
        return (ids_all.at[0, 0, three], ids_all.at[0, three], ids_all.at[three])[level]

    def ids_receive(level):
        await_bytes(three(level), id_recv.at[level])

    first = me - core

    def slab_of(ref, d, k, cols):
        i = near[d][k]
        if d == "z":
            return ref[i, :, :, :, cols]
        if d == "y":
            return ref[:, i, :, :, cols]
        return ref[:, :, i, :, cols]

    def slab_store(ref, d, k, cols, values):
        i = near[d][k]
        values = values.reshape(4, 4, 16, values.shape[-1])
        if d == "z":
            ref[i, :, :, :, cols] = values
        elif d == "y":
            ref[:, i, :, :, cols] = values
        else:
            ref[:, :, i, :, cols] = values

    tables = {}

    def read_ids():
        table = ids_all[:, :, :, pl.ds(0, 1), :].reshape(64, 128)
        all_gates = ids_all[:, :, :, pl.ds(1, 1), :].reshape(64, 128)
        lane = lax.broadcasted_iota(jnp.int32, (64, 128), 1)
        sender = lax.broadcasted_iota(jnp.int32, (64, 128), 0)
        found, gates = [], []
        for e in range(2):
            for k in range(2):
                wanted = (first + e + 128 * k).astype(F32)
                hit = (table == wanted) & (lane < 96)
                row = jnp.where(hit, lax.rem(lane, 16) + 16 * sender, -1)
                found.append(jnp.max(row.astype(F32), axis=1, keepdims=True))
                gates.append(jnp.sum(jnp.where(hit, all_gates, 0.0), axis=1, keepdims=True))
        code = jnp.concatenate(found, axis=0)
        tables["code"] = code
        tables["gates"] = jnp.concatenate(gates, axis=0)
        wide = jnp.broadcast_to(code, (256, 256))
        diagonal = lax.broadcasted_iota(jnp.int32, (256, 256), 0) == lax.broadcasted_iota(
            jnp.int32, (256, 256), 1
        )
        across = jnp.sum(jnp.where(diagonal, wide, 0.0), axis=0, keepdims=True)
        tables["across"] = across

    def slots_by_rows(z):
        number = z * 256 + lax.broadcasted_iota(jnp.int32, (256, 256), 0)
        hot = jnp.where(number.astype(F32) == tables["across"], 1.0, 0.0).astype(BF16)
        hc[z, :, :, :, pl.ds(128, 256)] = hot.reshape(4, 4, 16, 256)

    def slab_rows(colour, ks):
        d, cols = ORDERS[colour][2], whole(colour)
        slabs = [slab_of(x, d, k, cols).reshape(256, COLS[colour][1]) for k in ks]
        return jnp.concatenate(slabs, axis=0) if len(slabs) > 1 else slabs[0]

    def use_hidden(colour, ks):
        d = ORDERS[colour][2]
        every = pl.ds(0, 256)
        products = dot(slab_rows(colour, ks), w_turned[whole(colour), :])
        for i, k in enumerate(ks):
            total = slab_of(sums, d, k, every).reshape(256, 256)
            slab_store(sums, d, k, every, total + products[256 * i : 256 * i + 256])

    def use_pick(colour, ks):
        d = ORDERS[colour][2]
        cols = whole(colour)
        lane = lax.broadcasted_iota(jnp.int32, (1, 256), 1)
        a, b, r = lane // 64, lax.rem(lane // 16, 4), lax.rem(lane, 16)
        hots = []
        for k in ks:
            i = near[d][k]
            if d == "z":
                sender = i * 16 + a * 4 + b
            elif d == "y":
                sender = a * 16 + i * 4 + b
            else:
                sender = a * 16 + b * 4 + i
            number = (sender * 16 + r).astype(F32)
            hots.append(jnp.where(tables["code"] == number, 1.0, 0.0).astype(BF16))
        hot = jnp.concatenate(hots, axis=1) if len(hots) > 1 else hots[0]
        rows = dot(hot, slab_rows(colour, ks))
        if ks == (0,):
            picking[:, cols] = rows
        else:
            picking[:, cols] += rows


    experts_in = {}

    def turn_weights():
        weights_wait(0)
        for i in range(8):
            part = pl.ds(256 * i, 256)
            w_turned[part, :] = w_in[:, part].T

    def use_columns(colour):
        start, width = COLS[colour]
        cols = pl.ds(start, width)
        rows = picking[:, cols].astype(BF16)
        parts = []
        for e in range(2):
            mine = rows[e * 128 : (e + 1) * 128]
            parts += [dot(mine, eg[e, cols, :]), dot(mine, eu[e, cols, :])]
        for i, part in enumerate(parts):
            experts_in[i] = experts_in[i] + part if i in experts_in else part

    done = 0
    tasks = [
        (0, lambda: (write_words(), ids_send(0))),
        (14, lambda: (ids_receive(0), ids_send(1))),
        (24, turn_weights),
        (44, lambda: (ids_receive(1), ids_send(2))),
    ]
    more = swaps[7:]
    for action, c, m in GATHER_STEPS:
        if action == "task":
            name, *what = c
            if name == "ids":
                ids_receive(2)
                read_ids()
            elif name == "rows":
                slots_by_rows(*what)
            elif name == "hidden":
                use_hidden(*what)
            elif name == "pick":
                use_pick(*what)
            else:
                if not experts_in:
                    weights_wait(1)
                    weights_wait(2)
                use_columns(*what)
            continue
        if action != "receive":
            send(action, gather_copy(c, m))
            continue
        while tasks and done >= tasks[0][0]:
            tasks.pop(0)[1]()
        if more and done >= 12 * (8 - len(more)):
            more.pop(0).start()
        done += gather_wait(c, m)
    weights_wait(3)


    for zi in range(4):
        products = sums[zi].reshape(256, 256)
        words = jnp.broadcast_to(ids_all[zi, :, :, pl.ds(0, 1), :], (4, 4, 16, 128)).reshape(256, 128)
        lane = lax.broadcasted_iota(jnp.int32, (256, 128), 1)
        row = lax.broadcasted_iota(jnp.int32, (256, 128), 0)
        own_word = lane == 96 + lax.rem(row, 16)
        scale = jnp.sum(jnp.where(own_word, words, 0.0), axis=1, keepdims=True)
        hidden = (scale * jax.nn.silu(products[:, :128]) * products[:, 128:]).astype(BF16)
        hc[zi, :, :, :, pl.ds(0, 128)] = hidden.reshape(4, 4, 16, 128)

    for e in range(2):
        hidden = (jax.nn.silu(experts_in[2 * e]) * experts_in[2 * e + 1]).astype(BF16)
        result = dot(hidden, ed[e])
        weighted = result * tables["gates"][e * 128 : (e + 1) * 128]
        w_out[pl.ds(128 + e * 128, 128), :] = weighted.astype(BF16)

    def landing(colour, m):
        cols = pl.ds(0, COLS[colour][1])
        i = {1: 0, -1: 1, 2: 2}
        if m[0] == "m1":
            return r1.at[colour, i[m[1]], :, cols]
        if m[0] == "m2":
            return r2.at[colour, i[m[2]], m[1], :, cols]
        if m[0] == "f2":
            return r2.at[colour, 2, m[1], :, cols]
        if m[0] == "m3":
            return r3.at[colour, i[m[3]], m[1], m[2], :, cols]
        return r3.at[colour, 2, m[1], m[2], :, cols]

    def scatter_copy(colour, m):
        d, s = link_of(colour, m)
        where = {
            "m1": lambda: (-s, 0, 0),
            "m2": lambda: (m[1], -s, 0),
            "f2": lambda: (m[1], 2, 0),
            "m3": lambda: (m[1], m[2], -s),
            "f3": lambda: (m[1], m[2], 2),
        }[m[0]]()
        return pltpu.make_async_remote_copy(
            src_ref=view(p, colour, where, whole(colour)),
            dst_ref=landing(colour, m),
            send_sem=rs_send.at[colour, int(m[0][1]) - 1],
            recv_sem=receive_sem.at[SCATTER_SLOT[colour, scatter_group(m)[0]]],
            device_id=(peers[d, s if s == 2 else -s],),
            device_id_type=MESH,
        )

    def scatter_wait(colour, name):
        cols = pl.ds(0, COLS[colour][1])
        two = pl.ds(0, 2)
        if name[0] == "m1":
            ref = r1.at[colour, :, :, cols]
        elif name[0] == "m2":
            ref = r2.at[colour, two, name[1], :, cols]
        elif name[0] == "m3":
            ref = r3.at[colour, two, name[1], name[2], :, cols]
        else:
            ref = landing(colour, name)
        await_bytes(ref, receive_sem.at[SCATTER_SLOT[colour, name]])

    def product(colour, ks):
        d, cols = ORDERS[colour][2], whole(colour)
        left = [slab_of(hc, d, k, pl.ds(0, 384)).reshape(256, 384) for k in ks]
        left = jnp.concatenate(left, axis=0) if len(left) > 1 else left[0]
        values = dot(left, w_out[:, cols]).astype(BF16)
        for i, k in enumerate(ks):
            slab_store(p, d, k, cols, values[256 * i : 256 * i + 256])

    def add(colour, where, *messages):
        ref = view(p, colour, where, whole(colour))
        total = ref[...].astype(F32)
        for m in messages:
            total = total + landing(colour, m)[...].astype(F32)
        ref[...] = total.astype(BF16)

    done = 0
    for action, *what in SCATTER_STEPS:
        if action == "product":
            product(*what)
            continue
        c, m = what
        if action != "receive":
            send(action, scatter_copy(c, m))
            continue
        done += 1
        scatter_wait(c, m)
        if m[0] == "f3":
            add(c, (m[1], m[2], -sign_of(m[2])), m)
        elif m[0] == "f2":
            add(c, (m[1], -sign_of(m[1]), 0), m)
        elif m[0] == "m3":
            add(c, (m[1], m[2], 0), (*m, 1), (*m, -1))
        elif m[0] == "m2":
            add(c, (m[1], 0, 0), (*m, 1), (*m, -1))
    for c in range(3):
        start, width = COLS[c]
        cols = pl.ds(start, width)
        total = resid_ref[:, cols].astype(F32) + view(p, c, (0, 0, 0), cols)[...].astype(F32)
        for k in range(3):
            total = total + r1[c, k, :, pl.ds(0, width)].astype(F32)
        out_ref[:, cols] = total.astype(BF16)

    for level in range(3):
        await_bytes(three(level), id_send.at[level])
    for i in range(4):
        await_bytes(swapped[i], swap_send.at[i])
    for c in range(3):
        cols = whole(c)
        three_blocks = pl.ds(0, 3)
        sent = (
            x.at[0, 0, three_blocks, :, cols],
            x.at[0, three_blocks, :, :, cols],
            x.at[three_blocks, :, :, :, cols],
        )
        for i in range(3):
            await_bytes(sent[i], ag_send.at[c, i])
            await_bytes(sent[i], rs_send.at[c, i])


def finish_kernel(rows_ref, state_ref, rows_out, state_out, sem):
    copies = (
        pltpu.make_async_copy(rows_ref, rows_out, sem.at[0]),
        pltpu.make_async_copy(state_ref, state_out, sem.at[1]),
    )
    for copy in copies:
        copy.start()
    for copy in copies:
        copy.wait()


def finish(rows, state):
    return pl.pallas_call(
        finish_kernel,
        out_shape=(
            jax.ShapeDtypeStruct(rows.shape, rows.dtype),
            jax.ShapeDtypeStruct(state.shape, state.dtype),
        ),
        in_specs=[pl.BlockSpec(memory_space=pltpu.VMEM)] * 2,
        out_specs=[pl.BlockSpec(memory_space=pl.ANY)] * 2,
        scratch_shapes=[pltpu.SemaphoreType.DMA((2,))],
        compiler_params=pltpu.CompilerParams(vmem_limit_bytes=4 * 1024 * 1024),
    )(rows, state)


def on_device(
    tokens,
    state,
    norm_mix,
    w_drive,
    lam_real,
    lam_imag,
    log_step,
    b_real,
    b_imag,
    readout_real,
    readout_imaginary,
    d_skip,
    w_value,
    w_glugate,
    w_output,
    norm_ffn,
    w_group,
    w_expert,
    route_ids,
    expert_gate,
    expert_up,
    expert_down,
    dense_vector,
    dense_gate,
    dense_up,
    dense_down,
):
    vmem = pl.BlockSpec(memory_space=pltpu.VMEM)
    hbm = pl.BlockSpec(memory_space=pltpu.HBM)
    rows, new_state = pl.pallas_call(
        layer_kernel,
        out_shape=(
            jax.ShapeDtypeStruct((16, 2048), BF16),
            jax.ShapeDtypeStruct((2, 16, 2048), F32),
        ),
        in_specs=[hbm] * 26,
        out_specs=(vmem, vmem),
        scratch_shapes=[
            pltpu.VMEM((16, 2048), BF16),
            pltpu.VMEM((2, 16, 2048), F32),
            pltpu.VMEM((3, 1, 2048), F32),
            pltpu.VMEM((2048, 512), BF16),
            pltpu.VMEM((2, 32, 64), F32),
            pltpu.VMEM((1, 32), F32),
            pltpu.VMEM((4, 32, 16, 64), F32),
            pltpu.VMEM((1, 512), F32),
            pltpu.VMEM((2, 512, 512), BF16),
            pltpu.VMEM((512, 2048), BF16),
            pltpu.VMEM((4, 2048), BF16),
            pltpu.VMEM((2048, 128), BF16),
            pltpu.VMEM((6, 16), jnp.int32),
            pltpu.VMEM((4, 128, 512), BF16),
            pltpu.VMEM((4, 128, 512), BF16),
            pltpu.VMEM((4, 128, 512), BF16),
            pltpu.VMEM((4, 128, 512), BF16),
            pltpu.VMEM((2, 2048), F32),
            pltpu.VMEM((16, 2048), BF16),
            pltpu.VMEM((16, 2048), BF16),
            pltpu.VMEM((4, 4, 4, 16, 2048), BF16),
            pltpu.VMEM((256, 2048), BF16),
            pltpu.VMEM((384, 2048), BF16),
            pltpu.VMEM((2, 2048, 512), BF16),
            pltpu.VMEM((2, 2048, 512), BF16),
            pltpu.VMEM((2, 512, 2048), BF16),
            pltpu.VMEM((4, 4, 4, 2, 128), F32),
            pltpu.VMEM((2, 128), F32),
            pltpu.VMEM((4, 4, 4, 16, 256), F32),
            pltpu.VMEM((4, 4, 4, 16, 384), BF16),
            pltpu.VMEM((256, 2048), F32),
            pltpu.VMEM((2048, 256), BF16),
            pltpu.VMEM((4, 4, 4, 16, 2048), BF16),
            pltpu.VMEM((3, 3, 16, 768), BF16),
            pltpu.VMEM((3, 3, 4, 16, 768), BF16),
            pltpu.VMEM((3, 3, 4, 4, 16, 768), BF16),
            pltpu.SemaphoreType.DMA((13,)),
            pltpu.SemaphoreType.DMA((4,)),
            pltpu.SemaphoreType.DMA((4,)),
            pltpu.SemaphoreType.DMA((4,)),
            pltpu.SemaphoreType.DMA((3,)),
            pltpu.SemaphoreType.DMA((3,)),
            pltpu.SemaphoreType.DMA((3, 3)),
            pltpu.SemaphoreType.DMA((3, 3)),
            pltpu.SemaphoreType.DMA((RECEIVE_SLOTS,)),
        ],
        compiler_params=pltpu.CompilerParams(
            collective_id=0, has_side_effects=True, vmem_limit_bytes=47 * 1024 * 1024
        ),
        cost_estimate=pl.CostEstimate(
            flops=8_000_000_000, bytes_accessed=20_000_000, transcendentals=0
        ),
    )(*[pltpu.with_memory_space_constraint(a, pltpu.HBM) for a in (
        tokens,
        state,
        norm_mix.reshape(1, -1),
        w_drive,
        lam_real,
        lam_imag,
        log_step.reshape(1, -1),
        jnp.transpose(b_real, (0, 2, 1)),
        jnp.transpose(b_imag, (0, 2, 1)),
        readout_real,
        readout_imaginary,
        d_skip.reshape(1, -1),
        w_value,
        w_glugate,
        w_output,
        norm_ffn.reshape(1, -1),
        jnp.transpose(w_group),
        w_expert,
        jnp.transpose(route_ids),
        dense_vector.reshape(1, -1),
        jnp.transpose(dense_gate),
        jnp.transpose(dense_up),
        dense_down,
        expert_gate[0],
        expert_up[0],
        expert_down[0],
    )])
    return finish(rows, new_state)


def solution(mesh):
    placed = (
        P("ep", None),
        P(None, "ep", None),
        P(),
        P(),
        P(),
        P(),
        P(),
        P(),
        P(),
        P(),
        P(),
        P(),
        P(),
        P(),
        P(),
        P(),
        P(),
        P(),
        P("ep", None),
        P("ep", None, None),
        P("ep", None, None),
        P("ep", None, None),
        P(),
        P(None, "ep"),
        P(None, "ep"),
        P("ep", None),
    )
    return jax.shard_map(
        on_device,
        mesh=mesh,
        in_specs=placed,
        out_specs=(P("ep", None), P(None, "ep", None)),
        check_vma=False,
    )
```
